128 devices in a mesh: sp: 16 (over z, y), tp: 8 (over x, core).
Axes of the slice: x: 4, y: 4, z: 4, core: 2. Of those that a mesh axis runs over, the one named last changes fastest.
Arguments:
- query_first: bfloat16 [12288, 8, 128], P('sp', 'tp'), may hold values from -5.375 to 5.375
- key_first: bfloat16 [12288, 8, 128], P('sp', 'tp'), may hold values from -5.375 to 5.375
- value_first: bfloat16 [12288, 8, 128], P('sp', 'tp'), may hold values from -6 to 6
- query_second: bfloat16 [12288, 8, 256], P('sp', 'tp'), may hold values from -5.375 to 5.375
- key_second: bfloat16 [12288, 8, 256], P('sp', 'tp'), may hold values from -5.375 to 5.375
- value_second: bfloat16 [12288, 8, 128], P('sp', 'tp'), may hold values from -6 to 6
- mix_lambda: float32 [2, 8], P(None, 'tp'), may hold values from 0.3 to 0.8
- head_gain: float32 [2, 8, 128], P(None, 'tp'), may hold values from 0.1 to 1.9
- out_weight: bfloat16 [2, 8, 128, 2048], P(None, 'tp'), may hold values from -0.125 to 0.125
- residual: bfloat16 [12288, 2048], P(('sp', 'tp')), may hold values from -6 to 6
- norm_gain: float32 [2, 2048], replicated, may hold values from 0.1 to 1.9
- up_weight: bfloat16 [2048, 8192], P('sp', 'tp'), may hold values from -0.125 to 0.125
- down_weight: bfloat16 [8192, 2048], P('tp', 'sp'), may hold values from -0.0625 to 0.0625
Outputs:
- mixed: bfloat16 [12288, 2048], P(('sp', 'tp'))
The draws below stay inside these ranges and needn't reach their ends.
All inputs are finite; a program needn't handle non-finite values.
Results may differ from the reference program's by a relative error of at most 0.02.
Values may be sent and summed in bfloat16 or wider, within the bound.
A program may use at most 128 MiB of HBM per device.

```python
import math
import jax
import jax.numpy as jnp
from jax import lax

D = 2048
FF = 8192
HEADS = 8
KA = 64
KB = 128
VD = 128
TOK_DEV = 768
TOKENS = 12288
N_SP = 16


def drawn_pair(key, group_tag, key_size):
    seeded = jax.random.fold_in(key, group_tag)
    seed_query, seed_keys = jax.random.split(seeded, 2)
    array_shape = (TOKENS, HEADS, 2 * key_size)
    queries = 1.3 * jax.random.truncated_normal(seed_query, -3.4, 3.4, array_shape, jnp.float32)
    key_rows = 1.3 * jax.random.truncated_normal(seed_keys, -3.4, 3.4, array_shape, jnp.float32)
    return (queries, key_rows)


def draw_query_first(key, part):
    return drawn_pair(key, 11, KA)[0].astype(jnp.bfloat16)


def draw_key_first(key, part):
    return drawn_pair(key, 11, KA)[1].astype(jnp.bfloat16)


def draw_query_second(key, part):
    return drawn_pair(key, 23, KB)[0].astype(jnp.bfloat16)


def draw_key_second(key, part):
    return drawn_pair(key, 23, KB)[1].astype(jnp.bfloat16)


def shard_levels(own_key, dims, cuts, smallest, high):
    def one(position, blocks):
        heights = jax.random.uniform(jax.random.fold_in(jax.random.fold_in(own_key, 6), position), (blocks,), jnp.float32, smallest / len(cuts), high / len(cuts))
        return jnp.repeat(jnp.exp(heights), dims[position] // blocks).reshape((-1,) + (1,) * (len(dims) - position - 1))

    loudness = one(*cuts[0])
    for cut in cuts[1:]:
        loudness = loudness * one(*cut)
    return loudness


def scatter_about(key, shape, deviation, limit, cuts=(), kind=jnp.bfloat16):
    drawn = deviation * jax.random.normal(key, shape, jnp.float32)
    if cuts:
        drawn = drawn * shard_levels(key, shape, cuts, -0.22, 0.18)
    return jnp.clip(drawn, -limit, limit).astype(kind)


def setup_inputs(seed: int = 0) -> dict:
    seeds = jax.random.split(jax.random.key(seed), 14)
    return {
        "query_first": draw_query_first(jax.random.fold_in(seeds[13], 71), 0),
        "key_first": draw_key_first(jax.random.fold_in(seeds[13], 71), 0),
        "value_first": scatter_about(seeds[2], (TOKENS, HEADS, VD), 1.0, 6.0, ((0, 16), (1, 8))),
        "query_second": draw_query_second(jax.random.fold_in(seeds[13], 71), 0),
        "key_second": draw_key_second(jax.random.fold_in(seeds[13], 71), 0),
        "value_second": scatter_about(seeds[5], (TOKENS, HEADS, VD), 1.0, 6.0, ((0, 16), (1, 8))),
        "mix_lambda": jnp.clip(0.3 + 0.5 * jax.random.uniform(seeds[6], (2, HEADS), jnp.float32) ** shard_levels(seeds[6], (2, HEADS), ((1, 8),), -0.2, 0.2), 0.3, 0.8),
        "head_gain": jnp.clip(1.0 + 0.18 * jax.random.normal(seeds[7], (2, HEADS, VD), jnp.float32), 0.1, 1.9),
        "out_weight": scatter_about(seeds[8], (2, HEADS, VD, D), D ** -0.5, 0.125, ((1, 8),)),
        "residual": scatter_about(seeds[9], (TOKENS, D), 1.0, 6.0, ((0, 128),)),
        "norm_gain": jnp.clip(1.0 + 0.18 * jax.random.normal(seeds[10], (2, D), jnp.float32), 0.1, 1.9),
        "up_weight": scatter_about(seeds[11], (D, FF), D ** -0.5, 0.125, ((0, 16), (1, 8))),
        "down_weight": scatter_about(seeds[12], (FF, D), FF ** -0.5, 0.0625, ((0, 8), (1, 16))),
    }


EPSILON = 1e-05

def layer_norm(activations, scales):
    average = lax.optimization_barrier(jnp.mean(activations, axis=-1, keepdims=True))
    centred = activations - average
    spread = lax.optimization_barrier(jnp.mean(centred * centred, axis=-1, keepdims=True))
    return centred * lax.rsqrt(spread + EPSILON) * scales

def group_attention(queries_in, keys_in, values_in, lambdas, gains, key_size):
    score_scale = 1.0 / math.sqrt(key_size)
    queries = queries_in.astype(jnp.float32).reshape(TOKENS, HEADS, 2, key_size)
    key_rows = keys_in.astype(jnp.float32).reshape(TOKENS, HEADS, 2, key_size)
    value_rows = values_in.astype(jnp.float32)
    query_blocks = queries.reshape(N_SP, TOK_DEV, HEADS, 2, key_size)

    def one_block(query_block):
        scores = jnp.einsum('qhck,phck->hcqp', query_block, key_rows) * score_scale
        peak = lax.optimization_barrier(jnp.max(scores, axis=-1, keepdims=True))
        exponent = jnp.exp(scores - peak)
        denominator = lax.optimization_barrier(jnp.sum(exponent, axis=-1))
        rounded = lax.optimization_barrier(exponent.astype(jnp.bfloat16)).astype(jnp.float32)
        numerator = jnp.einsum('hcqp,phv->hcqv', rounded, value_rows)
        attended = numerator[:, 0] / denominator[:, 0, :, None] - lambdas[:, None, None] * numerator[:, 1] / denominator[:, 1, :, None]
        mean_square = lax.optimization_barrier(jnp.mean(attended * attended, axis=-1, keepdims=True))
        return (attended * lax.rsqrt(mean_square + EPSILON) * gains[:, None, :]).astype(jnp.bfloat16)
    blocks_out = lax.map(one_block, query_blocks)
    return blocks_out.transpose(1, 0, 2, 3).reshape(HEADS, TOKENS, VD)

def reference(query_first, key_first, value_first, query_second, key_second, value_second, mix_lambda, head_gain, out_weight, residual, norm_gain, up_weight, down_weight):
    heads_first = group_attention(query_first, key_first, value_first, mix_lambda[0], head_gain[0], KA)
    heads_second = group_attention(query_second, key_second, value_second, mix_lambda[1], head_gain[1], KB)
    stacked = jnp.stack([heads_first, heads_second]).astype(jnp.float32)
    projected = jnp.einsum('ghtv,ghvd->td', stacked, out_weight.astype(jnp.float32)) + residual.astype(jnp.float32)
    normed = layer_norm(projected, norm_gain[0])
    expanded = jnp.dot(normed.astype(jnp.bfloat16), up_weight, preferred_element_type=jnp.float32)
    hidden = jnp.square(jnp.maximum(expanded, 0.0)).astype(jnp.bfloat16)
    mixed_sum = jnp.dot(hidden, down_weight, preferred_element_type=jnp.float32)
    return layer_norm(normed + mixed_sum, norm_gain[1]).astype(jnp.bfloat16)
```

```python
import functools
import math

import jax
import jax.numpy as jnp
from jax import lax
from jax.experimental import pallas as pl
from jax.experimental.pallas import tpu as pltpu
from jax.sharding import PartitionSpec as P

EPSILON = 1e-05
LOWEST = -1e30
LOG2E = math.log2(math.e)
MESH = pl.DeviceIdType.MESH
BF16 = jnp.bfloat16
F32 = jnp.float32

TOK = 768
OWN = 96
SIZE = 128
VALUE = 128
SLAB = TOK + VALUE * TOK // 256
TILE = 512
TILES = 2 * TOK // TILE
ROWS = VALUE + 16


def attention_kernel(q_ref, kv_ref, prm_ref, out_ref, q_all, kv_all, prm_all, s0, s1, top, acc, heads, got,
                     q_send, kv_send, prm_send, right_send, left_send, side_send, head_send,
                     q_recv, kv_recv, prm_recv, head_recv):
    sp, tp = lax.axis_index("sp"), lax.axis_index("tp")
    z, y = lax.div(sp, 4), lax.rem(sp, 4)
    x, c = lax.div(tp, 2), lax.rem(tp, 2)

    def at(z_, y_, x_, c_):
        return {"sp": z_ * 4 + y_, "tp": x_ * 2 + c_}

    above, below = lax.rem(z + 1, 4), lax.rem(z + 3, 4)
    far = lax.rem(z + 2, 4)
    right, left, side = at(above, y, x, c), at(below, y, x, c), at(z, y, x, 1 - c)

    barrier = pltpu.get_barrier_semaphore()

    def greet(i, carry):
        other = lax.rem(y * 8 + tp + i, 32)
        pl.semaphore_signal(barrier, inc=1, device_id={"sp": z * 4 + lax.div(other, 8), "tp": lax.rem(other, 8)},
                            device_id_type=MESH)
        return carry

    lax.fori_loop(1, 32, greet, 0)
    pl.semaphore_signal(barrier, inc=1, device_id=right, device_id_type=MESH)
    pl.semaphore_signal(barrier, inc=1, device_id=left, device_id_type=MESH)
    pl.semaphore_wait(barrier, 33)

    def remote(src, dst, send, recv, device):
        return pltpu.make_async_remote_copy(src_ref=src, dst_ref=dst, send_sem=send, recv_sem=recv, device_id=device,
                                            device_id_type=MESH)

    half = lax.div(y, 2)
    slot_j = lax.rem(y, 2)

    def spread(g):
        u = 2 * c + g
        to = at(z, u, x, half)
        lanes = pl.ds(pl.multiple_of(slot_j * TOK, TOK), TOK)
        return (
            (q_ref.at[g], q_all.at[:, :, lanes], q_send.at[g], q_recv.at[slot_j], to),
            (prm_ref.at[g], prm_all.at[slot_j], prm_send.at[g], prm_recv.at[slot_j], to),
            (kv_ref.at[g], kv_all.at[z * 4 + y], kv_send.at[g], kv_recv.at[z * 4 + y], to),
        )

    for part in range(3):
        for g in range(2):
            src, dst, send, recv, to = spread(g)[part]
            mine = 2 * c + g == y

            @pl.when(mine)
            def _():
                pltpu.make_async_copy(src, dst, recv).start()

            @pl.when(jnp.logical_not(mine))
            def _():
                remote(src, dst, send, recv, to).start()

    def arrive(slot):
        remote(kv_all.at[slot], kv_all.at[slot], kv_send.at[0], kv_recv.at[slot], side).wait_recv()

    def to_side(slot, n):
        return remote(kv_all.at[slot], kv_all.at[slot], side_send.at[n], kv_recv.at[slot], side)

    def to_right(slot, n):
        return remote(kv_all.at[slot], kv_all.at[slot], right_send.at[n], kv_recv.at[slot], right)

    def to_left(slot, n):
        return remote(kv_all.at[slot], kv_all.at[slot], left_send.at[n], kv_recv.at[slot], left)

    first = z * 4 + 2 * c
    arrive(first)
    to_right(first, 0).start()
    arrive(first + 1)
    to_left(first + 1, 0).start()
    to_right(first + 1, 1).start()
    to_left(first, 1).start()
    to_side(first, 0).start()
    to_side(first + 1, 1).start()

    def slot_of(i):
        group, r = lax.div(i, 4), lax.rem(i, 4)
        e = lax.rem(r, 2)
        core = jnp.where(r >= 2, 1 - c, c)
        near = jnp.where(e == 0, below, above)
        row = jnp.where(group == 0, z, jnp.where(group == 3, far, near))
        j = jnp.where(group == 2, 1 - e, e)
        return row * 4 + 2 * core + j

    def duty(i):
        group, r = lax.div(i, 4), lax.rem(i, 4)

        @pl.when(jnp.logical_and(r == 0, jnp.logical_and(group > 0, group < 4)))
        def _():
            for e in range(2):
                slot = slot_of(group * 4 + e)
                arrive(slot)

                @pl.when(group == 1)
                def _():
                    (to_right if e == 0 else to_left)(slot, 2).start()

                to_side(slot, group * 2 + e).start()

        @pl.when(r >= 2)
        def _():
            arrive(slot_of(i))

    for j in range(2):
        remote(q_ref.at[0], q_all.at[:, :, pl.ds(j * TOK, TOK)], q_send.at[0], q_recv.at[j], side).wait_recv()
        remote(prm_ref.at[0], prm_all.at[j], prm_send.at[0], prm_recv.at[j], side).wait_recv()

    top[...] = jnp.full(top.shape, LOWEST, F32)
    acc[...] = jnp.zeros(acc.shape, F32)
    ones = jnp.ones((ROWS - VALUE, 256), BF16)

    def scores(slot, tile, m, held):
        queries = q_all[m, :, pl.ds(pl.multiple_of(tile * TILE, TILE), TILE)]
        peak = None
        for r in range(0, TOK, TOK // 2):
            s = jnp.dot(kv_all[slot, r : r + TOK // 2, m * SIZE : (m + 1) * SIZE], queries, preferred_element_type=F32)
            held[r : r + TOK // 2] = s
            p = jnp.max(s, axis=0, keepdims=True)
            peak = p if peak is None else jnp.maximum(peak, p)
        return peak

    def absorb(slot, tile, m, held, peak):
        old = top[tile, m]
        new = jnp.maximum(old, peak)
        top[tile, m] = new
        weights = jnp.exp2(held[...] - new).astype(BF16)
        added = None
        for b in range(TOK // 256):
            values = kv_all[slot, TOK + b * VALUE : TOK + (b + 1) * VALUE, :]
            d = jnp.dot(jnp.concatenate([values, ones], axis=0), weights[b * 256 : (b + 1) * 256],
                        preferred_element_type=F32)
            added = d if added is None else added + d
        acc[tile, m] = acc[tile, m] * jnp.exp2(old - new) + added

    peak = scores(first, 0, 0, s0)

    def step(t, peak0):
        i, tile = lax.div(t, TILES), lax.rem(t, TILES)
        slot = slot_of(i)

        @pl.when(tile == TILES - 1)
        def _():
            duty(i + 1)

        peak1 = scores(slot, tile, 1, s1)
        absorb(slot, tile, 0, s0, peak0)
        later = jnp.minimum(t + 1, 16 * TILES - 1)
        peak0 = scores(slot_of(lax.div(later, TILES)), lax.rem(later, TILES), 0, s0)
        absorb(slot, tile, 1, s1, peak1)
        return peak0

    lax.fori_loop(0, 16 * TILES, step, peak)

    gain = prm_all[0, 0:1, :]
    mix = prm_all[0, 1:2, 0:1]
    for tile in range(TILES):
        a1, a2 = acc[tile, 0], acc[tile, 1]
        attended = a1[:VALUE] / a1[VALUE : VALUE + 1] - mix * (a2[:VALUE] / a2[VALUE : VALUE + 1])
        square = jnp.mean(attended * attended, axis=0, keepdims=True)
        scaled = attended * lax.rsqrt(square + EPSILON)
        heads[tile * TILE : (tile + 1) * TILE, :] = (scaled.T * gain).astype(BF16)

    unit = (2 * x + lax.div(y, 2)) * 2 + lax.rem(y, 2)

    def deliver(n):
        j, tp_ = n // 8, n % 8
        to = {"sp": z * 4 + 2 * c + j, "tp": jnp.int32(tp_)}
        mine = jnp.logical_and(2 * c + j == y, tp == tp_)
        return heads.at[pl.ds(n * OWN, OWN)], got.at[unit], head_send.at[n], head_recv.at[unit], to, mine

    for n in range(16):
        src, dst, send, recv, to, mine = deliver(n)

        @pl.when(mine)
        def _():
            pltpu.make_async_copy(src, dst, recv).start()

        @pl.when(jnp.logical_not(mine))
        def _():
            remote(src, dst, send, recv, to).start()

    for part in range(3):
        for g in range(2):
            src, dst, send, recv, to = spread(g)[part]

            @pl.when(jnp.logical_not(2 * c + g == y))
            def _():
                remote(src, dst, send, recv, to).wait_send()

    for n in range(3):
        to_right(first, n).wait_send()
        to_left(first, n).wait_send()
    for n in range(8):
        to_side(first, n).wait_send()
    for n in range(16):
        src, dst, send, recv, to, mine = deliver(n)

        @pl.when(jnp.logical_not(mine))
        def _():
            remote(src, dst, send, recv, to).wait_send()

    for n in range(16):
        remote(got.at[n], got.at[n], head_send.at[n], head_recv.at[n], side).wait_recv()
    out_ref[...] = got[...]


def attention(q, kv, prm):
    dma = pltpu.SemaphoreType.DMA
    vmem = pl.BlockSpec(memory_space=pltpu.VMEM)
    return pl.pallas_call(
        attention_kernel,
        out_shape=jax.ShapeDtypeStruct((16, OWN, VALUE), BF16),
        in_specs=[vmem] * 3,
        out_specs=vmem,
        scratch_shapes=[
            pltpu.VMEM((2, SIZE, 2 * TOK), BF16),
            pltpu.VMEM((16, SLAB, 256), BF16),
            pltpu.VMEM((2, 8, 128), F32),
            pltpu.VMEM((TOK, TILE), F32),
            pltpu.VMEM((TOK, TILE), F32),
            pltpu.VMEM((TILES, 2, 1, TILE), F32),
            pltpu.VMEM((TILES, 2, ROWS, TILE), F32),
            pltpu.VMEM((2 * TOK, VALUE), BF16),
            pltpu.VMEM((16, OWN, VALUE), BF16),
            dma((2,)), dma((2,)), dma((2,)), dma((3,)), dma((3,)), dma((8,)), dma((16,)),
            dma((2,)), dma((16,)), dma((2,)), dma((16,)),
        ],
        compiler_params=pltpu.CompilerParams(collective_id=0, has_side_effects=True, vmem_limit_bytes=36 << 20),
        cost_estimate=pl.CostEstimate(flops=4 * 768 * 12288 * 4 * 128, bytes_accessed=4 << 20, transcendentals=4 * 768 * 12288),
        name="attention",
    )(q, kv, prm)


def layer_norm(activations, scales):
    average = jnp.mean(activations, axis=-1, keepdims=True)
    centred = activations - average
    spread = jnp.mean(centred * centred, axis=-1, keepdims=True)
    return centred * lax.rsqrt(spread + EPSILON) * scales


def kernel_operands(query_first, key_first, value_first, query_second, key_second, value_second, mix_lambda, head_gain):
    first = query_first[:, 0].astype(F32) * (LOG2E / 8.0)
    high = lax.reduce_precision(first, 8, 7)
    low = first - high
    second = query_second[:, 0].astype(F32) * (LOG2E / math.sqrt(128.0))
    q = jnp.stack([
        jnp.stack([jnp.concatenate([high[:, :64], low[:, :64]], 1), jnp.concatenate([high[:, 64:], low[:, 64:]], 1)]),
        jnp.stack([second[:, :128], second[:, 128:]]),
    ]).astype(BF16)
    q = jnp.swapaxes(q, 2, 3)
    one, two = key_first[:, 0, :64], key_first[:, 0, 64:]
    keys = jnp.stack([jnp.concatenate([one, one, two, two], 1), key_second[:, 0]])
    values = jnp.stack([value_first[:, 0], value_second[:, 0]])
    values = jnp.swapaxes(values.reshape(2, 3, 256, VALUE), 2, 3).reshape(2, 3 * VALUE, 256)
    kv = jnp.concatenate([keys, values], axis=1)
    prm = jnp.concatenate([head_gain, jnp.broadcast_to(mix_lambda[:, :, None], (2, 1, 128)), jnp.zeros((2, 6, 128), F32)], axis=1)
    return q, kv, prm


def squared_relu(expanded):
    return jnp.square(jnp.maximum(expanded, 0.0)).astype(BF16)


def local(query_first, key_first, value_first, query_second, key_second, value_second, mix_lambda, head_gain, out_weight,
          residual, norm_gain, up_weight, down_weight):
    both = lax.all_gather(jnp.concatenate([up_weight, down_weight.T], axis=1), "sp", axis=0, tiled=True)
    hidden_units = up_weight.shape[1]
    out_whole = lax.all_gather(out_weight[:, 0], "tp", axis=0, tiled=False).reshape(-1, out_weight.shape[-1])
    q, kv, prm = kernel_operands(query_first, key_first, value_first, query_second, key_second, value_second, mix_lambda, head_gain)
    heads = attention(q, kv, prm)
    heads = jnp.swapaxes(heads, 0, 1).reshape(OWN, 16 * VALUE)
    projected = jnp.dot(heads, out_whole, preferred_element_type=F32) + residual.astype(F32)
    normed = layer_norm(projected, norm_gain[0])
    mixer_in = lax.all_gather(normed.astype(BF16), "tp", axis=0, tiled=True)
    hidden = squared_relu(jnp.dot(mixer_in, both[:, :hidden_units], preferred_element_type=F32))
    partial = lax.dot_general(hidden, both[:, hidden_units:], (((1,), (1,)), ((), ())), preferred_element_type=F32)
    mixed_sum = lax.psum_scatter(partial.astype(BF16), "tp", scatter_dimension=0, tiled=True).astype(F32)
    return layer_norm(normed + mixed_sum, norm_gain[1]).astype(BF16)


def solution(mesh):
    heads = P("sp", "tp", None)
    return jax.shard_map(
        local,
        mesh=mesh,
        in_specs=(heads, heads, heads, heads, heads, heads, P(None, "tp"), P(None, "tp", None), P(None, "tp", None, None),
                  P(("sp", "tp"), None), P(), P("sp", "tp"), P("tp", "sp")),
        out_specs=P(("sp", "tp"), None),
        check_vma=False,
    )
```

```python
import functools
import math

import jax
import jax.numpy as jnp
from jax import lax
from jax.experimental import pallas as pl
from jax.experimental.pallas import tpu as pltpu
from jax.sharding import PartitionSpec as P

EPSILON = 1e-05
LOWEST = -1e30
LOG2E = math.log2(math.e)
MESH = pl.DeviceIdType.MESH
BF16 = jnp.bfloat16
F32 = jnp.float32

TOK = 768
OWN = 96
SIZE = 128
VALUE = 128
SLAB = TOK + VALUE * TOK // 256
TILE = 512
TILES = 2 * TOK // TILE
ROWS = VALUE + 16


def attention_kernel(q_ref, kv_ref, prm_ref, w_ref, up_ref, down_ref, residual_ref, gain_ref, out_ref, q_all, kv_all, prm_all, w_all, s0, s1, top, acc, heads, got,
                     q_send, kv_send, prm_send, right_send, left_send, side_send, head_send, w_send,
                     q_recv, kv_recv, prm_recv, head_recv, w_recv, w_far, w_own,
                     up_all, down_all, tokens, normed, hidden, keep, to_sib, from_sib, to_chip, from_chip,
                     ff_send, up_recv, down_recv, ff_far, ff_own, tok_send, tok_recv, tok_far, sib_send, sib_recv,
                     chip_send, chip_recv):
    sp, tp = lax.axis_index("sp"), lax.axis_index("tp")
    z, y = lax.div(sp, 4), lax.rem(sp, 4)
    x, c = lax.div(tp, 2), lax.rem(tp, 2)

    def at(z_, y_, x_, c_):
        return {"sp": z_ * 4 + y_, "tp": x_ * 2 + c_}

    above, below = lax.rem(z + 1, 4), lax.rem(z + 3, 4)
    far = lax.rem(z + 2, 4)
    right, left, side = at(above, y, x, c), at(below, y, x, c), at(z, y, x, 1 - c)

    barrier = pltpu.get_barrier_semaphore()

    def greet(i, carry):
        other = lax.rem(y * 8 + tp + i, 32)
        pl.semaphore_signal(barrier, inc=1, device_id={"sp": z * 4 + lax.div(other, 8), "tp": lax.rem(other, 8)},
                            device_id_type=MESH)
        return carry

    lax.fori_loop(1, 32, greet, 0)
    pl.semaphore_signal(barrier, inc=1, device_id=right, device_id_type=MESH)
    pl.semaphore_signal(barrier, inc=1, device_id=left, device_id_type=MESH)
    pl.semaphore_wait(barrier, 33)

    def remote(src, dst, send, recv, device):
        return pltpu.make_async_remote_copy(src_ref=src, dst_ref=dst, send_sem=send, recv_sem=recv, device_id=device,
                                            device_id_type=MESH)

    half, odd = lax.div(y, 2), lax.rem(y, 2)
    home = c == half

    def spread(g):
        to = at(z, 2 * c + g, x, half)
        lanes = pl.ds(pl.multiple_of(odd * TOK, TOK), TOK)
        return (
            (q_ref.at[g], q_all.at[:, :, lanes], q_send.at[g], q_recv.at[odd], to),
            (prm_ref.at[g], prm_all.at[odd], prm_send.at[g], prm_recv.at[odd], to),
            (kv_ref.at[g], kv_all.at[z * 4 + y], kv_send.at[g], kv_recv.at[z * 4 + y], to),
        )

    def own(part, g):
        src, dst, send, recv, to = spread(g)[part]

        @pl.when(2 * c + g == y)
        def _():
            pltpu.make_async_copy(src, dst, recv).start()

    def away(part, g):
        src, dst, send, recv, to = spread(g)[part]

        @pl.when(jnp.logical_not(2 * c + g == y))
        def _():
            remote(src, dst, send, recv, to).start()

    for part in range(3):
        for g in range(2):
            own(part, g)
    for part in range(2):
        for g in range(2):
            away(part, g)
    def near_or_far(far_ones):
        for g in range(2):
            @pl.when(odd == (g if far_ones else 1 - g))
            def _():
                away(2, g)

    near_or_far(False)

    def place(kind):
        return (y, y + 1 - 2 * odd, 3 - y, lax.rem(y + 2, 4))[kind]

    rows = (z, below, above, far)

    def arrive(slot):
        remote(kv_all.at[slot], kv_all.at[slot], kv_send.at[0], kv_recv.at[slot], side).wait_recv()

    def to_side(slot, n):
        return remote(kv_all.at[slot], kv_all.at[slot], side_send.at[n], kv_recv.at[slot], side)

    def to_right(slot, n):
        return remote(kv_all.at[slot], kv_all.at[slot], right_send.at[n], kv_recv.at[slot], right)

    def to_left(slot, n):
        return remote(kv_all.at[slot], kv_all.at[slot], left_send.at[n], kv_recv.at[slot], left)

    def pass_on(kind, row):
        slot = rows[row] * 4 + place(kind)
        second = kind % 2
        arrive(slot)
        if row == 0:
            to_right(slot, second).start()
            to_left(slot, second).start()
        elif row == 1 and not second:
            to_right(slot, 2).start()
        elif row == 2 and second:
            to_left(slot, 2).start()
        to_side(slot, second * 4 + row).start()

    east, west = at(z, y, lax.rem(x + 1, 4), c), at(z, y, lax.rem(x + 3, 4), c)
    head_here, head_east = 2 * x + c, 2 * lax.rem(x + 1, 4) + c
    head_west, head_far = 2 * lax.rem(x + 3, 4) + c, 2 * lax.rem(x + 2, 4) + c

    def w_copy(n):
        full = lambda h: w_all.at[h]
        part = lambda h, k: w_all.at[h, pl.ds(k * 128, 128)]
        return (
            lambda: remote(w_ref, full(head_here), w_send.at[0], w_recv.at[head_here], east),
            lambda: remote(w_ref, full(head_here), w_send.at[1], w_recv.at[head_here], west),
            lambda: remote(w_ref, full(head_here), w_send.at[2], w_recv.at[head_here], side),
            lambda: remote(part(head_west, 0), part(head_west, 0), w_send.at[3], w_far.at[0], east),
            lambda: remote(part(head_east, 1), part(head_east, 1), w_send.at[4], w_far.at[1], west),
            lambda: remote(full(head_west), full(head_west), w_send.at[5], w_recv.at[head_west], side),
            lambda: remote(full(head_east), full(head_east), w_send.at[6], w_recv.at[head_east], side),
            lambda: remote(full(head_far), full(head_far), w_send.at[7], w_recv.at[head_far], side),
        )[n]()

    def w_arrive(h):
        remote(w_all.at[h], w_all.at[h], w_send.at[0], w_recv.at[h], side).wait_recv()

    forth, back = at(z, lax.rem(y + 1, 4), x, c), at(z, lax.rem(y + 3, 4), x, c)
    y_forth, y_back, y_far = lax.rem(y + 1, 4), lax.rem(y + 3, 4), lax.rem(y + 2, 4)

    def up_at(s, k=None):
        if k is None:
            return up_all.at[pl.ds(pl.multiple_of(s * 128, 128), 128)]
        return up_all.at[pl.ds(pl.multiple_of(s * 128 + k * 64, 64), 64)]

    def down_at(s, k=None):
        lanes = pl.ds(pl.multiple_of(s * 128, 128), 128)
        return down_all.at[:, lanes] if k is None else down_all.at[pl.ds(k * 512, 512), lanes]

    own_refs, whole, ff_recv = (up_ref, down_ref), (up_at, down_at), (up_recv, down_recv)

    def ff_first(w, k):
        return remote(own_refs[w], whole[w](sp), ff_send.at[16 * w + k], ff_recv[w].at[sp], (right, left)[k])

    def ff_half(w, k):
        shard = whole[w]((below, above)[k] * 4 + y, k)
        return remote(shard, shard, ff_send.at[16 * w + 2 + k], ff_far.at[2 * w + k], (right, left)[k])

    def ff_column(w, row, k):
        s = row * 4 + y
        return remote(whole[w](s), whole[w](s), ff_send.at[16 * w + 4 + 2 * row + k], ff_recv[w].at[s], (forth, back)[k])

    def ff_onward(w, n, k):
        s = (n + 2 * k) * 4 + (y_back, y_forth)[k]
        return remote(whole[w](s), whole[w](s), ff_send.at[16 * w + 12 + 2 * n + k], ff_recv[w].at[s], (forth, back)[k])

    def ff_arrive(w, s):
        remote(whole[w](s), whole[w](s), ff_send.at[0], ff_recv[w].at[s], side).wait_recv()

    def weights_begin():
        for w in range(2):
            pltpu.make_async_copy(own_refs[w], whole[w](sp), ff_own.at[w]).start()
            for k in range(2):
                ff_first(w, k).start()

    def weights_halves():
        for w in range(2):
            ff_arrive(w, below * 4 + y)
            ff_half(w, 0).start()
            ff_arrive(w, above * 4 + y)
            ff_half(w, 1).start()

    def weights_columns(w):
        if w == 0:
            for v in range(2):
                for k in range(2):
                    shard = whole[v](far * 4 + y, k)
                    remote(shard, shard, ff_send.at[0], ff_far.at[2 * v + k], side).wait_recv()
                pltpu.make_async_copy(own_refs[v], whole[v](sp), ff_own.at[v]).wait()
        for n in range(2):
            for k in range(2):
                ff_column(w, n + 2 * k, k).start()
        for n in range(2):
            for k in range(2):
                ff_column(w, n + 2 - 2 * k, k).start()

    def weights_onward(w):
        for n in range(2):
            for k in range(2):
                ff_arrive(w, (n + 2 * k) * 4 + (y_back, y_forth)[k])
                ff_onward(w, n, k).start()

    def weights_rest(w):
        for n in range(2):
            for k in range(2):
                ff_arrive(w, (n + 2 - 2 * k) * 4 + (y_back, y_forth)[k])
                ff_arrive(w, (n + 2 * k) * 4 + y_far)

    for n in range(3):
        w_copy(n).start()
    pltpu.make_async_copy(w_ref, w_all.at[head_here], w_own).start()

    @pl.when(home)
    def _():
        pass_on(0, 0)

    weights_begin()

    @pl.when(home)
    def _():
        pass_on(0, 1)
        pass_on(0, 2)

    kinds = (0, 0, 0, 0, 1, 2, 1, 1, 2, 2, 3, 1, 2, 3, 3, 3)
    order = (0, 1, 2, 3, 0, 0, 1, 2, 1, 2, 0, 3, 3, 1, 2, 3)
    home_duties = {1: ((0, 3),), 2: ((1, 0),), 5: ((1, 1), (1, 2)), 9: ((1, 3),)}
    away_duties = {2: ((2, 0),), 5: ((2, 1), (2, 2)), 6: ((3, 0),), 9: ((2, 3),), 11: ((3, 1), (3, 2)), 13: ((3, 3),)}

    def pick(i, table):
        value = jnp.int32(table[0])
        for n in range(1, 16):
            if table[n] != table[n - 1]:
                value = jnp.where(i >= n, table[n], value)
        return value

    def slot_of(i):
        kind, row = pick(i, kinds), pick(i, order)
        row = jnp.where(row == 0, z, jnp.where(row == 1, below, jnp.where(row == 2, above, far)))
        spot = jnp.where(kind == 0, y, jnp.where(kind == 1, y + 1 - 2 * odd, jnp.where(kind == 2, 3 - y, lax.rem(y + 2, 4))))
        return row * 4 + spot

    def duty(i):
        for n in range(16):
            for mine, duties in ((home, home_duties), (jnp.logical_not(home), away_duties)):
                if n in duties:
                    @pl.when(jnp.logical_and(i == n, mine))
                    def _():
                        for kind, row in duties[n]:
                            pass_on(kind, row)
        kind = pick(i + 1, kinds)

        @pl.when(jnp.logical_and(i < 15, jnp.logical_not(home) == (kind < 2)))
        def _():
            arrive(slot_of(i + 1))

        @pl.when(i == 1)
        def _():
            near_or_far(True)

        @pl.when(i == 2)
        def _():
            weights_halves()

        @pl.when(i == 4)
        def _():
            weights_columns(0)

        @pl.when(i == 8)
        def _():
            weights_onward(0)
            weights_columns(1)

        @pl.when(i == 3)
        def _():
            w_arrive(head_west)
            w_copy(3).start()
            w_arrive(head_east)
            w_copy(4).start()
            w_copy(5).start()
            w_copy(6).start()

        @pl.when(i == 7)
        def _():
            for k in range(2):
                remote(w_all.at[0, pl.ds(0, 128)], w_all.at[head_far, pl.ds(k * 128, 128)], w_send.at[0], w_far.at[k],
                       side).wait_recv()
            w_copy(7).start()

    for j in range(2):
        remote(q_ref.at[0], q_all.at[:, :, pl.ds(j * TOK, TOK)], q_send.at[0], q_recv.at[j], side).wait_recv()
        remote(prm_ref.at[0], prm_all.at[j], prm_send.at[0], prm_recv.at[j], side).wait_recv()

    top[...] = jnp.full(top.shape, LOWEST, F32)
    acc[...] = jnp.zeros(acc.shape, F32)
    ones = jnp.ones((ROWS - VALUE, 256), BF16)

    def scores(slot, tile, m, held):
        queries = q_all[m, :, pl.ds(pl.multiple_of(tile * TILE, TILE), TILE)]
        peak = None
        for r in range(0, TOK, TOK // 2):
            s = jnp.dot(kv_all[slot, r : r + TOK // 2, m * SIZE : (m + 1) * SIZE], queries, preferred_element_type=F32)
            held[r : r + TOK // 2] = s
            p = jnp.max(s, axis=0, keepdims=True)
            peak = p if peak is None else jnp.maximum(peak, p)
        return peak

    def absorb(slot, tile, m, held, peak):
        old = top[tile, m]
        new = jnp.maximum(old, peak)
        top[tile, m] = new
        weights = jnp.exp2(held[...] - new).astype(BF16)
        added = None
        for b in range(TOK // 256):
            values = kv_all[slot, TOK + b * VALUE : TOK + (b + 1) * VALUE, :]
            d = jnp.dot(jnp.concatenate([values, ones], axis=0), weights[b * 256 : (b + 1) * 256],
                        preferred_element_type=F32)
            added = d if added is None else added + d
        acc[tile, m] = acc[tile, m] * jnp.exp2(old - new) + added

    @pl.when(jnp.logical_not(home))
    def _():
        arrive(slot_of(jnp.int32(0)))

    peak = scores(slot_of(jnp.int32(0)), 0, 0, s0)

    def step(t, peak0):
        i, tile = lax.div(t, TILES), lax.rem(t, TILES)
        slot = slot_of(i)

        @pl.when(tile == TILES - 1)
        def _():
            duty(i)

        peak1 = scores(slot, tile, 1, s1)
        absorb(slot, tile, 0, s0, peak0)
        later = jnp.minimum(t + 1, 16 * TILES - 1)
        peak0 = scores(slot_of(lax.div(later, TILES)), lax.rem(later, TILES), 0, s0)
        absorb(slot, tile, 1, s1, peak1)
        return peak0

    lax.fori_loop(0, 16 * TILES, step, peak)

    gain = prm_all[0, 0:1, :]
    mix = prm_all[0, 1:2, 0:1]
    for tile in range(TILES):
        a1, a2 = acc[tile, 0], acc[tile, 1]
        attended = a1[:VALUE] / a1[VALUE : VALUE + 1] - mix * (a2[:VALUE] / a2[VALUE : VALUE + 1])
        square = jnp.mean(attended * attended, axis=0, keepdims=True)
        scaled = attended * lax.rsqrt(square + EPSILON)
        heads[tile * TILE : (tile + 1) * TILE, :] = (scaled.T * gain).astype(BF16)

    unit = (2 * x + lax.div(y, 2)) * 2 + lax.rem(y, 2)

    def deliver(n):
        j, tp_ = n // 8, n % 8
        to = {"sp": z * 4 + 2 * c + j, "tp": jnp.int32(tp_)}
        mine = jnp.logical_and(2 * c + j == y, tp == tp_)
        return heads.at[pl.ds(n * OWN, OWN)], got.at[unit], head_send.at[n], head_recv.at[unit], to, mine

    for n in range(16):
        src, dst, send, recv, to, mine = deliver(n)

        @pl.when(mine)
        def _():
            pltpu.make_async_copy(src, dst, recv).start()

        @pl.when(jnp.logical_not(mine))
        def _():
            remote(src, dst, send, recv, to).start()

    weights_onward(1)
    for n in range(4):
        w_arrive(2 * n + 1 - c)
    pltpu.make_async_copy(w_ref, w_all.at[head_here], w_own).wait()
    for n in range(16):
        remote(got.at[n], got.at[n], head_send.at[n], head_recv.at[n], side).wait_recv()

    def project(n, carry):
        columns = pl.ds(pl.multiple_of(n * 512, 512), 512)
        total = residual_ref[:, columns].astype(F32)
        for h in range(8):
            pair = jnp.concatenate([got[2 * h], got[2 * h + 1]], axis=1)
            total = total + jnp.dot(pair, w_all[h, :, columns], preferred_element_type=F32)
        normed[:, columns] = total
        return carry

    lax.fori_loop(0, 4, project, 0)
    for r in range(0, OWN, 32):
        value = layer_norm(normed[r : r + 32], gain_ref[0:1])
        normed[r : r + 32] = value
        tokens[tp, r : r + 32] = value.astype(BF16)

    def tok_copy(n):
        t_west, t_east, t_far = 2 * lax.rem(x + 3, 4) + c, 2 * lax.rem(x + 1, 4) + c, 2 * lax.rem(x + 2, 4) + c
        half_of = lambda t, k: tokens.at[t, pl.ds(k * 48, 48)]
        return (
            lambda: remote(tokens.at[tp], tokens.at[tp], tok_send.at[0], tok_recv.at[tp], east),
            lambda: remote(tokens.at[tp], tokens.at[tp], tok_send.at[1], tok_recv.at[tp], west),
            lambda: remote(tokens.at[tp], tokens.at[tp], tok_send.at[2], tok_recv.at[tp], side),
            lambda: remote(half_of(t_west, 0), half_of(t_west, 0), tok_send.at[3], tok_far.at[0], east),
            lambda: remote(half_of(t_east, 1), half_of(t_east, 1), tok_send.at[4], tok_far.at[1], west),
            lambda: remote(tokens.at[t_west], tokens.at[t_west], tok_send.at[5], tok_recv.at[t_west], side),
            lambda: remote(tokens.at[t_east], tokens.at[t_east], tok_send.at[6], tok_recv.at[t_east], side),
            lambda: remote(tokens.at[t_far], tokens.at[t_far], tok_send.at[7], tok_recv.at[t_far], side),
        )[n]()

    def tok_arrive(t):
        remote(tokens.at[t], tokens.at[t], tok_send.at[0], tok_recv.at[t], side).wait_recv()

    for n in range(3):
        tok_copy(n).start()
    weights_rest(0)

    chips = (x, lax.rem(x + 3, 4), lax.rem(x + 1, 4), lax.rem(x + 2, 4))

    def feed(k):
        chip = chips[k]
        rows_in = (2 * chip + c, 2 * chip + 1 - c)

        def up(n, carry):
            columns = pl.ds(pl.multiple_of(n * 512, 512), 512)
            block = jnp.concatenate([tokens[rows_in[0]], tokens[rows_in[1]]], axis=0)
            e = jnp.maximum(jnp.dot(block, up_all[:, columns], preferred_element_type=F32), 0.0)
            hidden[:, columns] = (e * e).astype(BF16)
            return carry

        lax.fori_loop(0, 2, up, 0)
        if k == 0:
            weights_rest(1)

        def down(n, carry):
            columns = pl.ds(pl.multiple_of(n * 512, 512), 512)
            p = jnp.dot(hidden[...], down_all[:, columns], preferred_element_type=F32)
            keep[k, :, columns] = p[:OWN]
            to_sib[k, :, columns] = p[OWN:].astype(BF16)
            return carry

        lax.fori_loop(0, 4, down, 0)

    def to_sibling(k):
        return remote(to_sib.at[k], from_sib.at[k], sib_send.at[k], sib_recv.at[k], side)

    def to_owner(k):
        return remote(to_chip.at[k - 1], from_chip.at[k - 1], chip_send.at[k - 1], chip_recv.at[k - 1], (None, west, east, at(z, y, lax.rem(x + 2, 4), c))[k])

    def chip_sum(k):
        to_sibling(k).wait_recv()
        for r in range(0, OWN, 32):
            to_chip[k - 1, r : r + 32] = (keep[k, r : r + 32] + from_sib[k, r : r + 32].astype(F32)).astype(BF16)
        to_owner(k).start()

    tok_arrive(2 * x + 1 - c)
    feed(0)
    to_sibling(0).start()
    west_tok, east_tok, far_tok = (2 * chips[k] + c for k in (1, 2, 3))
    tok_arrive(west_tok)
    tok_copy(3).start()
    tok_copy(5).start()
    tok_arrive(east_tok)
    tok_copy(4).start()
    tok_copy(6).start()
    tok_arrive(2 * chips[1] + 1 - c)
    feed(1)
    to_sibling(1).start()
    tok_arrive(2 * chips[2] + 1 - c)
    feed(2)
    to_sibling(2).start()
    chip_sum(1)
    for k in range(2):
        spot = tokens.at[far_tok, pl.ds(k * 48, 48)]
        remote(spot, spot, tok_send.at[0], tok_far.at[k], side).wait_recv()
    tok_copy(7).start()
    chip_sum(2)
    tok_arrive(2 * chips[3] + 1 - c)
    feed(3)
    to_sibling(3).start()
    chip_sum(3)
    to_sibling(0).wait_recv()
    for k in range(1, 4):
        to_owner(k).wait_recv()
    for r in range(0, OWN, 32):
        span = slice(r, r + 32)
        total = normed[span] + keep[0, span] + from_sib[0, span].astype(F32)
        for k in range(3):
            total = total + from_chip[k, span].astype(F32)
        out_ref[span] = layer_norm(total, gain_ref[1:2]).astype(BF16)

    for part in range(3):
        for g in range(2):
            src, dst, send, recv, to = spread(g)[part]

            @pl.when(jnp.logical_not(2 * c + g == y))
            def _():
                remote(src, dst, send, recv, to).wait_send()

    for n in range(2):
        to_right(0, n).wait_send()
        to_left(0, n).wait_send()
    to_right(0, 2).wait_send()
    to_left(0, 2).wait_send()
    for n in range(8):
        to_side(0, n).wait_send()
        w_copy(n).wait_send()
        tok_copy(n).wait_send()
    for n in range(16):
        src, dst, send, recv, to, mine = deliver(n)

        @pl.when(jnp.logical_not(mine))
        def _():
            remote(src, dst, send, recv, to).wait_send()

    for w in range(2):
        for k in range(2):
            ff_first(w, k).wait_send()
            ff_half(w, k).wait_send()
            for row in range(4):
                ff_column(w, row, k).wait_send()
            for n in range(2):
                ff_onward(w, n, k).wait_send()
    for k in range(4):
        to_sibling(k).wait_send()
    for k in range(1, 4):
        to_owner(k).wait_send()


def attention(q, kv, prm, w, up, down, residual, gains):
    dma = pltpu.SemaphoreType.DMA
    vmem = pl.BlockSpec(memory_space=pltpu.VMEM)
    return pl.pallas_call(
        attention_kernel,
        out_shape=jax.ShapeDtypeStruct((OWN, 2048), BF16),
        in_specs=[vmem] * 8,
        out_specs=vmem,
        scratch_shapes=[
            pltpu.VMEM((2, SIZE, 2 * TOK), BF16),
            pltpu.VMEM((16, SLAB, 256), BF16),
            pltpu.VMEM((2, 8, 128), F32),
            pltpu.VMEM((8, 256, 2048), BF16),
            pltpu.VMEM((TOK, TILE), F32),
            pltpu.VMEM((TOK, TILE), F32),
            pltpu.VMEM((TILES, 2, 1, TILE), F32),
            pltpu.VMEM((TILES, 2, ROWS, TILE), F32),
            pltpu.VMEM((2 * TOK, VALUE), BF16),
            pltpu.VMEM((16, OWN, VALUE), BF16),
            dma((2,)), dma((2,)), dma((2,)), dma((3,)), dma((3,)), dma((8,)), dma((16,)), dma((8,)),
            dma((2,)), dma((16,)), dma((2,)), dma((16,)), dma((8,)), dma((2,)), dma(()),
            pltpu.VMEM((2048, 1024), BF16),
            pltpu.VMEM((1024, 2048), BF16),
            pltpu.VMEM((8, OWN, 2048), BF16),
            pltpu.VMEM((OWN, 2048), F32),
            pltpu.VMEM((2 * OWN, 1024), BF16),
            pltpu.VMEM((4, OWN, 2048), F32),
            pltpu.VMEM((4, OWN, 2048), BF16),
            pltpu.VMEM((4, OWN, 2048), BF16),
            pltpu.VMEM((3, OWN, 2048), BF16),
            pltpu.VMEM((3, OWN, 2048), BF16),
            dma((32,)), dma((16,)), dma((16,)), dma((4,)), dma((2,)), dma((8,)), dma((8,)), dma((2,)), dma((4,)), dma((4,)),
            dma((3,)), dma((3,)),
        ],
        compiler_params=pltpu.CompilerParams(collective_id=0, has_side_effects=True, vmem_limit_bytes=63 << 20),
        cost_estimate=pl.CostEstimate(flops=4 * 768 * 12288 * 4 * 128, bytes_accessed=4 << 20, transcendentals=4 * 768 * 12288),
        name="attention",
    )(q, kv, prm, w, up, down, residual, gains)


def layer_norm(activations, scales):
    average = jnp.mean(activations, axis=-1, keepdims=True)
    centred = activations - average
    spread = jnp.mean(centred * centred, axis=-1, keepdims=True)
    return centred * lax.rsqrt(spread + EPSILON) * scales


def kernel_operands(query_first, key_first, value_first, query_second, key_second, value_second, mix_lambda, head_gain):
    first = query_first[:, 0].astype(F32) * (LOG2E / 8.0)
    high = lax.reduce_precision(first, 8, 7)
    low = first - high
    second = query_second[:, 0].astype(F32) * (LOG2E / math.sqrt(128.0))
    q = jnp.stack([
        jnp.stack([jnp.concatenate([high[:, :64], low[:, :64]], 1), jnp.concatenate([high[:, 64:], low[:, 64:]], 1)]),
        jnp.stack([second[:, :128], second[:, 128:]]),
    ]).astype(BF16)
    q = jnp.swapaxes(q, 2, 3)
    one, two = key_first[:, 0, :64], key_first[:, 0, 64:]
    keys = jnp.stack([jnp.concatenate([one, one, two, two], 1), key_second[:, 0]])
    values = jnp.stack([value_first[:, 0], value_second[:, 0]])
    values = jnp.swapaxes(values.reshape(2, 3, 256, VALUE), 2, 3).reshape(2, 3 * VALUE, 256)
    kv = jnp.concatenate([keys, values], axis=1)
    prm = jnp.concatenate([head_gain, jnp.broadcast_to(mix_lambda[:, :, None], (2, 1, 128)), jnp.zeros((2, 6, 128), F32)], axis=1)
    return q, kv, prm


def local(query_first, key_first, value_first, query_second, key_second, value_second, mix_lambda, head_gain, out_weight,
          residual, norm_gain, up_weight, down_weight):
    q, kv, prm = kernel_operands(query_first, key_first, value_first, query_second, key_second, value_second, mix_lambda, head_gain)
    return attention(q, kv, prm, out_weight.reshape(2 * VALUE, -1), up_weight, down_weight, residual, norm_gain)


def solution(mesh):
    heads = P("sp", "tp", None)
    return jax.shard_map(
        local,
        mesh=mesh,
        in_specs=(heads, heads, heads, heads, heads, heads, P(None, "tp"), P(None, "tp", None), P(None, "tp", None, None),
                  P(("sp", "tp"), None), P(), P("sp", "tp"), P("tp", "sp")),
        out_specs=P(("sp", "tp"), None),
        check_vma=False,
    )
```

```python
import functools
import math

import jax
import jax.numpy as jnp
from jax import lax
from jax.experimental import pallas as pl
from jax.experimental.pallas import tpu as pltpu
from jax.sharding import PartitionSpec as P

EPSILON = 1e-05
LOWEST = -1e30
LOG2E = math.log2(math.e)
MESH = pl.DeviceIdType.MESH
BF16 = jnp.bfloat16
F32 = jnp.float32

TOK = 768
OWN = 96
SIZE = 128
VALUE = 128
HALF = TOK // 2
KEYS = VALUE * TOK // 256
SLAB = KEYS + TOK
LENGTHS = (KEYS + HALF, SLAB)
TILE = 512
TILES = 2 * TOK // TILE
ROWS = VALUE + 16


def attention_kernel(q1_ref, k1_ref, v1_ref, q2_ref, k2_ref, v2_ref, mix_ref, head_gain_ref, w_ref, up_ref, down_ref, residual_hbm,
                     gain_ref, out_ref, q_own, kv_own, prm_own, residual_ref, residual_sem, q_all, kv_all, prm_all, w_all, s0, s1, top, acc, heads, got,
                     q_send, kv_send, prm_send, right_send, left_send, side_send, head_send, w_send,
                     q_recv, kv_recv, prm_recv, head_recv, w_recv, w_far, w_own,
                     up_all, down_all, tokens, normed, hidden, keep, to_sib, from_sib, to_chip, from_chip,
                     ff_send, up_recv, down_recv, rest_recv, ff_far, ff_own, tok_send, tok_recv, tok_far, sib_send, sib_recv,
                     chip_send, chip_recv):
    sp, tp = lax.axis_index("sp"), lax.axis_index("tp")
    z, y = lax.div(sp, 4), lax.rem(sp, 4)
    x, c = lax.div(tp, 2), lax.rem(tp, 2)

    def at(z_, y_, x_, c_):
        return {"sp": z_ * 4 + y_, "tp": x_ * 2 + c_}

    above, below = lax.rem(z + 1, 4), lax.rem(z + 3, 4)
    far = lax.rem(z + 2, 4)
    right, left, side = at(above, y, x, c), at(below, y, x, c), at(z, y, x, 1 - c)

    barrier = pltpu.get_barrier_semaphore()

    def greet(i, carry):
        other = lax.rem(y * 8 + tp + i, 32)
        pl.semaphore_signal(barrier, inc=1, device_id={"sp": z * 4 + lax.div(other, 8), "tp": lax.rem(other, 8)},
                            device_id_type=MESH)
        return carry

    lax.fori_loop(1, 32, greet, 0)
    pl.semaphore_signal(barrier, inc=1, device_id=right, device_id_type=MESH)
    pl.semaphore_signal(barrier, inc=1, device_id=left, device_id_type=MESH)
    residual_copy = pltpu.make_async_copy(residual_hbm, residual_ref, residual_sem)
    residual_copy.start()

    q_own[0, 0] = (q1_ref[...].astype(F32) * (LOG2E / 8.0)).T.astype(BF16)
    for m in range(2):
        q_own[1, m] = (q2_ref[:, m * SIZE : (m + 1) * SIZE].astype(F32) * (LOG2E / math.sqrt(128.0))).T.astype(BF16)
    for g, values in ((0, v1_ref), (1, v2_ref)):
        for b in range(TOK // 256):
            kv_own[g, b * VALUE : (b + 1) * VALUE] = values[b * 256 : (b + 1) * 256].astype(F32).T.astype(BF16)
        prm_own[g, 0:1] = head_gain_ref[g : g + 1]
        prm_own[g, 1:2] = jnp.broadcast_to(mix_ref[g : g + 1], (1, 128))
    for h in range(2):
        kv_own[0, KEYS : KEYS + HALF, h * SIZE : (h + 1) * SIZE] = k1_ref[h * HALF : (h + 1) * HALF]
    kv_own[1, KEYS:SLAB] = k2_ref[...]
    pl.semaphore_wait(barrier, 33)

    def remote(src, dst, send, recv, device):
        return pltpu.make_async_remote_copy(src_ref=src, dst_ref=dst, send_sem=send, recv_sem=recv, device_id=device,
                                            device_id_type=MESH)

    half, odd = lax.div(y, 2), lax.rem(y, 2)
    home = c == half

    def q_views(g, j):
        lanes = pl.ds(j * TOK if isinstance(j, int) else pl.multiple_of(j * TOK, TOK), TOK)
        return (q_own.at[0, 0], q_all.at[0, :, lanes]) if g == 0 else (q_own.at[1], q_all.at[:, :, lanes])

    def slab(slot, g):
        return kv_all.at[slot, pl.ds(0, LENGTHS[g])]

    def spread(g):
        to = at(z, 2 * c + g, x, half)
        return (
            (*q_views(g, odd), q_send.at[g], q_recv.at[odd], to),
            (prm_own.at[g], prm_all.at[odd], prm_send.at[g], prm_recv.at[odd], to),
            (kv_own.at[g, pl.ds(0, LENGTHS[g])], slab(z * 4 + y, g), kv_send.at[g], kv_recv.at[z * 4 + y], to),
        )

    def away(part, g):
        src, dst, send, recv, to = spread(g)[part]

        @pl.when(jnp.logical_not(2 * c + g == y))
        def _():
            remote(src, dst, send, recv, to).start()

    for part in range(2):
        for g in range(2):
            away(part, g)
    def near_or_far(far_ones):
        for g in range(2):
            @pl.when(odd == (g if far_ones else 1 - g))
            def _():
                away(2, g)

    near_or_far(False)

    def place(kind):
        return (y, y + 1 - 2 * odd, 3 - y, lax.rem(y + 2, 4))[kind]

    rows = (z, below, above, far)

    def by_group(action):
        for g in range(2):
            @pl.when(odd == g)
            def _():
                action(g)

    def arrive_of(slot, g):
        remote(slab(slot, g), slab(slot, g), kv_send.at[0], kv_recv.at[slot], side).wait_recv()

    def arrive(slot):
        by_group(lambda g: arrive_of(slot, g))

    def to_side(slot, n, g):
        return remote(slab(slot, g), slab(slot, g), side_send.at[n], kv_recv.at[slot], side)

    def to_right(slot, n, g):
        return remote(slab(slot, g), slab(slot, g), right_send.at[n], kv_recv.at[slot], right)

    def to_left(slot, n, g):
        return remote(slab(slot, g), slab(slot, g), left_send.at[n], kv_recv.at[slot], left)

    def own_shard(g):
        slot = z * 4 + y
        for sends, to in ((right_send, right), (left_send, left), (side_send, side)):
            remote(kv_own.at[g, pl.ds(0, LENGTHS[g])], slab(slot, g), sends.at[0], kv_recv.at[slot], to).start()
        lanes = pl.ds(pl.multiple_of(odd * TOK, TOK), TOK)
        kv_all[slot, 0 : LENGTHS[g]] = kv_own[g, 0 : LENGTHS[g]]
        for m in range(1 + g):
            q_all[m, :, lanes] = q_own[g, m]
        prm_all[odd] = prm_own[g]

    def pass_on(kind, row):
        slot = rows[row] * 4 + place(kind)
        second = kind % 2

        def relay(g):
            arrive_of(slot, g)
            if row == 0:
                to_right(slot, second, g).start()
                to_left(slot, second, g).start()
            elif row == 1 and not second:
                to_right(slot, 2, g).start()
            elif row == 2 and second:
                to_left(slot, 2, g).start()
            to_side(slot, second * 4 + row, g).start()

        by_group(relay)

    east, west = at(z, y, lax.rem(x + 1, 4), c), at(z, y, lax.rem(x + 3, 4), c)
    head_here, head_east = 2 * x + c, 2 * lax.rem(x + 1, 4) + c
    head_west, head_far = 2 * lax.rem(x + 3, 4) + c, 2 * lax.rem(x + 2, 4) + c

    def w_copy(n):
        full = lambda h: w_all.at[h]
        part = lambda h, k: w_all.at[h, pl.ds(k * 128, 128)]
        return (
            lambda: remote(w_ref, full(head_here), w_send.at[0], w_recv.at[head_here], east),
            lambda: remote(w_ref, full(head_here), w_send.at[1], w_recv.at[head_here], west),
            lambda: remote(w_ref, full(head_here), w_send.at[2], w_recv.at[head_here], side),
            lambda: remote(part(head_west, 0), part(head_west, 0), w_send.at[3], w_far.at[0], east),
            lambda: remote(part(head_east, 1), part(head_east, 1), w_send.at[4], w_far.at[1], west),
            lambda: remote(full(head_west), full(head_west), w_send.at[5], w_recv.at[head_west], side),
            lambda: remote(full(head_east), full(head_east), w_send.at[6], w_recv.at[head_east], side),
            lambda: remote(full(head_far), full(head_far), w_send.at[7], w_recv.at[head_far], side),
        )[n]()

    def w_arrive(h):
        remote(w_all.at[h], w_all.at[h], w_send.at[0], w_recv.at[h], side).wait_recv()

    forth, back = at(z, lax.rem(y + 1, 4), x, c), at(z, lax.rem(y + 3, 4), x, c)
    y_forth, y_back, y_far = lax.rem(y + 1, 4), lax.rem(y + 3, 4), lax.rem(y + 2, 4)
    UP, DOWN_A, DOWN_B = 0, 1, 2

    def source(p):
        return up_ref if p == UP else down_ref.at[pl.ds(512 * (p - 1), 512)]

    def shard(p, s, k=None):
        if p == UP:
            if k is None:
                return up_all.at[pl.ds(pl.multiple_of(s * 128, 128), 128)]
            return up_all.at[pl.ds(pl.multiple_of(s * 128 + k * 64, 64), 64)]
        lanes = pl.ds(pl.multiple_of(s * 128, 128), 128)
        start = 512 * (p - 1)
        return down_all.at[pl.ds(start, 512) if k is None else pl.ds(start + k * 256, 256), lanes]

    def lines(p):
        by_z = ((right, left), (below * 4 + y, above * 4 + y, far * 4 + y), lambda r: r * 4 + y, lambda r: r * 4 + y_back,
                lambda r: r * 4 + y_forth, lambda r: r * 4 + y_far)
        by_y = ((forth, back), (z * 4 + y_back, z * 4 + y_forth, z * 4 + y_far), lambda r: z * 4 + r, lambda r: below * 4 + r,
                lambda r: above * 4 + r, lambda r: far * 4 + r)
        return by_y + ((right, left),) if p == UP else by_z + ((forth, back),)

    ff_recv = (up_recv, down_recv, rest_recv)

    def piece(p, n, s, to, k=None, recv=None):
        view = shard(p, s, k)
        return remote(view, view, ff_send.at[16 * p + n], ff_recv[p].at[s] if recv is None else recv, to)

    def ff_first(p, k):
        return remote(source(p), shard(p, sp), ff_send.at[16 * p + k], ff_recv[p].at[sp], lines(p)[0][k])

    def ff_half(p, k):
        return piece(p, 2 + k, lines(p)[1][k], lines(p)[0][k], k, ff_far.at[2 * p + k])

    def ff_column(p, r, k):
        return piece(p, 4 + 2 * r + k, lines(p)[2](r), lines(p)[6][k])

    def ff_onward(p, n, k):
        return piece(p, 12 + 2 * n + k, lines(p)[3 + k](n + 2 * k), lines(p)[6][k])

    def ff_arrive(p, s):
        piece(p, 0, s, side).wait_recv()

    def begin(p):
        pltpu.make_async_copy(source(p), shard(p, sp), ff_own.at[p]).start()
        for k in range(2):
            ff_first(p, k).start()

    def halves(p):
        for k in range(2):
            ff_arrive(p, lines(p)[1][k])
            ff_half(p, k).start()

    def gathered(p):
        for k in range(2):
            piece(p, 0, lines(p)[1][2], side, k, ff_far.at[2 * p + k]).wait_recv()
        pltpu.make_async_copy(source(p), shard(p, sp), ff_own.at[p]).wait()

    def columns(p, second):
        for n in range(2):
            for k in range(2):
                ff_column(p, (n + 2 - 2 * k) if second else (n + 2 * k), k).start()

    def onward(p):
        for n in range(2):
            for k in range(2):
                ff_arrive(p, lines(p)[3 + k](n + 2 * k))
                ff_onward(p, n, k).start()

    def complete(p):
        for n in range(2):
            for k in range(2):
                ff_arrive(p, lines(p)[3 + k](n + 2 - 2 * k))
        for r in range(4):
            ff_arrive(p, lines(p)[5](r))


    @pl.when(home)
    def _():
        by_group(own_shard)

    begin(DOWN_A)
    begin(DOWN_B)

    @pl.when(home)
    def _():
        pass_on(0, 1)
        pass_on(0, 2)


    kinds = (0, 0, 0, 0, 1, 2, 1, 1, 2, 2, 3, 1, 2, 3, 3, 3)
    order = (0, 1, 2, 3, 0, 0, 1, 2, 1, 2, 0, 3, 3, 1, 2, 3)
    home_duties = {0: ((1, 0),), 1: ((0, 3),), 5: ((1, 1), (1, 2)), 8: ((1, 3),)}
    away_duties = {1: ((2, 0),), 4: ((3, 0),), 5: ((2, 1), (2, 2)), 7: ((2, 3),), 9: ((3, 1), (3, 2)), 12: ((3, 3),)}

    def pick(i, table):
        value = jnp.int32(table[0])
        for n in range(1, 16):
            if table[n] != table[n - 1]:
                value = jnp.where(i >= n, table[n], value)
        return value

    def slot_of(i):
        kind, row = pick(i, kinds), pick(i, order)
        row = jnp.where(row == 0, z, jnp.where(row == 1, below, jnp.where(row == 2, above, far)))
        spot = jnp.where(kind == 0, y, jnp.where(kind == 1, y + 1 - 2 * odd, jnp.where(kind == 2, 3 - y, lax.rem(y + 2, 4))))
        return row * 4 + spot

    def duty(i):
        for n in range(16):
            for mine, duties in ((home, home_duties), (jnp.logical_not(home), away_duties)):
                if n in duties:
                    @pl.when(jnp.logical_and(i == n, mine))
                    def _():
                        for kind, row in duties[n]:
                            pass_on(kind, row)
        kind = pick(i + 1, kinds)

        @pl.when(jnp.logical_and(i < 15, jnp.logical_not(home) == (kind < 2)))
        def _():
            arrive(slot_of(i + 1))

        @pl.when(i == 0)
        def _():
            near_or_far(True)
            begin(UP)
            for n in range(3):
                w_copy(n).start()
            pltpu.make_async_copy(w_ref, w_all.at[head_here], w_own).start()

        @pl.when(i == 3)
        def _():
            halves(DOWN_A)
            halves(DOWN_B)
            halves(UP)

        @pl.when(i == 5)
        def _():
            gathered(DOWN_A)
            columns(DOWN_A, False)
            columns(DOWN_A, True)

        @pl.when(i == 6)
        def _():
            gathered(DOWN_B)
            columns(DOWN_B, False)
            columns(DOWN_B, True)

        @pl.when(i == 9)
        def _():
            gathered(UP)
            columns(UP, False)
            columns(UP, True)

        @pl.when(i == 10)
        def _():
            onward(DOWN_A)
            onward(DOWN_B)

        @pl.when(i == 8)
        def _():
            w_arrive(head_west)
            w_copy(3).start()
            w_arrive(head_east)
            w_copy(4).start()
            w_copy(5).start()
            w_copy(6).start()

        @pl.when(i == 12)
        def _():
            for k in range(2):
                remote(w_all.at[0, pl.ds(0, 128)], w_all.at[head_far, pl.ds(k * 128, 128)], w_send.at[0], w_far.at[k],
                       side).wait_recv()
            w_copy(7).start()

    for j in range(2):
        @pl.when(jnp.logical_not(jnp.logical_and(home, odd == j)))
        def _():
            by_group(lambda g: remote(*q_views(g, j), q_send.at[0], q_recv.at[j], side).wait_recv())
            remote(prm_own.at[0], prm_all.at[j], prm_send.at[0], prm_recv.at[j], side).wait_recv()

    @pl.when(odd == 0)
    def _():
        both = q_all[0]
        nothing = jnp.zeros((SIZE // 2, 2 * TOK), BF16)
        q_all[1, 0 : SIZE // 2] = nothing
        q_all[1, SIZE // 2 : SIZE] = both[SIZE // 2 : SIZE]
        q_all[0, SIZE // 2 : SIZE] = nothing

    top[...] = jnp.full(top.shape, LOWEST, F32)
    acc[...] = jnp.zeros(acc.shape, F32)
    ones = jnp.ones((ROWS - VALUE, 256), BF16)

    def scores(slot, tile, m, held):
        queries = q_all[m, :, pl.ds(pl.multiple_of(tile * TILE, TILE), TILE)]
        peak = None
        for h in range(2):
            start = KEYS + (odd * HALF if h else 0)
            entry = m * SIZE if h == m else (odd if m else 1 - odd) * SIZE
            keys = kv_all[slot, pl.ds(pl.multiple_of(start, HALF), HALF), pl.ds(pl.multiple_of(entry, SIZE), SIZE)]
            s = jnp.dot(keys, queries, preferred_element_type=F32)
            held[h * HALF : (h + 1) * HALF] = s
            p = jnp.max(s, axis=0, keepdims=True)
            peak = p if peak is None else jnp.maximum(peak, p)
        return peak

    def absorb(slot, tile, m, held, peak):
        old = top[tile, m]
        new = jnp.maximum(old, peak)
        top[tile, m] = new
        weights = jnp.exp2(held[...] - new).astype(BF16)
        added = None
        for b in range(TOK // 256):
            values = kv_all[slot, b * VALUE : (b + 1) * VALUE, :]
            d = jnp.dot(jnp.concatenate([values, ones], axis=0), weights[b * 256 : (b + 1) * 256],
                        preferred_element_type=F32)
            added = d if added is None else added + d
        acc[tile, m] = acc[tile, m] * jnp.exp2(old - new) + added

    @pl.when(jnp.logical_not(home))
    def _():
        arrive(slot_of(jnp.int32(0)))

    peak = scores(slot_of(jnp.int32(0)), 0, 0, s0)

    def step(t, peak0):
        i, tile = lax.div(t, TILES), lax.rem(t, TILES)
        slot = slot_of(i)

        @pl.when(tile == TILES - 1)
        def _():
            duty(i)

        peak1 = scores(slot, tile, 1, s1)
        absorb(slot, tile, 0, s0, peak0)
        later = jnp.minimum(t + 1, 16 * TILES - 1)
        peak0 = scores(slot_of(lax.div(later, TILES)), lax.rem(later, TILES), 0, s0)
        absorb(slot, tile, 1, s1, peak1)
        return peak0

    lax.fori_loop(0, 16 * TILES, step, peak)

    gain = prm_all[0, 0:1, :]
    mix = prm_all[0, 1:2, 0:1]
    for tile in range(TILES):
        a1, a2 = acc[tile, 0], acc[tile, 1]
        attended = a1[:VALUE] / a1[VALUE : VALUE + 1] - mix * (a2[:VALUE] / a2[VALUE : VALUE + 1])
        square = jnp.mean(attended * attended, axis=0, keepdims=True)
        scaled = attended * lax.rsqrt(square + EPSILON)
        heads[tile * TILE : (tile + 1) * TILE, :] = (scaled.T * gain).astype(BF16)

    unit = (2 * x + lax.div(y, 2)) * 2 + lax.rem(y, 2)

    def deliver(n):
        j, tp_ = n // 8, n % 8
        to = {"sp": z * 4 + 2 * c + j, "tp": jnp.int32(tp_)}
        mine = jnp.logical_and(2 * c + j == y, tp == tp_)
        return heads.at[pl.ds(n * OWN, OWN)], got.at[unit], head_send.at[n], head_recv.at[unit], to, mine

    for n in range(16):
        src, dst, send, recv, to, mine = deliver(n)

        @pl.when(mine)
        def _():
            pltpu.make_async_copy(src, dst, recv).start()

        @pl.when(jnp.logical_not(mine))
        def _():
            remote(src, dst, send, recv, to).start()

    onward(UP)
    for n in range(4):
        w_arrive(2 * n + 1 - c)
    pltpu.make_async_copy(w_ref, w_all.at[head_here], w_own).wait()
    for n in range(16):
        remote(got.at[n], got.at[n], head_send.at[n], head_recv.at[n], side).wait_recv()

    residual_copy.wait()

    def project(n, carry):
        columns = pl.ds(pl.multiple_of(n * 512, 512), 512)
        total = residual_ref[:, columns].astype(F32)
        for h in range(8):
            pair = jnp.concatenate([got[2 * h], got[2 * h + 1]], axis=1)
            total = total + jnp.dot(pair, w_all[h, :, columns], preferred_element_type=F32)
        normed[:, columns] = total
        return carry

    lax.fori_loop(0, 4, project, 0)
    for r in range(0, OWN, 32):
        value = layer_norm(normed[r : r + 32], gain_ref[0:1])
        normed[r : r + 32] = value
        tokens[tp, r : r + 32] = value.astype(BF16)

    def tok_copy(n):
        t_west, t_east, t_far = 2 * lax.rem(x + 3, 4) + c, 2 * lax.rem(x + 1, 4) + c, 2 * lax.rem(x + 2, 4) + c
        half_of = lambda t, k: tokens.at[t, pl.ds(k * 48, 48)]
        return (
            lambda: remote(tokens.at[tp], tokens.at[tp], tok_send.at[0], tok_recv.at[tp], east),
            lambda: remote(tokens.at[tp], tokens.at[tp], tok_send.at[1], tok_recv.at[tp], west),
            lambda: remote(tokens.at[tp], tokens.at[tp], tok_send.at[2], tok_recv.at[tp], side),
            lambda: remote(half_of(t_west, 0), half_of(t_west, 0), tok_send.at[3], tok_far.at[0], east),
            lambda: remote(half_of(t_east, 1), half_of(t_east, 1), tok_send.at[4], tok_far.at[1], west),
            lambda: remote(tokens.at[t_west], tokens.at[t_west], tok_send.at[5], tok_recv.at[t_west], side),
            lambda: remote(tokens.at[t_east], tokens.at[t_east], tok_send.at[6], tok_recv.at[t_east], side),
            lambda: remote(tokens.at[t_far], tokens.at[t_far], tok_send.at[7], tok_recv.at[t_far], side),
        )[n]()

    def tok_arrive(t):
        remote(tokens.at[t], tokens.at[t], tok_send.at[0], tok_recv.at[t], side).wait_recv()

    for n in range(3):
        tok_copy(n).start()
    complete(UP)

    chips = (x, lax.rem(x + 3, 4), lax.rem(x + 1, 4), lax.rem(x + 2, 4))

    def feed(k):
        chip = chips[k]
        rows_in = (2 * chip + c, 2 * chip + 1 - c)

        def up(n, carry):
            columns = pl.ds(pl.multiple_of(n * 512, 512), 512)
            block = jnp.concatenate([tokens[rows_in[0]], tokens[rows_in[1]]], axis=0)
            e = jnp.maximum(jnp.dot(block, up_all[:, columns], preferred_element_type=F32), 0.0)
            hidden[:, columns] = (e * e).astype(BF16)
            return carry

        lax.fori_loop(0, 2, up, 0)
        if k == 0:
            complete(DOWN_A)
            complete(DOWN_B)

        def down(n, carry):
            columns = pl.ds(pl.multiple_of(n * 512, 512), 512)
            p = jnp.dot(hidden[...], down_all[:, columns], preferred_element_type=F32)
            keep[k, :, columns] = p[:OWN]
            to_sib[k, :, columns] = p[OWN:].astype(BF16)
            return carry

        lax.fori_loop(0, 4, down, 0)

    def to_sibling(k):
        return remote(to_sib.at[k], from_sib.at[k], sib_send.at[k], sib_recv.at[k], side)

    def to_owner(k):
        return remote(to_chip.at[k - 1], from_chip.at[k - 1], chip_send.at[k - 1], chip_recv.at[k - 1], (None, west, east, at(z, y, lax.rem(x + 2, 4), c))[k])

    def chip_sum(k):
        to_sibling(k).wait_recv()
        for r in range(0, OWN, 32):
            to_chip[k - 1, r : r + 32] = (keep[k, r : r + 32] + from_sib[k, r : r + 32].astype(F32)).astype(BF16)
        to_owner(k).start()

    tok_arrive(2 * x + 1 - c)
    feed(0)
    to_sibling(0).start()
    west_tok, east_tok, far_tok = (2 * chips[k] + c for k in (1, 2, 3))
    tok_arrive(west_tok)
    tok_copy(3).start()
    tok_copy(5).start()
    tok_arrive(east_tok)
    tok_copy(4).start()
    tok_copy(6).start()
    tok_arrive(2 * chips[1] + 1 - c)
    feed(1)
    to_sibling(1).start()
    tok_arrive(2 * chips[2] + 1 - c)
    feed(2)
    to_sibling(2).start()
    chip_sum(1)
    for k in range(2):
        spot = tokens.at[far_tok, pl.ds(k * 48, 48)]
        remote(spot, spot, tok_send.at[0], tok_far.at[k], side).wait_recv()
    tok_copy(7).start()
    chip_sum(2)
    tok_arrive(2 * chips[3] + 1 - c)
    feed(3)
    to_sibling(3).start()
    chip_sum(3)
    to_sibling(0).wait_recv()
    for k in range(1, 4):
        to_owner(k).wait_recv()
    for r in range(0, OWN, 32):
        span = slice(r, r + 32)
        total = normed[span] + keep[0, span] + from_sib[0, span].astype(F32)
        for k in range(3):
            total = total + from_chip[k, span].astype(F32)
        out_ref[span] = layer_norm(total, gain_ref[1:2]).astype(BF16)

    for part in range(3):
        for g in range(2):
            src, dst, send, recv, to = spread(g)[part]

            @pl.when(jnp.logical_not(2 * c + g == y))
            def _():
                remote(src, dst, send, recv, to).wait_send()

    def sent(g):
        for n in range(3):
            to_right(0, n, g).wait_send()
            to_left(0, n, g).wait_send()
        for n in range(8):
            to_side(0, n, g).wait_send()

    by_group(sent)
    for n in range(8):
        w_copy(n).wait_send()
        tok_copy(n).wait_send()
    for n in range(16):
        src, dst, send, recv, to, mine = deliver(n)

        @pl.when(jnp.logical_not(mine))
        def _():
            remote(src, dst, send, recv, to).wait_send()

    for w in range(3):
        for k in range(2):
            ff_first(w, k).wait_send()
            ff_half(w, k).wait_send()
            for row in range(4):
                ff_column(w, row, k).wait_send()
            for n in range(2):
                ff_onward(w, n, k).wait_send()
    for k in range(4):
        to_sibling(k).wait_send()
    for k in range(1, 4):
        to_owner(k).wait_send()


def layer(*operands):
    dma = pltpu.SemaphoreType.DMA
    vmem, hbm = pl.BlockSpec(memory_space=pltpu.VMEM), pl.BlockSpec(memory_space=pl.ANY)
    return pl.pallas_call(
        attention_kernel,
        out_shape=jax.ShapeDtypeStruct((OWN, 2048), BF16),
        in_specs=[vmem] * 8 + [hbm] * 4 + [vmem],
        out_specs=vmem,
        scratch_shapes=[
            pltpu.VMEM((2, 2, SIZE, TOK), BF16),
            pltpu.VMEM((2, SLAB, 256), BF16),
            pltpu.VMEM((2, 8, 128), F32),
            pltpu.VMEM((OWN, 2048), BF16),
            dma(()),
            pltpu.VMEM((2, SIZE, 2 * TOK), BF16),
            pltpu.VMEM((16, SLAB, 256), BF16),
            pltpu.VMEM((2, 8, 128), F32),
            pltpu.VMEM((8, 256, 2048), BF16),
            pltpu.VMEM((TOK, TILE), F32),
            pltpu.VMEM((TOK, TILE), F32),
            pltpu.VMEM((TILES, 2, 1, TILE), F32),
            pltpu.VMEM((TILES, 2, ROWS, TILE), F32),
            pltpu.VMEM((2 * TOK, VALUE), BF16),
            pltpu.VMEM((16, OWN, VALUE), BF16),
            dma((2,)), dma((2,)), dma((2,)), dma((3,)), dma((3,)), dma((8,)), dma((16,)), dma((8,)),
            dma((2,)), dma((16,)), dma((2,)), dma((16,)), dma((8,)), dma((2,)), dma(()),
            pltpu.VMEM((2048, 1024), BF16),
            pltpu.VMEM((1024, 2048), BF16),
            pltpu.VMEM((8, OWN, 2048), BF16),
            pltpu.VMEM((OWN, 2048), F32),
            pltpu.VMEM((2 * OWN, 1024), BF16),
            pltpu.VMEM((4, OWN, 2048), F32),
            pltpu.VMEM((4, OWN, 2048), BF16),
            pltpu.VMEM((4, OWN, 2048), BF16),
            pltpu.VMEM((3, OWN, 2048), BF16),
            pltpu.VMEM((3, OWN, 2048), BF16),
            dma((48,)), dma((16,)), dma((16,)), dma((16,)), dma((6,)), dma((3,)), dma((8,)), dma((8,)), dma((2,)), dma((4,)), dma((4,)),
            dma((3,)), dma((3,)),
        ],
        compiler_params=pltpu.CompilerParams(collective_id=0, has_side_effects=True, vmem_limit_bytes=63 << 20),
        cost_estimate=pl.CostEstimate(flops=4 * 768 * 12288 * 4 * 128, bytes_accessed=4 << 20, transcendentals=4 * 768 * 12288),
        name="attention",
    )(*operands)


def layer_norm(activations, scales):
    average = jnp.mean(activations, axis=-1, keepdims=True)
    centred = activations - average
    spread = jnp.mean(centred * centred, axis=-1, keepdims=True)
    return centred * lax.rsqrt(spread + EPSILON) * scales


def local(query_first, key_first, value_first, query_second, key_second, value_second, mix_lambda, head_gain, out_weight,
          residual, norm_gain, up_weight, down_weight):
    return layer(query_first[:, 0], key_first[:, 0], value_first[:, 0], query_second[:, 0], key_second[:, 0], value_second[:, 0],
                 mix_lambda, head_gain[:, 0], out_weight.reshape(2 * VALUE, -1), up_weight, down_weight, residual, norm_gain)


def solution(mesh):
    heads = P("sp", "tp", None)
    return jax.shard_map(
        local,
        mesh=mesh,
        in_specs=(heads, heads, heads, heads, heads, heads, P(None, "tp"), P(None, "tp", None), P(None, "tp", None, None),
                  P(("sp", "tp"), None), P(), P("sp", "tp"), P("tp", "sp")),
        out_specs=P(("sp", "tp"), None),
        check_vma=False,
    )
```

```python
import functools
import math

import jax
import jax.numpy as jnp
from jax import lax
from jax.experimental import pallas as pl
from jax.experimental.pallas import tpu as pltpu
from jax.sharding import PartitionSpec as P

EPSILON = 1e-05
LOWEST = -1e30
LOG2E = math.log2(math.e)
MESH = pl.DeviceIdType.MESH
BF16 = jnp.bfloat16
F32 = jnp.float32

TOK = 768
OWN = 96
SIZE = 128
VALUE = 128
HALF = TOK // 2
KEYS = VALUE * TOK // 256
SLAB = KEYS + TOK
LENGTHS = (KEYS + HALF, SLAB)
TILE = 512
TILES = 2 * TOK // TILE
ROWS = VALUE + 16


def attention_kernel(q1_ref, k1_ref, v1_ref, q2_ref, k2_ref, v2_ref, mix_ref, head_gain_ref, w_ref, up_ref, down_ref, residual_hbm,
                     gain_ref, out_ref, q_own, kv_own, prm_own, residual_ref, residual_sem, q_all, kv_all, prm_all, w_all, s0, s1, top, acc, heads, got,
                     q_send, kv_send, prm_send, right_send, left_send, side_send, head_send, w_send,
                     q_recv, kv_recv, prm_recv, head_recv, w_recv, w_far, w_own,
                     up_all, down_all, tokens, normed, hidden, keep, to_sib, from_sib, to_chip, from_chip,
                     ff_send, up_recv, down_recv, rest_recv, ff_far, ff_own, tok_send, tok_recv, tok_far, sib_send, sib_recv,
                     chip_send, chip_recv):
    sp, tp = lax.axis_index("sp"), lax.axis_index("tp")
    z, y = lax.div(sp, 4), lax.rem(sp, 4)
    x, c = lax.div(tp, 2), lax.rem(tp, 2)

    def at(z_, y_, x_, c_):
        return {"sp": z_ * 4 + y_, "tp": x_ * 2 + c_}

    above, below = lax.rem(z + 1, 4), lax.rem(z + 3, 4)
    far = lax.rem(z + 2, 4)
    right, left, side = at(above, y, x, c), at(below, y, x, c), at(z, y, x, 1 - c)

    barrier = pltpu.get_barrier_semaphore()

    def greet(i, carry):
        other = lax.rem(y * 8 + tp + i, 32)
        pl.semaphore_signal(barrier, inc=1, device_id={"sp": z * 4 + lax.div(other, 8), "tp": lax.rem(other, 8)},
                            device_id_type=MESH)
        return carry

    lax.fori_loop(1, 32, greet, 0)
    pl.semaphore_signal(barrier, inc=1, device_id=right, device_id_type=MESH)
    pl.semaphore_signal(barrier, inc=1, device_id=left, device_id_type=MESH)
    residual_copy = pltpu.make_async_copy(residual_hbm, residual_ref, residual_sem)
    residual_copy.start()

    q_own[0, 0] = (q1_ref[...].astype(F32) * (LOG2E / 8.0)).T.astype(BF16)
    for m in range(2):
        q_own[1, m] = (q2_ref[:, m * SIZE : (m + 1) * SIZE].astype(F32) * (LOG2E / math.sqrt(128.0))).T.astype(BF16)
    for g, values in ((0, v1_ref), (1, v2_ref)):
        for b in range(TOK // 256):
            kv_own[g, b * VALUE : (b + 1) * VALUE] = values[b * 256 : (b + 1) * 256].astype(F32).T.astype(BF16)
        prm_own[g, 0:1] = head_gain_ref[g : g + 1]
        prm_own[g, 1:2] = jnp.broadcast_to(mix_ref[g : g + 1], (1, 128))
    for h in range(2):
        kv_own[0, KEYS : KEYS + HALF, h * SIZE : (h + 1) * SIZE] = k1_ref[h * HALF : (h + 1) * HALF]
    kv_own[1, KEYS:SLAB] = k2_ref[...]
    pl.semaphore_wait(barrier, 33)

    def remote(src, dst, send, recv, device):
        return pltpu.make_async_remote_copy(src_ref=src, dst_ref=dst, send_sem=send, recv_sem=recv, device_id=device,
                                            device_id_type=MESH)

    half, odd = lax.div(y, 2), lax.rem(y, 2)
    home = c == half

    def q_views(g, j):
        lanes = pl.ds(j * TOK if isinstance(j, int) else pl.multiple_of(j * TOK, TOK), TOK)
        return (q_own.at[0, 0], q_all.at[0, :, lanes]) if g == 0 else (q_own.at[1], q_all.at[:, :, lanes])

    def slab(slot, g):
        return kv_all.at[slot, pl.ds(0, LENGTHS[g])]

    def spread(g):
        to = at(z, 2 * c + g, x, half)
        return (
            (*q_views(g, odd), q_send.at[g], q_recv.at[odd], to),
            (prm_own.at[g], prm_all.at[odd], prm_send.at[g], prm_recv.at[odd], to),
            (kv_own.at[g, pl.ds(0, LENGTHS[g])], slab(z * 4 + y, g), kv_send.at[g], kv_recv.at[z * 4 + y], to),
        )

    def away(part, g):
        src, dst, send, recv, to = spread(g)[part]

        @pl.when(jnp.logical_not(2 * c + g == y))
        def _():
            remote(src, dst, send, recv, to).start()

    for part in range(2):
        for g in range(2):
            away(part, g)
    def near_or_far(far_ones):
        for g in range(2):
            @pl.when(odd == (g if far_ones else 1 - g))
            def _():
                away(2, g)

    near_or_far(False)

    def place(kind):
        return (y, y + 1 - 2 * odd, 3 - y, lax.rem(y + 2, 4))[kind]

    rows = (z, below, above, far)

    def by_group(action):
        for g in range(2):
            @pl.when(odd == g)
            def _():
                action(g)

    def arrive_of(slot, g):
        remote(slab(slot, g), slab(slot, g), kv_send.at[0], kv_recv.at[slot], side).wait_recv()

    def arrive(slot):
        by_group(lambda g: arrive_of(slot, g))

    def to_side(slot, n, g):
        return remote(slab(slot, g), slab(slot, g), side_send.at[n], kv_recv.at[slot], side)

    def to_right(slot, n, g):
        return remote(slab(slot, g), slab(slot, g), right_send.at[n], kv_recv.at[slot], right)

    def to_left(slot, n, g):
        return remote(slab(slot, g), slab(slot, g), left_send.at[n], kv_recv.at[slot], left)

    def own_shard(g):
        slot = z * 4 + y
        for sends, to in ((right_send, right), (left_send, left), (side_send, side)):
            remote(kv_own.at[g, pl.ds(0, LENGTHS[g])], slab(slot, g), sends.at[0], kv_recv.at[slot], to).start()
        lanes = pl.ds(pl.multiple_of(odd * TOK, TOK), TOK)
        kv_all[slot, 0 : LENGTHS[g]] = kv_own[g, 0 : LENGTHS[g]]
        for m in range(1 + g):
            q_all[m, :, lanes] = q_own[g, m]
        prm_all[odd] = prm_own[g]

    def pass_on(kind, row):
        slot = rows[row] * 4 + place(kind)
        second = kind % 2

        def relay(g):
            arrive_of(slot, g)
            if row == 0:
                to_right(slot, second, g).start()
                to_left(slot, second, g).start()
            elif row == 1 and not second:
                to_right(slot, 2, g).start()
            elif row == 2 and second:
                to_left(slot, 2, g).start()
            to_side(slot, second * 4 + row, g).start()

        by_group(relay)

    east, west = at(z, y, lax.rem(x + 1, 4), c), at(z, y, lax.rem(x + 3, 4), c)
    head_here, head_east = 2 * x + c, 2 * lax.rem(x + 1, 4) + c
    head_west, head_far = 2 * lax.rem(x + 3, 4) + c, 2 * lax.rem(x + 2, 4) + c

    def w_copy(n):
        full = lambda h: w_all.at[h]
        part = lambda h, k: w_all.at[h, pl.ds(k * 128, 128)]
        return (
            lambda: remote(w_ref, full(head_here), w_send.at[0], w_recv.at[head_here], east),
            lambda: remote(w_ref, full(head_here), w_send.at[1], w_recv.at[head_here], west),
            lambda: remote(w_ref, full(head_here), w_send.at[2], w_recv.at[head_here], side),
            lambda: remote(part(head_west, 0), part(head_west, 0), w_send.at[3], w_far.at[0], east),
            lambda: remote(part(head_east, 1), part(head_east, 1), w_send.at[4], w_far.at[1], west),
            lambda: remote(full(head_west), full(head_west), w_send.at[5], w_recv.at[head_west], side),
            lambda: remote(full(head_east), full(head_east), w_send.at[6], w_recv.at[head_east], side),
            lambda: remote(full(head_far), full(head_far), w_send.at[7], w_recv.at[head_far], side),
        )[n]()

    def w_arrive(h):
        remote(w_all.at[h], w_all.at[h], w_send.at[0], w_recv.at[h], side).wait_recv()

    forth, back = at(z, lax.rem(y + 1, 4), x, c), at(z, lax.rem(y + 3, 4), x, c)
    y_forth, y_back, y_far = lax.rem(y + 1, 4), lax.rem(y + 3, 4), lax.rem(y + 2, 4)
    UP, DOWN_A, DOWN_B = 0, 1, 2

    def source(p):
        return up_ref if p == UP else down_ref.at[pl.ds(512 * (p - 1), 512)]

    def shard(p, s, k=None):
        if p == UP:
            if k is None:
                return up_all.at[pl.ds(pl.multiple_of(s * 128, 128), 128)]
            return up_all.at[pl.ds(pl.multiple_of(s * 128 + k * 64, 64), 64)]
        lanes = pl.ds(pl.multiple_of(s * 128, 128), 128)
        start = 512 * (p - 1)
        return down_all.at[pl.ds(start, 512) if k is None else pl.ds(start + k * 256, 256), lanes]

    def lines(p):
        by_z = ((right, left), (below * 4 + y, above * 4 + y, far * 4 + y), lambda r: r * 4 + y, lambda r: r * 4 + y_back,
                lambda r: r * 4 + y_forth, lambda r: r * 4 + y_far)
        by_y = ((forth, back), (z * 4 + y_back, z * 4 + y_forth, z * 4 + y_far), lambda r: z * 4 + r, lambda r: below * 4 + r,
                lambda r: above * 4 + r, lambda r: far * 4 + r)
        return by_y + ((right, left),) if p == UP else by_z + ((forth, back),)

    ff_recv = (up_recv, down_recv, rest_recv)

    def piece(p, n, s, to, k=None, recv=None):
        view = shard(p, s, k)
        return remote(view, view, ff_send.at[16 * p + n], ff_recv[p].at[s] if recv is None else recv, to)

    def ff_first(p, k):
        return remote(source(p), shard(p, sp), ff_send.at[16 * p + k], ff_recv[p].at[sp], lines(p)[0][k])

    def ff_half(p, k):
        return piece(p, 2 + k, lines(p)[1][k], lines(p)[0][k], k, ff_far.at[2 * p + k])

    def ff_column(p, r, k):
        return piece(p, 4 + 2 * r + k, lines(p)[2](r), lines(p)[6][k])

    def ff_onward(p, n, k):
        return piece(p, 12 + 2 * n + k, lines(p)[3 + k](n + 2 * k), lines(p)[6][k])

    def ff_arrive(p, s):
        piece(p, 0, s, side).wait_recv()

    def begin(p):
        pltpu.make_async_copy(source(p), shard(p, sp), ff_own.at[p]).start()
        for k in range(2):
            ff_first(p, k).start()

    def halves(p):
        for k in range(2):
            ff_arrive(p, lines(p)[1][k])
            ff_half(p, k).start()

    def gathered(p):
        for k in range(2):
            piece(p, 0, lines(p)[1][2], side, k, ff_far.at[2 * p + k]).wait_recv()
        pltpu.make_async_copy(source(p), shard(p, sp), ff_own.at[p]).wait()

    def columns(p, second):
        for n in range(2):
            for k in range(2):
                ff_column(p, (n + 2 - 2 * k) if second else (n + 2 * k), k).start()

    def onward(p):
        for n in range(2):
            for k in range(2):
                ff_arrive(p, lines(p)[3 + k](n + 2 * k))
                ff_onward(p, n, k).start()

    def complete(p):
        for n in range(2):
            for k in range(2):
                ff_arrive(p, lines(p)[3 + k](n + 2 - 2 * k))
        for r in range(4):
            ff_arrive(p, lines(p)[5](r))


    @pl.when(home)
    def _():
        by_group(own_shard)

    begin(DOWN_A)
    begin(DOWN_B)

    @pl.when(home)
    def _():
        pass_on(0, 1)
        pass_on(0, 2)


    kinds = (0, 0, 0, 0, 1, 2, 1, 1, 2, 2, 3, 1, 2, 3, 3, 3)
    order = (0, 1, 2, 3, 0, 0, 1, 2, 1, 2, 0, 3, 3, 1, 2, 3)
    home_duties = {0: ((1, 0),), 1: ((0, 3),), 5: ((1, 1), (1, 2)), 10: ((1, 3),)}
    away_duties = {1: ((2, 0),), 4: ((3, 0),), 5: ((2, 1), (2, 2)), 9: ((3, 1), (3, 2)), 10: ((2, 3),), 12: ((3, 3),)}

    def pick(i, table):
        value = jnp.int32(table[0])
        for n in range(1, 16):
            if table[n] != table[n - 1]:
                value = jnp.where(i >= n, table[n], value)
        return value

    def slot_of(i):
        kind, row = pick(i, kinds), pick(i, order)
        row = jnp.where(row == 0, z, jnp.where(row == 1, below, jnp.where(row == 2, above, far)))
        spot = jnp.where(kind == 0, y, jnp.where(kind == 1, y + 1 - 2 * odd, jnp.where(kind == 2, 3 - y, lax.rem(y + 2, 4))))
        return row * 4 + spot

    def duty(i):
        for n in range(16):
            for mine, duties in ((home, home_duties), (jnp.logical_not(home), away_duties)):
                if n in duties:
                    @pl.when(jnp.logical_and(i == n, mine))
                    def _():
                        for kind, row in duties[n]:
                            pass_on(kind, row)
        kind = pick(i + 1, kinds)

        @pl.when(jnp.logical_and(i < 15, jnp.logical_not(home) == (kind < 2)))
        def _():
            arrive(slot_of(i + 1))

        @pl.when(i == 0)
        def _():
            near_or_far(True)
            begin(UP)
            for n in range(3):
                w_copy(n).start()
            pltpu.make_async_copy(w_ref, w_all.at[head_here], w_own).start()

        @pl.when(i == 3)
        def _():
            halves(DOWN_A)
            halves(DOWN_B)
            halves(UP)

        @pl.when(i == 5)
        def _():
            gathered(DOWN_A)
            columns(DOWN_A, False)
            columns(DOWN_A, True)

        @pl.when(i == 6)
        def _():
            gathered(DOWN_B)
            columns(DOWN_B, False)
            columns(DOWN_B, True)

        @pl.when(i == 9)
        def _():
            gathered(UP)
            columns(UP, False)
            columns(UP, True)

        @pl.when(i == 10)
        def _():
            onward(DOWN_A)
            onward(DOWN_B)

        @pl.when(i == 8)
        def _():
            w_arrive(head_west)
            w_copy(3).start()
            w_arrive(head_east)
            w_copy(4).start()
            w_copy(5).start()
            w_copy(6).start()

        @pl.when(i == 12)
        def _():
            for k in range(2):
                remote(w_all.at[0, pl.ds(0, 128)], w_all.at[head_far, pl.ds(k * 128, 128)], w_send.at[0], w_far.at[k],
                       side).wait_recv()
            w_copy(7).start()

    for j in range(2):
        @pl.when(jnp.logical_not(jnp.logical_and(home, odd == j)))
        def _():
            by_group(lambda g: remote(*q_views(g, j), q_send.at[0], q_recv.at[j], side).wait_recv())
            remote(prm_own.at[0], prm_all.at[j], prm_send.at[0], prm_recv.at[j], side).wait_recv()

    @pl.when(odd == 0)
    def _():
        both = q_all[0]
        nothing = jnp.zeros((SIZE // 2, 2 * TOK), BF16)
        q_all[1, 0 : SIZE // 2] = nothing
        q_all[1, SIZE // 2 : SIZE] = both[SIZE // 2 : SIZE]
        q_all[0, SIZE // 2 : SIZE] = nothing

    top[...] = jnp.full(top.shape, LOWEST, F32)
    acc[...] = jnp.zeros(acc.shape, F32)
    ones = jnp.ones((ROWS - VALUE, 256), BF16)

    def scores(slot, tile, m, held):
        queries = q_all[m, :, pl.ds(pl.multiple_of(tile * TILE, TILE), TILE)]
        peak = None
        for h in range(2):
            start = KEYS + (odd * HALF if h else 0)
            entry = m * SIZE if h == m else (odd if m else 1 - odd) * SIZE
            keys = kv_all[slot, pl.ds(pl.multiple_of(start, HALF), HALF), pl.ds(pl.multiple_of(entry, SIZE), SIZE)]
            s = jnp.dot(keys, queries, preferred_element_type=F32)
            held[h * HALF : (h + 1) * HALF] = s
            p = jnp.max(s, axis=0, keepdims=True)
            peak = p if peak is None else jnp.maximum(peak, p)
        return peak

    def absorb(slot, tile, m, held, peak):
        old = top[tile, m]
        new = jnp.maximum(old, peak)
        top[tile, m] = new
        weights = jnp.exp2(held[...] - new).astype(BF16)
        added = None
        for b in range(TOK // 256):
            values = kv_all[slot, b * VALUE : (b + 1) * VALUE, :]
            d = jnp.dot(jnp.concatenate([values, ones], axis=0), weights[b * 256 : (b + 1) * 256],
                        preferred_element_type=F32)
            added = d if added is None else added + d
        acc[tile, m] = acc[tile, m] * jnp.exp2(old - new) + added

    @pl.when(jnp.logical_not(home))
    def _():
        arrive(slot_of(jnp.int32(0)))

    peak = scores(slot_of(jnp.int32(0)), 0, 0, s0)

    def step(t, peak0):
        i, tile = lax.div(t, TILES), lax.rem(t, TILES)
        slot = slot_of(i)

        @pl.when(tile == TILES - 1)
        def _():
            duty(i)

        peak1 = scores(slot, tile, 1, s1)
        absorb(slot, tile, 0, s0, peak0)
        later = jnp.minimum(t + 1, 16 * TILES - 1)
        peak0 = scores(slot_of(lax.div(later, TILES)), lax.rem(later, TILES), 0, s0)
        absorb(slot, tile, 1, s1, peak1)
        return peak0

    lax.fori_loop(0, 16 * TILES, step, peak)

    gain = prm_all[0, 0:1, :]
    mix = prm_all[0, 1:2, 0:1]
    for tile in range(TILES):
        a1, a2 = acc[tile, 0], acc[tile, 1]
        attended = a1[:VALUE] / a1[VALUE : VALUE + 1] - mix * (a2[:VALUE] / a2[VALUE : VALUE + 1])
        square = jnp.mean(attended * attended, axis=0, keepdims=True)
        scaled = attended * lax.rsqrt(square + EPSILON)
        heads[tile * TILE : (tile + 1) * TILE, :] = (scaled.T * gain).astype(BF16)

    unit = (2 * x + lax.div(y, 2)) * 2 + lax.rem(y, 2)

    def deliver(n):
        j, tp_ = n // 8, n % 8
        to = {"sp": z * 4 + 2 * c + j, "tp": jnp.int32(tp_)}
        mine = jnp.logical_and(2 * c + j == y, tp == tp_)
        return heads.at[pl.ds(n * OWN, OWN)], got.at[unit], head_send.at[n], head_recv.at[unit], to, mine

    for n in range(16):
        src, dst, send, recv, to, mine = deliver(n)

        @pl.when(mine)
        def _():
            pltpu.make_async_copy(src, dst, recv).start()

        @pl.when(jnp.logical_not(mine))
        def _():
            remote(src, dst, send, recv, to).start()

    onward(UP)
    for n in range(4):
        w_arrive(2 * n + 1 - c)
    pltpu.make_async_copy(w_ref, w_all.at[head_here], w_own).wait()
    for n in range(16):
        remote(got.at[n], got.at[n], head_send.at[n], head_recv.at[n], side).wait_recv()

    residual_copy.wait()

    def project(n, carry):
        columns = pl.ds(pl.multiple_of(n * 512, 512), 512)
        total = residual_ref[:, columns].astype(F32)
        for h in range(8):
            pair = jnp.concatenate([got[2 * h], got[2 * h + 1]], axis=1)
            total = total + jnp.dot(pair, w_all[h, :, columns], preferred_element_type=F32)
        normed[:, columns] = total
        return carry

    lax.fori_loop(0, 4, project, 0)
    for r in range(0, OWN, 32):
        value = layer_norm(normed[r : r + 32], gain_ref[0:1])
        normed[r : r + 32] = value
        tokens[tp, r : r + 32] = value.astype(BF16)

    def tok_copy(n):
        t_west, t_east, t_far = 2 * lax.rem(x + 3, 4) + c, 2 * lax.rem(x + 1, 4) + c, 2 * lax.rem(x + 2, 4) + c
        half_of = lambda t, k: tokens.at[t, pl.ds(k * 48, 48)]
        return (
            lambda: remote(tokens.at[tp], tokens.at[tp], tok_send.at[0], tok_recv.at[tp], east),
            lambda: remote(tokens.at[tp], tokens.at[tp], tok_send.at[1], tok_recv.at[tp], west),
            lambda: remote(tokens.at[tp], tokens.at[tp], tok_send.at[2], tok_recv.at[tp], side),
            lambda: remote(half_of(t_west, 0), half_of(t_west, 0), tok_send.at[3], tok_far.at[0], east),
            lambda: remote(half_of(t_east, 1), half_of(t_east, 1), tok_send.at[4], tok_far.at[1], west),
            lambda: remote(tokens.at[t_west], tokens.at[t_west], tok_send.at[5], tok_recv.at[t_west], side),
            lambda: remote(tokens.at[t_east], tokens.at[t_east], tok_send.at[6], tok_recv.at[t_east], side),
            lambda: remote(tokens.at[t_far], tokens.at[t_far], tok_send.at[7], tok_recv.at[t_far], side),
        )[n]()

    def tok_arrive(t):
        remote(tokens.at[t], tokens.at[t], tok_send.at[0], tok_recv.at[t], side).wait_recv()

    for n in range(3):
        tok_copy(n).start()
    complete(UP)

    chips = (x, lax.rem(x + 3, 4), lax.rem(x + 1, 4), lax.rem(x + 2, 4))

    def feed(k):
        chip = chips[k]
        rows_in = (2 * chip + c, 2 * chip + 1 - c)

        def up(n, carry):
            columns = pl.ds(pl.multiple_of(n * 512, 512), 512)
            block = jnp.concatenate([tokens[rows_in[0]], tokens[rows_in[1]]], axis=0)
            e = jnp.maximum(jnp.dot(block, up_all[:, columns], preferred_element_type=F32), 0.0)
            hidden[:, columns] = (e * e).astype(BF16)
            return carry

        lax.fori_loop(0, 2, up, 0)
        if k == 0:
            complete(DOWN_A)
            complete(DOWN_B)

        def down(n, carry):
            columns = pl.ds(pl.multiple_of(n * 512, 512), 512)
            p = jnp.dot(hidden[...], down_all[:, columns], preferred_element_type=F32)
            keep[k, :, columns] = p[:OWN]
            to_sib[k, :, columns] = p[OWN:].astype(BF16)
            return carry

        lax.fori_loop(0, 4, down, 0)

    def to_sibling(k):
        return remote(to_sib.at[k], from_sib.at[k], sib_send.at[k], sib_recv.at[k], side)

    def to_owner(k):
        return remote(to_chip.at[k - 1], from_chip.at[k - 1], chip_send.at[k - 1], chip_recv.at[k - 1], (None, west, east, at(z, y, lax.rem(x + 2, 4), c))[k])

    def chip_sum(k):
        to_sibling(k).wait_recv()
        for r in range(0, OWN, 32):
            to_chip[k - 1, r : r + 32] = (keep[k, r : r + 32] + from_sib[k, r : r + 32].astype(F32)).astype(BF16)
        to_owner(k).start()

    tok_arrive(2 * x + 1 - c)
    feed(0)
    to_sibling(0).start()
    west_tok, east_tok, far_tok = (2 * chips[k] + c for k in (1, 2, 3))
    tok_arrive(west_tok)
    tok_copy(3).start()
    tok_copy(5).start()
    tok_arrive(east_tok)
    tok_copy(4).start()
    tok_copy(6).start()
    tok_arrive(2 * chips[1] + 1 - c)
    feed(1)
    to_sibling(1).start()
    tok_arrive(2 * chips[2] + 1 - c)
    feed(2)
    to_sibling(2).start()
    chip_sum(1)
    for k in range(2):
        spot = tokens.at[far_tok, pl.ds(k * 48, 48)]
        remote(spot, spot, tok_send.at[0], tok_far.at[k], side).wait_recv()
    tok_copy(7).start()
    chip_sum(2)
    tok_arrive(2 * chips[3] + 1 - c)
    feed(3)
    to_sibling(3).start()
    chip_sum(3)
    to_sibling(0).wait_recv()
    for k in range(1, 4):
        to_owner(k).wait_recv()
    for r in range(0, OWN, 32):
        span = slice(r, r + 32)
        total = normed[span] + keep[0, span] + from_sib[0, span].astype(F32)
        for k in range(3):
            total = total + from_chip[k, span].astype(F32)
        out_ref[span] = layer_norm(total, gain_ref[1:2]).astype(BF16)

    for part in range(3):
        for g in range(2):
            src, dst, send, recv, to = spread(g)[part]

            @pl.when(jnp.logical_not(2 * c + g == y))
            def _():
                remote(src, dst, send, recv, to).wait_send()

    def sent(g):
        for n in range(3):
            to_right(0, n, g).wait_send()
            to_left(0, n, g).wait_send()
        for n in range(8):
            to_side(0, n, g).wait_send()

    by_group(sent)
    for n in range(8):
        w_copy(n).wait_send()
        tok_copy(n).wait_send()
    for n in range(16):
        src, dst, send, recv, to, mine = deliver(n)

        @pl.when(jnp.logical_not(mine))
        def _():
            remote(src, dst, send, recv, to).wait_send()

    for w in range(3):
        for k in range(2):
            ff_first(w, k).wait_send()
            ff_half(w, k).wait_send()
            for row in range(4):
                ff_column(w, row, k).wait_send()
            for n in range(2):
                ff_onward(w, n, k).wait_send()
    for k in range(4):
        to_sibling(k).wait_send()
    for k in range(1, 4):
        to_owner(k).wait_send()


def layer(*operands):
    dma = pltpu.SemaphoreType.DMA
    vmem, hbm = pl.BlockSpec(memory_space=pltpu.VMEM), pl.BlockSpec(memory_space=pl.ANY)
    return pl.pallas_call(
        attention_kernel,
        out_shape=jax.ShapeDtypeStruct((OWN, 2048), BF16),
        in_specs=[vmem] * 8 + [hbm] * 4 + [vmem],
        out_specs=vmem,
        scratch_shapes=[
            pltpu.VMEM((2, 2, SIZE, TOK), BF16),
            pltpu.VMEM((2, SLAB, 256), BF16),
            pltpu.VMEM((2, 8, 128), F32),
            pltpu.VMEM((OWN, 2048), BF16),
            dma(()),
            pltpu.VMEM((2, SIZE, 2 * TOK), BF16),
            pltpu.VMEM((16, SLAB, 256), BF16),
            pltpu.VMEM((2, 8, 128), F32),
            pltpu.VMEM((8, 256, 2048), BF16),
            pltpu.VMEM((TOK, TILE), F32),
            pltpu.VMEM((TOK, TILE), F32),
            pltpu.VMEM((TILES, 2, 1, TILE), F32),
            pltpu.VMEM((TILES, 2, ROWS, TILE), F32),
            pltpu.VMEM((2 * TOK, VALUE), BF16),
            pltpu.VMEM((16, OWN, VALUE), BF16),
            dma((2,)), dma((2,)), dma((2,)), dma((3,)), dma((3,)), dma((8,)), dma((16,)), dma((8,)),
            dma((2,)), dma((16,)), dma((2,)), dma((16,)), dma((8,)), dma((2,)), dma(()),
            pltpu.VMEM((2048, 1024), BF16),
            pltpu.VMEM((1024, 2048), BF16),
            pltpu.VMEM((8, OWN, 2048), BF16),
            pltpu.VMEM((OWN, 2048), F32),
            pltpu.VMEM((2 * OWN, 1024), BF16),
            pltpu.VMEM((4, OWN, 2048), F32),
            pltpu.VMEM((4, OWN, 2048), BF16),
            pltpu.VMEM((4, OWN, 2048), BF16),
            pltpu.VMEM((3, OWN, 2048), BF16),
            pltpu.VMEM((3, OWN, 2048), BF16),
            dma((48,)), dma((16,)), dma((16,)), dma((16,)), dma((6,)), dma((3,)), dma((8,)), dma((8,)), dma((2,)), dma((4,)), dma((4,)),
            dma((3,)), dma((3,)),
        ],
        compiler_params=pltpu.CompilerParams(collective_id=0, has_side_effects=True, vmem_limit_bytes=63 << 20),
        cost_estimate=pl.CostEstimate(flops=4 * 768 * 12288 * 4 * 128, bytes_accessed=4 << 20, transcendentals=4 * 768 * 12288),
        name="attention",
    )(*operands)


def layer_norm(activations, scales):
    average = jnp.mean(activations, axis=-1, keepdims=True)
    centred = activations - average
    spread = jnp.mean(centred * centred, axis=-1, keepdims=True)
    return centred * lax.rsqrt(spread + EPSILON) * scales


def local(query_first, key_first, value_first, query_second, key_second, value_second, mix_lambda, head_gain, out_weight,
          residual, norm_gain, up_weight, down_weight):
    return layer(query_first[:, 0], key_first[:, 0], value_first[:, 0], query_second[:, 0], key_second[:, 0], value_second[:, 0],
                 mix_lambda, head_gain[:, 0], out_weight.reshape(2 * VALUE, -1), up_weight, down_weight, residual, norm_gain)


def solution(mesh):
    heads = P("sp", "tp", None)
    return jax.shard_map(
        local,
        mesh=mesh,
        in_specs=(heads, heads, heads, heads, heads, heads, P(None, "tp"), P(None, "tp", None), P(None, "tp", None, None),
                  P(("sp", "tp"), None), P(), P("sp", "tp"), P("tp", "sp")),
        out_specs=P(("sp", "tp"), None),
        check_vma=False,
    )
```

```python
import functools
import math

import jax
import jax.numpy as jnp
from jax import lax
from jax.experimental import pallas as pl
from jax.experimental.pallas import tpu as pltpu
from jax.sharding import PartitionSpec as P

EPSILON = 1e-05
LOWEST = -1e30
LOG2E = math.log2(math.e)
MESH = pl.DeviceIdType.MESH
BF16 = jnp.bfloat16
F32 = jnp.float32

TOK = 768
OWN = 96
SIZE = 128
VALUE = 128
HALF = TOK // 2
KEYS = VALUE * TOK // 256
SLAB = KEYS + TOK
LENGTHS = (KEYS + HALF, SLAB)
TILE = 512
TILES = 2 * TOK // TILE
ROWS = VALUE + 16


def attention_kernel(q1_ref, k1_ref, v1_ref, q2_ref, k2_ref, v2_ref, mix_ref, head_gain_ref, w_ref, up_ref, down_ref, residual_hbm,
                     gain_ref, out_ref, q_own, kv_own, prm_own, residual_ref, residual_sem, q_all, kv_all, prm_all, w_all, s0, s1, top, acc, heads, got,
                     q_send, kv_send, prm_send, right_send, left_send, side_send, head_send, w_send,
                     q_recv, kv_recv, prm_recv, head_recv, w_recv, w_far, w_own,
                     up_all, down_all, tokens, normed, hidden, keep, to_sib, from_sib, to_chip, from_chip,
                     ff_send, up_recv, down_recv, rest_recv, ff_far, ff_own, tok_send, tok_recv, tok_far, sib_send, sib_recv,
                     chip_send, chip_recv):
    sp, tp = lax.axis_index("sp"), lax.axis_index("tp")
    z, y = lax.div(sp, 4), lax.rem(sp, 4)
    x, c = lax.div(tp, 2), lax.rem(tp, 2)

    def at(z_, y_, x_, c_):
        return {"sp": z_ * 4 + y_, "tp": x_ * 2 + c_}

    above, below = lax.rem(z + 1, 4), lax.rem(z + 3, 4)
    far = lax.rem(z + 2, 4)
    right, left, side = at(above, y, x, c), at(below, y, x, c), at(z, y, x, 1 - c)

    barrier = pltpu.get_barrier_semaphore()

    def greet(i, carry):
        other = lax.rem(y * 8 + tp + i, 32)
        pl.semaphore_signal(barrier, inc=1, device_id={"sp": z * 4 + lax.div(other, 8), "tp": lax.rem(other, 8)},
                            device_id_type=MESH)
        return carry

    lax.fori_loop(1, 32, greet, 0)
    pl.semaphore_signal(barrier, inc=1, device_id=right, device_id_type=MESH)
    pl.semaphore_signal(barrier, inc=1, device_id=left, device_id_type=MESH)
    residual_copy = pltpu.make_async_copy(residual_hbm, residual_ref, residual_sem)
    residual_copy.start()

    q_own[0, 0] = (q1_ref[...].astype(F32) * (LOG2E / 8.0)).T.astype(BF16)
    for m in range(2):
        q_own[1, m] = (q2_ref[:, m * SIZE : (m + 1) * SIZE].astype(F32) * (LOG2E / math.sqrt(128.0))).T.astype(BF16)
    for g, values in ((0, v1_ref), (1, v2_ref)):
        for b in range(TOK // 256):
            kv_own[g, b * VALUE : (b + 1) * VALUE] = values[b * 256 : (b + 1) * 256].astype(F32).T.astype(BF16)
        prm_own[g, 0:1] = head_gain_ref[g : g + 1]
        prm_own[g, 1:2] = jnp.broadcast_to(mix_ref[g : g + 1], (1, 128))
    for h in range(2):
        kv_own[0, KEYS : KEYS + HALF, h * SIZE : (h + 1) * SIZE] = k1_ref[h * HALF : (h + 1) * HALF]
    kv_own[1, KEYS:SLAB] = k2_ref[...]
    pl.semaphore_wait(barrier, 33)

    def remote(src, dst, send, recv, device):
        return pltpu.make_async_remote_copy(src_ref=src, dst_ref=dst, send_sem=send, recv_sem=recv, device_id=device,
                                            device_id_type=MESH)

    half, odd = lax.div(y, 2), lax.rem(y, 2)
    home = c == half

    def q_views(g, j):
        lanes = pl.ds(j * TOK if isinstance(j, int) else pl.multiple_of(j * TOK, TOK), TOK)
        return (q_own.at[0, 0], q_all.at[0, :, lanes]) if g == 0 else (q_own.at[1], q_all.at[:, :, lanes])

    def slab(slot, g):
        return kv_all.at[slot, pl.ds(0, LENGTHS[g])]

    def spread(g):
        to = at(z, 2 * c + g, x, half)
        return (
            (*q_views(g, odd), q_send.at[g], q_recv.at[odd], to),
            (prm_own.at[g], prm_all.at[odd], prm_send.at[g], prm_recv.at[odd], to),
            (kv_own.at[g, pl.ds(0, LENGTHS[g])], slab(z * 4 + y, g), kv_send.at[g], kv_recv.at[z * 4 + y], to),
        )

    def away(part, g):
        src, dst, send, recv, to = spread(g)[part]

        @pl.when(jnp.logical_not(2 * c + g == y))
        def _():
            remote(src, dst, send, recv, to).start()

    for part in range(2):
        for g in range(2):
            away(part, g)
    def near_or_far(far_ones):
        for g in range(2):
            @pl.when(odd == (g if far_ones else 1 - g))
            def _():
                away(2, g)

    near_or_far(False)

    def place(kind):
        return (y, y + 1 - 2 * odd, 3 - y, lax.rem(y + 2, 4))[kind]

    rows = (z, below, above, far)

    def by_group(action):
        for g in range(2):
            @pl.when(odd == g)
            def _():
                action(g)

    def arrive_of(slot, g):
        remote(slab(slot, g), slab(slot, g), kv_send.at[0], kv_recv.at[slot], side).wait_recv()

    def arrive(slot):
        by_group(lambda g: arrive_of(slot, g))

    def to_side(slot, n, g):
        return remote(slab(slot, g), slab(slot, g), side_send.at[n], kv_recv.at[slot], side)

    def to_right(slot, n, g):
        return remote(slab(slot, g), slab(slot, g), right_send.at[n], kv_recv.at[slot], right)

    def to_left(slot, n, g):
        return remote(slab(slot, g), slab(slot, g), left_send.at[n], kv_recv.at[slot], left)

    def own_shard(g):
        slot = z * 4 + y
        for sends, to in ((right_send, right), (left_send, left), (side_send, side)):
            remote(kv_own.at[g, pl.ds(0, LENGTHS[g])], slab(slot, g), sends.at[0], kv_recv.at[slot], to).start()
        lanes = pl.ds(pl.multiple_of(odd * TOK, TOK), TOK)
        kv_all[slot, 0 : LENGTHS[g]] = kv_own[g, 0 : LENGTHS[g]]
        for m in range(1 + g):
            q_all[m, :, lanes] = q_own[g, m]
        prm_all[odd] = prm_own[g]

    def pass_on(kind, row):
        slot = rows[row] * 4 + place(kind)
        second = kind % 2

        def relay(g):
            arrive_of(slot, g)
            if row == 0:
                to_right(slot, second, g).start()
                to_left(slot, second, g).start()
            elif row == 1 and not second:
                to_right(slot, 2, g).start()
            elif row == 2 and second:
                to_left(slot, 2, g).start()
            to_side(slot, second * 4 + row, g).start()

        by_group(relay)

    east, west = at(z, y, lax.rem(x + 1, 4), c), at(z, y, lax.rem(x + 3, 4), c)
    head_here, head_east = 2 * x + c, 2 * lax.rem(x + 1, 4) + c
    head_west, head_far = 2 * lax.rem(x + 3, 4) + c, 2 * lax.rem(x + 2, 4) + c

    def w_copy(n):
        full = lambda h: w_all.at[h]
        part = lambda h, k: w_all.at[h, pl.ds(k * 128, 128)]
        return (
            lambda: remote(w_ref, full(head_here), w_send.at[0], w_recv.at[head_here], east),
            lambda: remote(w_ref, full(head_here), w_send.at[1], w_recv.at[head_here], west),
            lambda: remote(w_ref, full(head_here), w_send.at[2], w_recv.at[head_here], side),
            lambda: remote(part(head_west, 0), part(head_west, 0), w_send.at[3], w_far.at[0], east),
            lambda: remote(part(head_east, 1), part(head_east, 1), w_send.at[4], w_far.at[1], west),
            lambda: remote(full(head_west), full(head_west), w_send.at[5], w_recv.at[head_west], side),
            lambda: remote(full(head_east), full(head_east), w_send.at[6], w_recv.at[head_east], side),
            lambda: remote(full(head_far), full(head_far), w_send.at[7], w_recv.at[head_far], side),
        )[n]()

    def w_arrive(h):
        remote(w_all.at[h], w_all.at[h], w_send.at[0], w_recv.at[h], side).wait_recv()

    forth, back = at(z, lax.rem(y + 1, 4), x, c), at(z, lax.rem(y + 3, 4), x, c)
    y_forth, y_back, y_far = lax.rem(y + 1, 4), lax.rem(y + 3, 4), lax.rem(y + 2, 4)
    UP, DOWN_A, DOWN_B = 0, 1, 2

    def source(p):
        return up_ref if p == UP else down_ref.at[pl.ds(512 * (p - 1), 512)]

    def shard(p, s, k=None):
        if p == UP:
            if k is None:
                return up_all.at[pl.ds(pl.multiple_of(s * 128, 128), 128)]
            return up_all.at[pl.ds(pl.multiple_of(s * 128 + k * 64, 64), 64)]
        lanes = pl.ds(pl.multiple_of(s * 128, 128), 128)
        start = 512 * (p - 1)
        return down_all.at[pl.ds(start, 512) if k is None else pl.ds(start + k * 256, 256), lanes]

    def lines(p):
        by_z = ((right, left), (below * 4 + y, above * 4 + y, far * 4 + y), lambda r: r * 4 + y, lambda r: r * 4 + y_back,
                lambda r: r * 4 + y_forth, lambda r: r * 4 + y_far)
        by_y = ((forth, back), (z * 4 + y_back, z * 4 + y_forth, z * 4 + y_far), lambda r: z * 4 + r, lambda r: below * 4 + r,
                lambda r: above * 4 + r, lambda r: far * 4 + r)
        return by_y + ((right, left),) if p == UP else by_z + ((forth, back),)

    ff_recv = (up_recv, down_recv, rest_recv)

    def piece(p, n, s, to, k=None, recv=None):
        view = shard(p, s, k)
        return remote(view, view, ff_send.at[16 * p + n], ff_recv[p].at[s] if recv is None else recv, to)

    def ff_first(p, k):
        return remote(source(p), shard(p, sp), ff_send.at[16 * p + k], ff_recv[p].at[sp], lines(p)[0][k])

    def ff_half(p, k):
        return piece(p, 2 + k, lines(p)[1][k], lines(p)[0][k], k, ff_far.at[2 * p + k])

    def ff_column(p, r, k):
        return piece(p, 4 + 2 * r + k, lines(p)[2](r), lines(p)[6][k])

    def ff_onward(p, n, k):
        return piece(p, 12 + 2 * n + k, lines(p)[3 + k](n + 2 * k), lines(p)[6][k])

    def ff_arrive(p, s):
        piece(p, 0, s, side).wait_recv()

    def begin(p):
        pltpu.make_async_copy(source(p), shard(p, sp), ff_own.at[p]).start()
        for k in range(2):
            ff_first(p, k).start()

    def halves(p):
        for k in range(2):
            ff_arrive(p, lines(p)[1][k])
            ff_half(p, k).start()

    def gathered(p):
        for k in range(2):
            piece(p, 0, lines(p)[1][2], side, k, ff_far.at[2 * p + k]).wait_recv()
        pltpu.make_async_copy(source(p), shard(p, sp), ff_own.at[p]).wait()

    def columns(p, second):
        for n in range(2):
            for k in range(2):
                ff_column(p, (n + 2 - 2 * k) if second else (n + 2 * k), k).start()

    def onward(p):
        for n in range(2):
            for k in range(2):
                ff_arrive(p, lines(p)[3 + k](n + 2 * k))
                ff_onward(p, n, k).start()

    def complete(p):
        for n in range(2):
            for k in range(2):
                ff_arrive(p, lines(p)[3 + k](n + 2 - 2 * k))
        for r in range(4):
            ff_arrive(p, lines(p)[5](r))


    @pl.when(home)
    def _():
        by_group(own_shard)

    begin(DOWN_A)
    begin(DOWN_B)

    @pl.when(home)
    def _():
        pass_on(0, 1)
        pass_on(0, 2)


    kinds = (0, 0, 0, 0, 1, 2, 1, 1, 2, 2, 3, 1, 2, 3, 3, 3)
    order = (0, 1, 2, 3, 0, 0, 1, 2, 1, 2, 0, 3, 3, 1, 2, 3)
    home_duties = {0: ((1, 0),), 1: ((0, 3),), 5: ((1, 1), (1, 2)), 10: ((1, 3),)}
    away_duties = {1: ((2, 0),), 4: ((3, 0),), 5: ((2, 1), (2, 2)), 9: ((3, 1), (3, 2)), 10: ((2, 3),), 13: ((3, 3),)}

    def pick(i, table):
        value = jnp.int32(table[0])
        for n in range(1, 16):
            if table[n] != table[n - 1]:
                value = jnp.where(i >= n, table[n], value)
        return value

    def slot_of(i):
        kind, row = pick(i, kinds), pick(i, order)
        row = jnp.where(row == 0, z, jnp.where(row == 1, below, jnp.where(row == 2, above, far)))
        spot = jnp.where(kind == 0, y, jnp.where(kind == 1, y + 1 - 2 * odd, jnp.where(kind == 2, 3 - y, lax.rem(y + 2, 4))))
        return row * 4 + spot

    def duty(i):
        for n in range(16):
            for mine, duties in ((home, home_duties), (jnp.logical_not(home), away_duties)):
                if n in duties:
                    @pl.when(jnp.logical_and(i == n, mine))
                    def _():
                        for kind, row in duties[n]:
                            pass_on(kind, row)
        kind = pick(i + 1, kinds)

        @pl.when(jnp.logical_and(i < 15, jnp.logical_not(home) == (kind < 2)))
        def _():
            arrive(slot_of(i + 1))

        @pl.when(i == 0)
        def _():
            near_or_far(True)
            begin(UP)
            for n in range(3):
                w_copy(n).start()
            pltpu.make_async_copy(w_ref, w_all.at[head_here], w_own).start()

        @pl.when(i == 3)
        def _():
            halves(DOWN_A)
            halves(DOWN_B)
            halves(UP)

        @pl.when(i == 5)
        def _():
            gathered(DOWN_A)
            columns(DOWN_A, False)
            columns(DOWN_A, True)

        @pl.when(i == 6)
        def _():
            gathered(DOWN_B)
            columns(DOWN_B, False)
            columns(DOWN_B, True)

        @pl.when(i == 9)
        def _():
            gathered(UP)
            columns(UP, False)
            columns(UP, True)

        @pl.when(i == 10)
        def _():
            onward(DOWN_A)
            onward(DOWN_B)

        @pl.when(i == 8)
        def _():
            w_arrive(head_west)
            w_copy(3).start()
            w_arrive(head_east)
            w_copy(4).start()
            w_copy(5).start()
            w_copy(6).start()

        @pl.when(i == 12)
        def _():
            for k in range(2):
                remote(w_all.at[0, pl.ds(0, 128)], w_all.at[head_far, pl.ds(k * 128, 128)], w_send.at[0], w_far.at[k],
                       side).wait_recv()
            w_copy(7).start()

    for j in range(2):
        @pl.when(jnp.logical_not(jnp.logical_and(home, odd == j)))
        def _():
            by_group(lambda g: remote(*q_views(g, j), q_send.at[0], q_recv.at[j], side).wait_recv())
            remote(prm_own.at[0], prm_all.at[j], prm_send.at[0], prm_recv.at[j], side).wait_recv()

    @pl.when(odd == 0)
    def _():
        both = q_all[0]
        nothing = jnp.zeros((SIZE // 2, 2 * TOK), BF16)
        q_all[1, 0 : SIZE // 2] = nothing
        q_all[1, SIZE // 2 : SIZE] = both[SIZE // 2 : SIZE]
        q_all[0, SIZE // 2 : SIZE] = nothing

    top[...] = jnp.full(top.shape, LOWEST, F32)
    acc[...] = jnp.zeros(acc.shape, F32)
    ones = jnp.ones((ROWS - VALUE, 256), BF16)

    def scores(slot, tile, m, held):
        queries = q_all[m, :, pl.ds(pl.multiple_of(tile * TILE, TILE), TILE)]
        peak = None
        for h in range(2):
            start = KEYS + (odd * HALF if h else 0)
            entry = m * SIZE if h == m else (odd if m else 1 - odd) * SIZE
            keys = kv_all[slot, pl.ds(pl.multiple_of(start, HALF), HALF), pl.ds(pl.multiple_of(entry, SIZE), SIZE)]
            s = jnp.dot(keys, queries, preferred_element_type=F32)
            held[h * HALF : (h + 1) * HALF] = s
            p = jnp.max(s, axis=0, keepdims=True)
            peak = p if peak is None else jnp.maximum(peak, p)
        return peak

    def absorb(slot, tile, m, held, peak):
        old = top[tile, m]
        new = jnp.maximum(old, peak)
        top[tile, m] = new
        weights = jnp.exp2(held[...] - new).astype(BF16)
        added = None
        for b in range(TOK // 256):
            values = kv_all[slot, b * VALUE : (b + 1) * VALUE, :]
            d = jnp.dot(jnp.concatenate([values, ones], axis=0), weights[b * 256 : (b + 1) * 256],
                        preferred_element_type=F32)
            added = d if added is None else added + d
        acc[tile, m] = acc[tile, m] * jnp.exp2(old - new) + added

    @pl.when(jnp.logical_not(home))
    def _():
        arrive(slot_of(jnp.int32(0)))

    peak = scores(slot_of(jnp.int32(0)), 0, 0, s0)

    def step(t, peak0):
        i, tile = lax.div(t, TILES), lax.rem(t, TILES)
        slot = slot_of(i)

        @pl.when(tile == TILES - 1)
        def _():
            duty(i)

        peak1 = scores(slot, tile, 1, s1)
        absorb(slot, tile, 0, s0, peak0)
        later = jnp.minimum(t + 1, 16 * TILES - 1)
        peak0 = scores(slot_of(lax.div(later, TILES)), lax.rem(later, TILES), 0, s0)
        absorb(slot, tile, 1, s1, peak1)
        return peak0

    lax.fori_loop(0, 16 * TILES, step, peak)

    gain = prm_all[0, 0:1, :]
    mix = prm_all[0, 1:2, 0:1]
    for tile in range(TILES):
        a1, a2 = acc[tile, 0], acc[tile, 1]
        attended = a1[:VALUE] / a1[VALUE : VALUE + 1] - mix * (a2[:VALUE] / a2[VALUE : VALUE + 1])
        square = jnp.mean(attended * attended, axis=0, keepdims=True)
        scaled = attended * lax.rsqrt(square + EPSILON)
        heads[tile * TILE : (tile + 1) * TILE, :] = (scaled.T * gain).astype(BF16)

    unit = (2 * x + lax.div(y, 2)) * 2 + lax.rem(y, 2)

    def deliver(n):
        j, tp_ = n // 8, n % 8
        to = {"sp": z * 4 + 2 * c + j, "tp": jnp.int32(tp_)}
        mine = jnp.logical_and(2 * c + j == y, tp == tp_)
        return heads.at[pl.ds(n * OWN, OWN)], got.at[unit], head_send.at[n], head_recv.at[unit], to, mine

    for n in range(16):
        src, dst, send, recv, to, mine = deliver(n)

        @pl.when(mine)
        def _():
            pltpu.make_async_copy(src, dst, recv).start()

        @pl.when(jnp.logical_not(mine))
        def _():
            remote(src, dst, send, recv, to).start()

    onward(UP)
    for n in range(4):
        w_arrive(2 * n + 1 - c)
    pltpu.make_async_copy(w_ref, w_all.at[head_here], w_own).wait()
    for n in range(16):
        remote(got.at[n], got.at[n], head_send.at[n], head_recv.at[n], side).wait_recv()

    residual_copy.wait()

    def project(n, carry):
        columns = pl.ds(pl.multiple_of(n * 512, 512), 512)
        total = residual_ref[:, columns].astype(F32)
        for h in range(8):
            pair = jnp.concatenate([got[2 * h], got[2 * h + 1]], axis=1)
            total = total + jnp.dot(pair, w_all[h, :, columns], preferred_element_type=F32)
        normed[:, columns] = total
        return carry

    lax.fori_loop(0, 4, project, 0)
    for r in range(0, OWN, 32):
        value = layer_norm(normed[r : r + 32], gain_ref[0:1])
        normed[r : r + 32] = value
        tokens[tp, r : r + 32] = value.astype(BF16)

    def tok_copy(n):
        t_west, t_east, t_far = 2 * lax.rem(x + 3, 4) + c, 2 * lax.rem(x + 1, 4) + c, 2 * lax.rem(x + 2, 4) + c
        half_of = lambda t, k: tokens.at[t, pl.ds(k * 48, 48)]
        return (
            lambda: remote(tokens.at[tp], tokens.at[tp], tok_send.at[0], tok_recv.at[tp], east),
            lambda: remote(tokens.at[tp], tokens.at[tp], tok_send.at[1], tok_recv.at[tp], west),
            lambda: remote(tokens.at[tp], tokens.at[tp], tok_send.at[2], tok_recv.at[tp], side),
            lambda: remote(half_of(t_west, 0), half_of(t_west, 0), tok_send.at[3], tok_far.at[0], east),
            lambda: remote(half_of(t_east, 1), half_of(t_east, 1), tok_send.at[4], tok_far.at[1], west),
            lambda: remote(tokens.at[t_west], tokens.at[t_west], tok_send.at[5], tok_recv.at[t_west], side),
            lambda: remote(tokens.at[t_east], tokens.at[t_east], tok_send.at[6], tok_recv.at[t_east], side),
            lambda: remote(tokens.at[t_far], tokens.at[t_far], tok_send.at[7], tok_recv.at[t_far], side),
        )[n]()

    def tok_arrive(t):
        remote(tokens.at[t], tokens.at[t], tok_send.at[0], tok_recv.at[t], side).wait_recv()

    for n in range(3):
        tok_copy(n).start()
    complete(UP)

    chips = (x, lax.rem(x + 3, 4), lax.rem(x + 1, 4), lax.rem(x + 2, 4))

    def feed(k):
        chip = chips[k]
        rows_in = (2 * chip + c, 2 * chip + 1 - c)

        def up(n, carry):
            columns = pl.ds(pl.multiple_of(n * 512, 512), 512)
            block = jnp.concatenate([tokens[rows_in[0]], tokens[rows_in[1]]], axis=0)
            e = jnp.maximum(jnp.dot(block, up_all[:, columns], preferred_element_type=F32), 0.0)
            hidden[:, columns] = (e * e).astype(BF16)
            return carry

        lax.fori_loop(0, 2, up, 0)
        if k == 0:
            complete(DOWN_A)
            complete(DOWN_B)

        def down(n, carry):
            columns = pl.ds(pl.multiple_of(n * 512, 512), 512)
            p = jnp.dot(hidden[...], down_all[:, columns], preferred_element_type=F32)
            keep[k, :, columns] = p[:OWN]
            to_sib[k, :, columns] = p[OWN:].astype(BF16)
            return carry

        lax.fori_loop(0, 4, down, 0)

    def to_sibling(k):
        return remote(to_sib.at[k], from_sib.at[k], sib_send.at[k], sib_recv.at[k], side)

    def to_owner(k):
        return remote(to_chip.at[k - 1], from_chip.at[k - 1], chip_send.at[k - 1], chip_recv.at[k - 1], (None, west, east, at(z, y, lax.rem(x + 2, 4), c))[k])

    def chip_sum(k):
        to_sibling(k).wait_recv()
        for r in range(0, OWN, 32):
            to_chip[k - 1, r : r + 32] = (keep[k, r : r + 32] + from_sib[k, r : r + 32].astype(F32)).astype(BF16)
        to_owner(k).start()

    tok_arrive(2 * x + 1 - c)
    feed(0)
    to_sibling(0).start()
    west_tok, east_tok, far_tok = (2 * chips[k] + c for k in (1, 2, 3))
    tok_arrive(west_tok)
    tok_copy(3).start()
    tok_copy(5).start()
    tok_arrive(east_tok)
    tok_copy(4).start()
    tok_copy(6).start()
    tok_arrive(2 * chips[1] + 1 - c)
    feed(1)
    to_sibling(1).start()
    tok_arrive(2 * chips[2] + 1 - c)
    feed(2)
    to_sibling(2).start()
    chip_sum(1)
    for k in range(2):
        spot = tokens.at[far_tok, pl.ds(k * 48, 48)]
        remote(spot, spot, tok_send.at[0], tok_far.at[k], side).wait_recv()
    tok_copy(7).start()
    chip_sum(2)
    tok_arrive(2 * chips[3] + 1 - c)
    feed(3)
    to_sibling(3).start()
    chip_sum(3)
    to_sibling(0).wait_recv()
    for k in range(1, 4):
        to_owner(k).wait_recv()
    for r in range(0, OWN, 32):
        span = slice(r, r + 32)
        total = normed[span] + keep[0, span] + from_sib[0, span].astype(F32)
        for k in range(3):
            total = total + from_chip[k, span].astype(F32)
        out_ref[span] = layer_norm(total, gain_ref[1:2]).astype(BF16)

    for part in range(3):
        for g in range(2):
            src, dst, send, recv, to = spread(g)[part]

            @pl.when(jnp.logical_not(2 * c + g == y))
            def _():
                remote(src, dst, send, recv, to).wait_send()

    def sent(g):
        for n in range(3):
            to_right(0, n, g).wait_send()
            to_left(0, n, g).wait_send()
        for n in range(8):
            to_side(0, n, g).wait_send()

    by_group(sent)
    for n in range(8):
        w_copy(n).wait_send()
        tok_copy(n).wait_send()
    for n in range(16):
        src, dst, send, recv, to, mine = deliver(n)

        @pl.when(jnp.logical_not(mine))
        def _():
            remote(src, dst, send, recv, to).wait_send()

    for w in range(3):
        for k in range(2):
            ff_first(w, k).wait_send()
            ff_half(w, k).wait_send()
            for row in range(4):
                ff_column(w, row, k).wait_send()
            for n in range(2):
                ff_onward(w, n, k).wait_send()
    for k in range(4):
        to_sibling(k).wait_send()
    for k in range(1, 4):
        to_owner(k).wait_send()


def layer(*operands):
    dma = pltpu.SemaphoreType.DMA
    vmem, hbm = pl.BlockSpec(memory_space=pltpu.VMEM), pl.BlockSpec(memory_space=pl.ANY)
    return pl.pallas_call(
        attention_kernel,
        out_shape=jax.ShapeDtypeStruct((OWN, 2048), BF16),
        in_specs=[vmem] * 8 + [hbm] * 4 + [vmem],
        out_specs=vmem,
        scratch_shapes=[
            pltpu.VMEM((2, 2, SIZE, TOK), BF16),
            pltpu.VMEM((2, SLAB, 256), BF16),
            pltpu.VMEM((2, 8, 128), F32),
            pltpu.VMEM((OWN, 2048), BF16),
            dma(()),
            pltpu.VMEM((2, SIZE, 2 * TOK), BF16),
            pltpu.VMEM((16, SLAB, 256), BF16),
            pltpu.VMEM((2, 8, 128), F32),
            pltpu.VMEM((8, 256, 2048), BF16),
            pltpu.VMEM((TOK, TILE), F32),
            pltpu.VMEM((TOK, TILE), F32),
            pltpu.VMEM((TILES, 2, 1, TILE), F32),
            pltpu.VMEM((TILES, 2, ROWS, TILE), F32),
            pltpu.VMEM((2 * TOK, VALUE), BF16),
            pltpu.VMEM((16, OWN, VALUE), BF16),
            dma((2,)), dma((2,)), dma((2,)), dma((3,)), dma((3,)), dma((8,)), dma((16,)), dma((8,)),
            dma((2,)), dma((16,)), dma((2,)), dma((16,)), dma((8,)), dma((2,)), dma(()),
            pltpu.VMEM((2048, 1024), BF16),
            pltpu.VMEM((1024, 2048), BF16),
            pltpu.VMEM((8, OWN, 2048), BF16),
            pltpu.VMEM((OWN, 2048), F32),
            pltpu.VMEM((2 * OWN, 1024), BF16),
            pltpu.VMEM((4, OWN, 2048), F32),
            pltpu.VMEM((4, OWN, 2048), BF16),
            pltpu.VMEM((4, OWN, 2048), BF16),
            pltpu.VMEM((3, OWN, 2048), BF16),
            pltpu.VMEM((3, OWN, 2048), BF16),
            dma((48,)), dma((16,)), dma((16,)), dma((16,)), dma((6,)), dma((3,)), dma((8,)), dma((8,)), dma((2,)), dma((4,)), dma((4,)),
            dma((3,)), dma((3,)),
        ],
        compiler_params=pltpu.CompilerParams(collective_id=0, has_side_effects=True, vmem_limit_bytes=63 << 20),
        cost_estimate=pl.CostEstimate(flops=4 * 768 * 12288 * 4 * 128, bytes_accessed=4 << 20, transcendentals=4 * 768 * 12288),
        name="attention",
    )(*operands)


def layer_norm(activations, scales):
    average = jnp.mean(activations, axis=-1, keepdims=True)
    centred = activations - average
    spread = jnp.mean(centred * centred, axis=-1, keepdims=True)
    return centred * lax.rsqrt(spread + EPSILON) * scales


def local(query_first, key_first, value_first, query_second, key_second, value_second, mix_lambda, head_gain, out_weight,
          residual, norm_gain, up_weight, down_weight):
    return layer(query_first[:, 0], key_first[:, 0], value_first[:, 0], query_second[:, 0], key_second[:, 0], value_second[:, 0],
                 mix_lambda, head_gain[:, 0], out_weight.reshape(2 * VALUE, -1), up_weight, down_weight, residual, norm_gain)


def solution(mesh):
    heads = P("sp", "tp", None)
    return jax.shard_map(
        local,
        mesh=mesh,
        in_specs=(heads, heads, heads, heads, heads, heads, P(None, "tp"), P(None, "tp", None), P(None, "tp", None, None),
                  P(("sp", "tp"), None), P(), P("sp", "tp"), P("tp", "sp")),
        out_specs=P(("sp", "tp"), None),
        check_vma=False,
    )
```

```python
import functools
import math

import jax
import jax.numpy as jnp
from jax import lax
from jax.experimental import pallas as pl
from jax.experimental.pallas import tpu as pltpu
from jax.sharding import PartitionSpec as P

EPSILON = 1e-05
LOWEST = -1e30
LOG2E = math.log2(math.e)
MESH = pl.DeviceIdType.MESH
BF16 = jnp.bfloat16
F32 = jnp.float32

TOK = 768
OWN = 96
SIZE = 128
VALUE = 128
HALF = TOK // 2
KEYS = VALUE * TOK // 256
SLAB = KEYS + TOK
LENGTHS = (KEYS + HALF, SLAB)
TILE = 512
TILES = 2 * TOK // TILE
ROWS = VALUE + 16


def attention_kernel(q1_ref, k1_ref, v1_ref, q2_ref, k2_ref, v2_ref, mix_ref, head_gain_ref, w_ref, up_ref, down_ref, residual_hbm,
                     gain_ref, out_ref, q_own, kv_own, prm_own, residual_ref, residual_sem, q_all, kv_all, prm_all, w_all, s0, s1, top, acc, heads, got,
                     q_send, kv_send, prm_send, right_send, left_send, side_send, head_send, w_send,
                     q_recv, kv_recv, prm_recv, head_recv, w_recv, w_far, w_own,
                     up_all, down_all, tokens, normed, hidden, keep, to_sib, from_sib, to_chip, from_chip,
                     ff_send, up_recv, down_recv, rest_recv, ff_far, ff_own, tok_send, tok_recv, tok_far, sib_send, sib_recv,
                     chip_send, chip_recv):
    sp, tp = lax.axis_index("sp"), lax.axis_index("tp")
    z, y = lax.div(sp, 4), lax.rem(sp, 4)
    x, c = lax.div(tp, 2), lax.rem(tp, 2)

    def at(z_, y_, x_, c_):
        return {"sp": z_ * 4 + y_, "tp": x_ * 2 + c_}

    above, below = lax.rem(z + 1, 4), lax.rem(z + 3, 4)
    far = lax.rem(z + 2, 4)
    right, left, side = at(above, y, x, c), at(below, y, x, c), at(z, y, x, 1 - c)

    barrier = pltpu.get_barrier_semaphore()

    def greet(i, carry):
        other = lax.rem(y * 8 + tp + i, 32)
        pl.semaphore_signal(barrier, inc=1, device_id={"sp": z * 4 + lax.div(other, 8), "tp": lax.rem(other, 8)},
                            device_id_type=MESH)
        return carry

    lax.fori_loop(1, 32, greet, 0)
    pl.semaphore_signal(barrier, inc=1, device_id=right, device_id_type=MESH)
    pl.semaphore_signal(barrier, inc=1, device_id=left, device_id_type=MESH)
    residual_copy = pltpu.make_async_copy(residual_hbm, residual_ref, residual_sem)
    residual_copy.start()

    q_own[0, 0] = (q1_ref[...].astype(F32) * (LOG2E / 8.0)).T.astype(BF16)
    for m in range(2):
        q_own[1, m] = (q2_ref[:, m * SIZE : (m + 1) * SIZE].astype(F32) * (LOG2E / math.sqrt(128.0))).T.astype(BF16)
    for g, values in ((0, v1_ref), (1, v2_ref)):
        for b in range(TOK // 256):
            kv_own[g, b * VALUE : (b + 1) * VALUE] = values[b * 256 : (b + 1) * 256].astype(F32).T.astype(BF16)
        prm_own[g, 0:1] = head_gain_ref[g : g + 1]
        prm_own[g, 1:2] = jnp.broadcast_to(mix_ref[g : g + 1], (1, 128))
    for h in range(2):
        kv_own[0, KEYS : KEYS + HALF, h * SIZE : (h + 1) * SIZE] = k1_ref[h * HALF : (h + 1) * HALF]
    kv_own[1, KEYS:SLAB] = k2_ref[...]
    pl.semaphore_wait(barrier, 33)

    def remote(src, dst, send, recv, device):
        return pltpu.make_async_remote_copy(src_ref=src, dst_ref=dst, send_sem=send, recv_sem=recv, device_id=device,
                                            device_id_type=MESH)

    half, odd = lax.div(y, 2), lax.rem(y, 2)
    home = c == half

    def q_views(g, j):
        lanes = pl.ds(j * TOK if isinstance(j, int) else pl.multiple_of(j * TOK, TOK), TOK)
        return (q_own.at[0, 0], q_all.at[0, :, lanes]) if g == 0 else (q_own.at[1], q_all.at[:, :, lanes])

    def slab(slot, g):
        return kv_all.at[slot, pl.ds(0, LENGTHS[g])]

    def spread(g):
        to = at(z, 2 * c + g, x, half)
        return (
            (*q_views(g, odd), q_send.at[g], q_recv.at[odd], to),
            (prm_own.at[g], prm_all.at[odd], prm_send.at[g], prm_recv.at[odd], to),
            (kv_own.at[g, pl.ds(0, LENGTHS[g])], slab(z * 4 + y, g), kv_send.at[g], kv_recv.at[z * 4 + y], to),
        )

    def away(part, g):
        src, dst, send, recv, to = spread(g)[part]

        @pl.when(jnp.logical_not(2 * c + g == y))
        def _():
            remote(src, dst, send, recv, to).start()

    for part in range(2):
        for g in range(2):
            away(part, g)
    def near_or_far(far_ones):
        for g in range(2):
            @pl.when(odd == (g if far_ones else 1 - g))
            def _():
                away(2, g)

    near_or_far(False)

    def place(kind):
        return (y, y + 1 - 2 * odd, 3 - y, lax.rem(y + 2, 4))[kind]

    rows = (z, below, above, far)

    def by_group(action):
        for g in range(2):
            @pl.when(odd == g)
            def _():
                action(g)

    def arrive_of(slot, g):
        remote(slab(slot, g), slab(slot, g), kv_send.at[0], kv_recv.at[slot], side).wait_recv()

    def arrive(slot):
        by_group(lambda g: arrive_of(slot, g))

    def to_side(slot, n, g):
        return remote(slab(slot, g), slab(slot, g), side_send.at[n], kv_recv.at[slot], side)

    def to_right(slot, n, g):
        return remote(slab(slot, g), slab(slot, g), right_send.at[n], kv_recv.at[slot], right)

    def to_left(slot, n, g):
        return remote(slab(slot, g), slab(slot, g), left_send.at[n], kv_recv.at[slot], left)

    def own_shard(g):
        slot = z * 4 + y
        for sends, to in ((right_send, right), (left_send, left), (side_send, side)):
            remote(kv_own.at[g, pl.ds(0, LENGTHS[g])], slab(slot, g), sends.at[0], kv_recv.at[slot], to).start()
        lanes = pl.ds(pl.multiple_of(odd * TOK, TOK), TOK)
        kv_all[slot, 0 : LENGTHS[g]] = kv_own[g, 0 : LENGTHS[g]]
        for m in range(1 + g):
            q_all[m, :, lanes] = q_own[g, m]
        prm_all[odd] = prm_own[g]

    def pass_on(kind, row):
        slot = rows[row] * 4 + place(kind)
        second = kind % 2

        def relay(g):
            arrive_of(slot, g)
            if row == 0:
                to_right(slot, second, g).start()
                to_left(slot, second, g).start()
            elif row == 1 and not second:
                to_right(slot, 2, g).start()
            elif row == 2 and second:
                to_left(slot, 2, g).start()
            to_side(slot, second * 4 + row, g).start()

        by_group(relay)

    east, west = at(z, y, lax.rem(x + 1, 4), c), at(z, y, lax.rem(x + 3, 4), c)
    head_here, head_east = 2 * x + c, 2 * lax.rem(x + 1, 4) + c
    head_west, head_far = 2 * lax.rem(x + 3, 4) + c, 2 * lax.rem(x + 2, 4) + c

    def w_copy(n):
        full = lambda h: w_all.at[h]
        part = lambda h, k: w_all.at[h, pl.ds(k * 128, 128)]
        return (
            lambda: remote(w_ref, full(head_here), w_send.at[0], w_recv.at[head_here], east),
            lambda: remote(w_ref, full(head_here), w_send.at[1], w_recv.at[head_here], west),
            lambda: remote(w_ref, full(head_here), w_send.at[2], w_recv.at[head_here], side),
            lambda: remote(part(head_west, 0), part(head_west, 0), w_send.at[3], w_far.at[0], east),
            lambda: remote(part(head_east, 1), part(head_east, 1), w_send.at[4], w_far.at[1], west),
            lambda: remote(full(head_west), full(head_west), w_send.at[5], w_recv.at[head_west], side),
            lambda: remote(full(head_east), full(head_east), w_send.at[6], w_recv.at[head_east], side),
            lambda: remote(full(head_far), full(head_far), w_send.at[7], w_recv.at[head_far], side),
        )[n]()

    def w_arrive(h):
        remote(w_all.at[h], w_all.at[h], w_send.at[0], w_recv.at[h], side).wait_recv()

    forth, back = at(z, lax.rem(y + 1, 4), x, c), at(z, lax.rem(y + 3, 4), x, c)
    y_forth, y_back, y_far = lax.rem(y + 1, 4), lax.rem(y + 3, 4), lax.rem(y + 2, 4)
    UP, DOWN_A, DOWN_B = 0, 1, 2

    def source(p):
        return up_ref if p == UP else down_ref.at[pl.ds(512 * (p - 1), 512)]

    def shard(p, s, k=None):
        if p == UP:
            if k is None:
                return up_all.at[pl.ds(pl.multiple_of(s * 128, 128), 128)]
            return up_all.at[pl.ds(pl.multiple_of(s * 128 + k * 64, 64), 64)]
        lanes = pl.ds(pl.multiple_of(s * 128, 128), 128)
        start = 512 * (p - 1)
        return down_all.at[pl.ds(start, 512) if k is None else pl.ds(start + k * 256, 256), lanes]

    def lines(p):
        by_z = ((right, left), (below * 4 + y, above * 4 + y, far * 4 + y), lambda r: r * 4 + y, lambda r: r * 4 + y_back,
                lambda r: r * 4 + y_forth, lambda r: r * 4 + y_far)
        by_y = ((forth, back), (z * 4 + y_back, z * 4 + y_forth, z * 4 + y_far), lambda r: z * 4 + r, lambda r: below * 4 + r,
                lambda r: above * 4 + r, lambda r: far * 4 + r)
        return by_y + ((right, left),) if p == UP else by_z + ((forth, back),)

    ff_recv = (up_recv, down_recv, rest_recv)

    def piece(p, n, s, to, k=None, recv=None):
        view = shard(p, s, k)
        return remote(view, view, ff_send.at[16 * p + n], ff_recv[p].at[s] if recv is None else recv, to)

    def ff_first(p, k):
        return remote(source(p), shard(p, sp), ff_send.at[16 * p + k], ff_recv[p].at[sp], lines(p)[0][k])

    def ff_half(p, k):
        return piece(p, 2 + k, lines(p)[1][k], lines(p)[0][k], k, ff_far.at[2 * p + k])

    def ff_column(p, r, k):
        return piece(p, 4 + 2 * r + k, lines(p)[2](r), lines(p)[6][k])

    def ff_onward(p, n, k):
        return piece(p, 12 + 2 * n + k, lines(p)[3 + k](n + 2 * k), lines(p)[6][k])

    def ff_arrive(p, s):
        piece(p, 0, s, side).wait_recv()

    def begin(p):
        pltpu.make_async_copy(source(p), shard(p, sp), ff_own.at[p]).start()
        for k in range(2):
            ff_first(p, k).start()

    def halves(p):
        for k in range(2):
            ff_arrive(p, lines(p)[1][k])
            ff_half(p, k).start()

    def gathered(p):
        for k in range(2):
            piece(p, 0, lines(p)[1][2], side, k, ff_far.at[2 * p + k]).wait_recv()
        pltpu.make_async_copy(source(p), shard(p, sp), ff_own.at[p]).wait()

    def columns(p, second):
        for n in range(2):
            for k in range(2):
                ff_column(p, (n + 2 - 2 * k) if second else (n + 2 * k), k).start()

    def onward(p):
        for n in range(2):
            for k in range(2):
                ff_arrive(p, lines(p)[3 + k](n + 2 * k))
                ff_onward(p, n, k).start()

    def complete(p):
        for n in range(2):
            for k in range(2):
                ff_arrive(p, lines(p)[3 + k](n + 2 - 2 * k))
        for r in range(4):
            ff_arrive(p, lines(p)[5](r))


    @pl.when(home)
    def _():
        by_group(own_shard)

    begin(DOWN_A)
    begin(DOWN_B)

    @pl.when(home)
    def _():
        pass_on(0, 1)
        pass_on(0, 2)


    kinds = (0, 0, 0, 0, 1, 2, 1, 1, 2, 2, 3, 1, 2, 3, 3, 3)
    order = (0, 1, 2, 3, 0, 0, 1, 2, 1, 2, 0, 3, 3, 1, 2, 3)
    home_duties = {0: ((1, 0),), 1: ((0, 3),), 5: ((1, 1), (1, 2)), 10: ((1, 3),)}
    away_duties = {1: ((2, 0),), 4: ((3, 0),), 5: ((2, 1), (2, 2)), 9: ((3, 1), (3, 2)), 10: ((2, 3),), 13: ((3, 3),)}

    def pick(i, table):
        value = jnp.int32(table[0])
        for n in range(1, 16):
            if table[n] != table[n - 1]:
                value = jnp.where(i >= n, table[n], value)
        return value

    def slot_of(i):
        kind, row = pick(i, kinds), pick(i, order)
        row = jnp.where(row == 0, z, jnp.where(row == 1, below, jnp.where(row == 2, above, far)))
        spot = jnp.where(kind == 0, y, jnp.where(kind == 1, y + 1 - 2 * odd, jnp.where(kind == 2, 3 - y, lax.rem(y + 2, 4))))
        return row * 4 + spot

    def duty(i):
        for n in range(16):
            for mine, duties in ((home, home_duties), (jnp.logical_not(home), away_duties)):
                if n in duties:
                    @pl.when(jnp.logical_and(i == n, mine))
                    def _():
                        for kind, row in duties[n]:
                            pass_on(kind, row)
        kind = pick(i + 1, kinds)

        @pl.when(jnp.logical_and(i < 15, jnp.logical_not(home) == (kind < 2)))
        def _():
            arrive(slot_of(i + 1))

        @pl.when(i == 0)
        def _():
            near_or_far(True)
            begin(UP)
            for n in range(3):
                w_copy(n).start()
            pltpu.make_async_copy(w_ref, w_all.at[head_here], w_own).start()

        @pl.when(i == 3)
        def _():
            halves(DOWN_A)
            halves(DOWN_B)
            halves(UP)

        @pl.when(i == 5)
        def _():
            gathered(DOWN_A)
            columns(DOWN_A, False)
            columns(DOWN_A, True)

        @pl.when(i == 7)
        def _():
            gathered(DOWN_B)
            columns(DOWN_B, False)
            columns(DOWN_B, True)

        @pl.when(i == 9)
        def _():
            gathered(UP)
            columns(UP, False)
            columns(UP, True)

        @pl.when(i == 11)
        def _():
            onward(DOWN_A)
            onward(DOWN_B)

        @pl.when(i == 8)
        def _():
            w_arrive(head_west)
            w_copy(3).start()
            w_arrive(head_east)
            w_copy(4).start()
            w_copy(5).start()
            w_copy(6).start()

        @pl.when(i == 12)
        def _():
            for k in range(2):
                remote(w_all.at[0, pl.ds(0, 128)], w_all.at[head_far, pl.ds(k * 128, 128)], w_send.at[0], w_far.at[k],
                       side).wait_recv()
            w_copy(7).start()

    for j in range(2):
        @pl.when(jnp.logical_not(jnp.logical_and(home, odd == j)))
        def _():
            by_group(lambda g: remote(*q_views(g, j), q_send.at[0], q_recv.at[j], side).wait_recv())
            remote(prm_own.at[0], prm_all.at[j], prm_send.at[0], prm_recv.at[j], side).wait_recv()

    @pl.when(odd == 0)
    def _():
        both = q_all[0]
        nothing = jnp.zeros((SIZE // 2, 2 * TOK), BF16)
        q_all[1, 0 : SIZE // 2] = nothing
        q_all[1, SIZE // 2 : SIZE] = both[SIZE // 2 : SIZE]
        q_all[0, SIZE // 2 : SIZE] = nothing

    top[...] = jnp.full(top.shape, LOWEST, F32)
    acc[...] = jnp.zeros(acc.shape, F32)
    ones = jnp.ones((ROWS - VALUE, 256), BF16)

    def scores(slot, tile, m, held):
        queries = q_all[m, :, pl.ds(pl.multiple_of(tile * TILE, TILE), TILE)]
        peak = None
        for h in range(2):
            start = KEYS + (odd * HALF if h else 0)
            entry = m * SIZE if h == m else (odd if m else 1 - odd) * SIZE
            keys = kv_all[slot, pl.ds(pl.multiple_of(start, HALF), HALF), pl.ds(pl.multiple_of(entry, SIZE), SIZE)]
            s = jnp.dot(keys, queries, preferred_element_type=F32)
            held[h * HALF : (h + 1) * HALF] = s
            p = jnp.max(s, axis=0, keepdims=True)
            peak = p if peak is None else jnp.maximum(peak, p)
        return peak

    def absorb(slot, tile, m, held, peak):
        old = top[tile, m]
        new = jnp.maximum(old, peak)
        top[tile, m] = new
        weights = jnp.exp2(held[...] - new).astype(BF16)
        added = None
        for b in range(TOK // 256):
            values = kv_all[slot, b * VALUE : (b + 1) * VALUE, :]
            d = jnp.dot(jnp.concatenate([values, ones], axis=0), weights[b * 256 : (b + 1) * 256],
                        preferred_element_type=F32)
            added = d if added is None else added + d
        acc[tile, m] = acc[tile, m] * jnp.exp2(old - new) + added

    @pl.when(jnp.logical_not(home))
    def _():
        arrive(slot_of(jnp.int32(0)))

    peak = scores(slot_of(jnp.int32(0)), 0, 0, s0)

    def step(t, peak0):
        i, tile = lax.div(t, TILES), lax.rem(t, TILES)
        slot = slot_of(i)

        @pl.when(tile == TILES - 1)
        def _():
            duty(i)

        peak1 = scores(slot, tile, 1, s1)
        absorb(slot, tile, 0, s0, peak0)
        later = jnp.minimum(t + 1, 16 * TILES - 1)
        peak0 = scores(slot_of(lax.div(later, TILES)), lax.rem(later, TILES), 0, s0)
        absorb(slot, tile, 1, s1, peak1)
        return peak0

    lax.fori_loop(0, 16 * TILES, step, peak)

    gain = prm_all[0, 0:1, :]
    mix = prm_all[0, 1:2, 0:1]
    for tile in range(TILES):
        a1, a2 = acc[tile, 0], acc[tile, 1]
        attended = a1[:VALUE] / a1[VALUE : VALUE + 1] - mix * (a2[:VALUE] / a2[VALUE : VALUE + 1])
        square = jnp.mean(attended * attended, axis=0, keepdims=True)
        scaled = attended * lax.rsqrt(square + EPSILON)
        heads[tile * TILE : (tile + 1) * TILE, :] = (scaled.T * gain).astype(BF16)

    unit = (2 * x + lax.div(y, 2)) * 2 + lax.rem(y, 2)

    def deliver(n):
        j, tp_ = n // 8, n % 8
        to = {"sp": z * 4 + 2 * c + j, "tp": jnp.int32(tp_)}
        mine = jnp.logical_and(2 * c + j == y, tp == tp_)
        return heads.at[pl.ds(n * OWN, OWN)], got.at[unit], head_send.at[n], head_recv.at[unit], to, mine

    for n in range(16):
        src, dst, send, recv, to, mine = deliver(n)

        @pl.when(mine)
        def _():
            pltpu.make_async_copy(src, dst, recv).start()

        @pl.when(jnp.logical_not(mine))
        def _():
            remote(src, dst, send, recv, to).start()

    onward(UP)
    for n in range(4):
        w_arrive(2 * n + 1 - c)
    pltpu.make_async_copy(w_ref, w_all.at[head_here], w_own).wait()
    for n in range(16):
        remote(got.at[n], got.at[n], head_send.at[n], head_recv.at[n], side).wait_recv()

    residual_copy.wait()

    def project(n, carry):
        columns = pl.ds(pl.multiple_of(n * 512, 512), 512)
        total = residual_ref[:, columns].astype(F32)
        for h in range(8):
            pair = jnp.concatenate([got[2 * h], got[2 * h + 1]], axis=1)
            total = total + jnp.dot(pair, w_all[h, :, columns], preferred_element_type=F32)
        normed[:, columns] = total
        return carry

    lax.fori_loop(0, 4, project, 0)
    for r in range(0, OWN, 32):
        value = layer_norm(normed[r : r + 32], gain_ref[0:1])
        normed[r : r + 32] = value
        tokens[tp, r : r + 32] = value.astype(BF16)

    def tok_copy(n):
        t_west, t_east, t_far = 2 * lax.rem(x + 3, 4) + c, 2 * lax.rem(x + 1, 4) + c, 2 * lax.rem(x + 2, 4) + c
        half_of = lambda t, k: tokens.at[t, pl.ds(k * 48, 48)]
        return (
            lambda: remote(tokens.at[tp], tokens.at[tp], tok_send.at[0], tok_recv.at[tp], east),
            lambda: remote(tokens.at[tp], tokens.at[tp], tok_send.at[1], tok_recv.at[tp], west),
            lambda: remote(tokens.at[tp], tokens.at[tp], tok_send.at[2], tok_recv.at[tp], side),
            lambda: remote(half_of(t_west, 0), half_of(t_west, 0), tok_send.at[3], tok_far.at[0], east),
            lambda: remote(half_of(t_east, 1), half_of(t_east, 1), tok_send.at[4], tok_far.at[1], west),
            lambda: remote(tokens.at[t_west], tokens.at[t_west], tok_send.at[5], tok_recv.at[t_west], side),
            lambda: remote(tokens.at[t_east], tokens.at[t_east], tok_send.at[6], tok_recv.at[t_east], side),
            lambda: remote(tokens.at[t_far], tokens.at[t_far], tok_send.at[7], tok_recv.at[t_far], side),
        )[n]()

    def tok_arrive(t):
        remote(tokens.at[t], tokens.at[t], tok_send.at[0], tok_recv.at[t], side).wait_recv()

    for n in range(3):
        tok_copy(n).start()
    complete(UP)

    chips = (x, lax.rem(x + 3, 4), lax.rem(x + 1, 4), lax.rem(x + 2, 4))

    def feed(k):
        chip = chips[k]
        rows_in = (2 * chip + c, 2 * chip + 1 - c)

        def up(n, carry):
            columns = pl.ds(pl.multiple_of(n * 512, 512), 512)
            block = jnp.concatenate([tokens[rows_in[0]], tokens[rows_in[1]]], axis=0)
            e = jnp.maximum(jnp.dot(block, up_all[:, columns], preferred_element_type=F32), 0.0)
            hidden[:, columns] = (e * e).astype(BF16)
            return carry

        lax.fori_loop(0, 2, up, 0)
        if k == 0:
            complete(DOWN_A)
            complete(DOWN_B)

        def down(n, carry):
            columns = pl.ds(pl.multiple_of(n * 512, 512), 512)
            p = jnp.dot(hidden[...], down_all[:, columns], preferred_element_type=F32)
            keep[k, :, columns] = p[:OWN]
            to_sib[k, :, columns] = p[OWN:].astype(BF16)
            return carry

        lax.fori_loop(0, 4, down, 0)

    def to_sibling(k):
        return remote(to_sib.at[k], from_sib.at[k], sib_send.at[k], sib_recv.at[k], side)

    def to_owner(k):
        return remote(to_chip.at[k - 1], from_chip.at[k - 1], chip_send.at[k - 1], chip_recv.at[k - 1], (None, west, east, at(z, y, lax.rem(x + 2, 4), c))[k])

    def chip_sum(k):
        to_sibling(k).wait_recv()
        for r in range(0, OWN, 32):
            to_chip[k - 1, r : r + 32] = (keep[k, r : r + 32] + from_sib[k, r : r + 32].astype(F32)).astype(BF16)
        to_owner(k).start()

    tok_arrive(2 * x + 1 - c)
    feed(0)
    to_sibling(0).start()
    west_tok, east_tok, far_tok = (2 * chips[k] + c for k in (1, 2, 3))
    tok_arrive(west_tok)
    tok_copy(3).start()
    tok_copy(5).start()
    tok_arrive(east_tok)
    tok_copy(4).start()
    tok_copy(6).start()
    tok_arrive(2 * chips[1] + 1 - c)
    feed(1)
    to_sibling(1).start()
    tok_arrive(2 * chips[2] + 1 - c)
    feed(2)
    to_sibling(2).start()
    chip_sum(1)
    for k in range(2):
        spot = tokens.at[far_tok, pl.ds(k * 48, 48)]
        remote(spot, spot, tok_send.at[0], tok_far.at[k], side).wait_recv()
    tok_copy(7).start()
    chip_sum(2)
    tok_arrive(2 * chips[3] + 1 - c)
    feed(3)
    to_sibling(3).start()
    chip_sum(3)
    to_sibling(0).wait_recv()
    for k in range(1, 4):
        to_owner(k).wait_recv()
    for r in range(0, OWN, 32):
        span = slice(r, r + 32)
        total = normed[span] + keep[0, span] + from_sib[0, span].astype(F32)
        for k in range(3):
            total = total + from_chip[k, span].astype(F32)
        out_ref[span] = layer_norm(total, gain_ref[1:2]).astype(BF16)

    for part in range(3):
        for g in range(2):
            src, dst, send, recv, to = spread(g)[part]

            @pl.when(jnp.logical_not(2 * c + g == y))
            def _():
                remote(src, dst, send, recv, to).wait_send()

    def sent(g):
        for n in range(3):
            to_right(0, n, g).wait_send()
            to_left(0, n, g).wait_send()
        for n in range(8):
            to_side(0, n, g).wait_send()

    by_group(sent)
    for n in range(8):
        w_copy(n).wait_send()
        tok_copy(n).wait_send()
    for n in range(16):
        src, dst, send, recv, to, mine = deliver(n)

        @pl.when(jnp.logical_not(mine))
        def _():
            remote(src, dst, send, recv, to).wait_send()

    for w in range(3):
        for k in range(2):
            ff_first(w, k).wait_send()
            ff_half(w, k).wait_send()
            for row in range(4):
                ff_column(w, row, k).wait_send()
            for n in range(2):
                ff_onward(w, n, k).wait_send()
    for k in range(4):
        to_sibling(k).wait_send()
    for k in range(1, 4):
        to_owner(k).wait_send()


def layer(*operands):
    dma = pltpu.SemaphoreType.DMA
    vmem, hbm = pl.BlockSpec(memory_space=pltpu.VMEM), pl.BlockSpec(memory_space=pl.ANY)
    return pl.pallas_call(
        attention_kernel,
        out_shape=jax.ShapeDtypeStruct((OWN, 2048), BF16),
        in_specs=[vmem] * 8 + [hbm] * 4 + [vmem],
        out_specs=vmem,
        scratch_shapes=[
            pltpu.VMEM((2, 2, SIZE, TOK), BF16),
            pltpu.VMEM((2, SLAB, 256), BF16),
            pltpu.VMEM((2, 8, 128), F32),
            pltpu.VMEM((OWN, 2048), BF16),
            dma(()),
            pltpu.VMEM((2, SIZE, 2 * TOK), BF16),
            pltpu.VMEM((16, SLAB, 256), BF16),
            pltpu.VMEM((2, 8, 128), F32),
            pltpu.VMEM((8, 256, 2048), BF16),
            pltpu.VMEM((TOK, TILE), F32),
            pltpu.VMEM((TOK, TILE), F32),
            pltpu.VMEM((TILES, 2, 1, TILE), F32),
            pltpu.VMEM((TILES, 2, ROWS, TILE), F32),
            pltpu.VMEM((2 * TOK, VALUE), BF16),
            pltpu.VMEM((16, OWN, VALUE), BF16),
            dma((2,)), dma((2,)), dma((2,)), dma((3,)), dma((3,)), dma((8,)), dma((16,)), dma((8,)),
            dma((2,)), dma((16,)), dma((2,)), dma((16,)), dma((8,)), dma((2,)), dma(()),
            pltpu.VMEM((2048, 1024), BF16),
            pltpu.VMEM((1024, 2048), BF16),
            pltpu.VMEM((8, OWN, 2048), BF16),
            pltpu.VMEM((OWN, 2048), F32),
            pltpu.VMEM((2 * OWN, 1024), BF16),
            pltpu.VMEM((4, OWN, 2048), F32),
            pltpu.VMEM((4, OWN, 2048), BF16),
            pltpu.VMEM((4, OWN, 2048), BF16),
            pltpu.VMEM((3, OWN, 2048), BF16),
            pltpu.VMEM((3, OWN, 2048), BF16),
            dma((48,)), dma((16,)), dma((16,)), dma((16,)), dma((6,)), dma((3,)), dma((8,)), dma((8,)), dma((2,)), dma((4,)), dma((4,)),
            dma((3,)), dma((3,)),
        ],
        compiler_params=pltpu.CompilerParams(collective_id=0, has_side_effects=True, vmem_limit_bytes=63 << 20),
        cost_estimate=pl.CostEstimate(flops=4 * 768 * 12288 * 4 * 128, bytes_accessed=4 << 20, transcendentals=4 * 768 * 12288),
        name="attention",
    )(*operands)


def layer_norm(activations, scales):
    average = jnp.mean(activations, axis=-1, keepdims=True)
    centred = activations - average
    spread = jnp.mean(centred * centred, axis=-1, keepdims=True)
    return centred * lax.rsqrt(spread + EPSILON) * scales


def local(query_first, key_first, value_first, query_second, key_second, value_second, mix_lambda, head_gain, out_weight,
          residual, norm_gain, up_weight, down_weight):
    return layer(query_first[:, 0], key_first[:, 0], value_first[:, 0], query_second[:, 0], key_second[:, 0], value_second[:, 0],
                 mix_lambda, head_gain[:, 0], out_weight.reshape(2 * VALUE, -1), up_weight, down_weight, residual, norm_gain)


def solution(mesh):
    heads = P("sp", "tp", None)
    return jax.shard_map(
        local,
        mesh=mesh,
        in_specs=(heads, heads, heads, heads, heads, heads, P(None, "tp"), P(None, "tp", None), P(None, "tp", None, None),
                  P(("sp", "tp"), None), P(), P("sp", "tp"), P("tp", "sp")),
        out_specs=P(("sp", "tp"), None),
        check_vma=False,
    )
```

```python
import functools
import math

import jax
import jax.numpy as jnp
from jax import lax
from jax.experimental import pallas as pl
from jax.experimental.pallas import tpu as pltpu
from jax.sharding import PartitionSpec as P

EPSILON = 1e-05
LOWEST = -1e30
LOG2E = math.log2(math.e)
MESH = pl.DeviceIdType.MESH
BF16 = jnp.bfloat16
F32 = jnp.float32

TOK = 768
OWN = 96
SIZE = 128
VALUE = 128
HALF = TOK // 2
KEYS = VALUE * TOK // 256
SLAB = KEYS + TOK
LENGTHS = (KEYS + HALF, SLAB)
TILE = 512
TILES = 2 * TOK // TILE
ROWS = VALUE + 16


def attention_kernel(q1_ref, k1_ref, v1_ref, q2_ref, k2_ref, v2_ref, mix_ref, head_gain_ref, w_ref, up_ref, down_ref, residual_hbm,
                     gain_ref, out_ref, q_own, kv_own, prm_own, residual_ref, residual_sem, q_all, kv_all, prm_all, w_all, s0, s1, top, acc, heads, got,
                     q_send, kv_send, prm_send, right_send, left_send, side_send, head_send, w_send,
                     q_recv, kv_recv, prm_recv, head_recv, w_recv, w_far, w_own,
                     up_all, down_all, tokens, normed, hidden, keep, to_sib, from_sib, to_chip, from_chip,
                     ff_send, up_recv, down_recv, rest_recv, ff_far, ff_own, tok_send, tok_recv, tok_far, sib_send, sib_recv,
                     chip_send, chip_recv):
    sp, tp = lax.axis_index("sp"), lax.axis_index("tp")
    z, y = lax.div(sp, 4), lax.rem(sp, 4)
    x, c = lax.div(tp, 2), lax.rem(tp, 2)

    def at(z_, y_, x_, c_):
        return {"sp": z_ * 4 + y_, "tp": x_ * 2 + c_}

    above, below = lax.rem(z + 1, 4), lax.rem(z + 3, 4)
    far = lax.rem(z + 2, 4)
    right, left, side = at(above, y, x, c), at(below, y, x, c), at(z, y, x, 1 - c)

    barrier = pltpu.get_barrier_semaphore()

    def greet(i, carry):
        other = lax.rem(y * 8 + tp + i, 32)
        pl.semaphore_signal(barrier, inc=1, device_id={"sp": z * 4 + lax.div(other, 8), "tp": lax.rem(other, 8)},
                            device_id_type=MESH)
        return carry

    lax.fori_loop(1, 32, greet, 0)
    pl.semaphore_signal(barrier, inc=1, device_id=right, device_id_type=MESH)
    pl.semaphore_signal(barrier, inc=1, device_id=left, device_id_type=MESH)
    residual_copy = pltpu.make_async_copy(residual_hbm, residual_ref, residual_sem)
    residual_copy.start()

    q_own[0, 0] = (q1_ref[...].astype(F32) * (LOG2E / 8.0)).T.astype(BF16)
    for m in range(2):
        q_own[1, m] = (q2_ref[:, m * SIZE : (m + 1) * SIZE].astype(F32) * (LOG2E / math.sqrt(128.0))).T.astype(BF16)
    for g, values in ((0, v1_ref), (1, v2_ref)):
        for b in range(TOK // 256):
            kv_own[g, b * VALUE : (b + 1) * VALUE] = values[b * 256 : (b + 1) * 256].astype(F32).T.astype(BF16)
        prm_own[g, 0:1] = head_gain_ref[g : g + 1]
        prm_own[g, 1:2] = jnp.broadcast_to(mix_ref[g : g + 1], (1, 128))
    for h in range(2):
        kv_own[0, KEYS : KEYS + HALF, h * SIZE : (h + 1) * SIZE] = k1_ref[h * HALF : (h + 1) * HALF]
    kv_own[1, KEYS:SLAB] = k2_ref[...]
    pl.semaphore_wait(barrier, 33)

    def remote(src, dst, send, recv, device):
        return pltpu.make_async_remote_copy(src_ref=src, dst_ref=dst, send_sem=send, recv_sem=recv, device_id=device,
                                            device_id_type=MESH)

    half, odd = lax.div(y, 2), lax.rem(y, 2)
    home = c == half

    def q_views(g, j):
        lanes = pl.ds(j * TOK if isinstance(j, int) else pl.multiple_of(j * TOK, TOK), TOK)
        return (q_own.at[0, 0], q_all.at[0, :, lanes]) if g == 0 else (q_own.at[1], q_all.at[:, :, lanes])

    def slab(slot, g):
        return kv_all.at[slot, pl.ds(0, LENGTHS[g])]

    def spread(g):
        to = at(z, 2 * c + g, x, half)
        return (
            (*q_views(g, odd), q_send.at[g], q_recv.at[odd], to),
            (prm_own.at[g], prm_all.at[odd], prm_send.at[g], prm_recv.at[odd], to),
            (kv_own.at[g, pl.ds(0, LENGTHS[g])], slab(z * 4 + y, g), kv_send.at[g], kv_recv.at[z * 4 + y], to),
        )

    def away(part, g):
        src, dst, send, recv, to = spread(g)[part]

        @pl.when(jnp.logical_not(2 * c + g == y))
        def _():
            remote(src, dst, send, recv, to).start()

    for part in range(2):
        for g in range(2):
            away(part, g)
    def near_or_far(far_ones):
        for g in range(2):
            @pl.when(odd == (g if far_ones else 1 - g))
            def _():
                away(2, g)

    near_or_far(False)

    def place(kind):
        return (y, y + 1 - 2 * odd, 3 - y, lax.rem(y + 2, 4))[kind]

    rows = (z, below, above, far)

    def by_group(action):
        for g in range(2):
            @pl.when(odd == g)
            def _():
                action(g)

    def arrive_of(slot, g):
        remote(slab(slot, g), slab(slot, g), kv_send.at[0], kv_recv.at[slot], side).wait_recv()

    def arrive(slot):
        by_group(lambda g: arrive_of(slot, g))

    def to_side(slot, n, g):
        return remote(slab(slot, g), slab(slot, g), side_send.at[n], kv_recv.at[slot], side)

    def to_right(slot, n, g):
        return remote(slab(slot, g), slab(slot, g), right_send.at[n], kv_recv.at[slot], right)

    def to_left(slot, n, g):
        return remote(slab(slot, g), slab(slot, g), left_send.at[n], kv_recv.at[slot], left)

    def own_shard(g):
        slot = z * 4 + y
        for sends, to in ((right_send, right), (left_send, left), (side_send, side)):
            remote(kv_own.at[g, pl.ds(0, LENGTHS[g])], slab(slot, g), sends.at[0], kv_recv.at[slot], to).start()
        lanes = pl.ds(pl.multiple_of(odd * TOK, TOK), TOK)
        kv_all[slot, 0 : LENGTHS[g]] = kv_own[g, 0 : LENGTHS[g]]
        for m in range(1 + g):
            q_all[m, :, lanes] = q_own[g, m]
        prm_all[odd] = prm_own[g]

    def pass_on(kind, row):
        slot = rows[row] * 4 + place(kind)
        second = kind % 2

        def relay(g):
            arrive_of(slot, g)
            if row == 0:
                to_right(slot, second, g).start()
                to_left(slot, second, g).start()
            elif row == 1 and not second:
                to_right(slot, 2, g).start()
            elif row == 2 and second:
                to_left(slot, 2, g).start()
            to_side(slot, second * 4 + row, g).start()

        by_group(relay)

    east, west = at(z, y, lax.rem(x + 1, 4), c), at(z, y, lax.rem(x + 3, 4), c)
    head_here, head_east = 2 * x + c, 2 * lax.rem(x + 1, 4) + c
    head_west, head_far = 2 * lax.rem(x + 3, 4) + c, 2 * lax.rem(x + 2, 4) + c

    def w_copy(n):
        full = lambda h: w_all.at[h]
        part = lambda h, k: w_all.at[h, pl.ds(k * 128, 128)]
        return (
            lambda: remote(w_ref, full(head_here), w_send.at[0], w_recv.at[head_here], east),
            lambda: remote(w_ref, full(head_here), w_send.at[1], w_recv.at[head_here], west),
            lambda: remote(w_ref, full(head_here), w_send.at[2], w_recv.at[head_here], side),
            lambda: remote(part(head_west, 0), part(head_west, 0), w_send.at[3], w_far.at[0], east),
            lambda: remote(part(head_east, 1), part(head_east, 1), w_send.at[4], w_far.at[1], west),
            lambda: remote(full(head_west), full(head_west), w_send.at[5], w_recv.at[head_west], side),
            lambda: remote(full(head_east), full(head_east), w_send.at[6], w_recv.at[head_east], side),
            lambda: remote(full(head_far), full(head_far), w_send.at[7], w_recv.at[head_far], side),
        )[n]()

    def w_arrive(h):
        remote(w_all.at[h], w_all.at[h], w_send.at[0], w_recv.at[h], side).wait_recv()

    forth, back = at(z, lax.rem(y + 1, 4), x, c), at(z, lax.rem(y + 3, 4), x, c)
    y_forth, y_back, y_far = lax.rem(y + 1, 4), lax.rem(y + 3, 4), lax.rem(y + 2, 4)
    UP, DOWN_A, DOWN_B = 0, 1, 2

    def source(p):
        return up_ref if p == UP else down_ref.at[pl.ds(512 * (p - 1), 512)]

    def shard(p, s, k=None):
        if p == UP:
            if k is None:
                return up_all.at[pl.ds(pl.multiple_of(s * 128, 128), 128)]
            return up_all.at[pl.ds(pl.multiple_of(s * 128 + k * 64, 64), 64)]
        lanes = pl.ds(pl.multiple_of(s * 128, 128), 128)
        start = 512 * (p - 1)
        return down_all.at[pl.ds(start, 512) if k is None else pl.ds(start + k * 256, 256), lanes]

    def lines(p):
        by_z = ((right, left), (below * 4 + y, above * 4 + y, far * 4 + y), lambda r: r * 4 + y, lambda r: r * 4 + y_back,
                lambda r: r * 4 + y_forth, lambda r: r * 4 + y_far)
        by_y = ((forth, back), (z * 4 + y_back, z * 4 + y_forth, z * 4 + y_far), lambda r: z * 4 + r, lambda r: below * 4 + r,
                lambda r: above * 4 + r, lambda r: far * 4 + r)
        return by_y + ((right, left),) if p == UP else by_z + ((forth, back),)

    ff_recv = (up_recv, down_recv, rest_recv)

    def piece(p, n, s, to, k=None, recv=None):
        view = shard(p, s, k)
        return remote(view, view, ff_send.at[16 * p + n], ff_recv[p].at[s] if recv is None else recv, to)

    def ff_first(p, k):
        return remote(source(p), shard(p, sp), ff_send.at[16 * p + k], ff_recv[p].at[sp], lines(p)[0][k])

    def ff_half(p, k):
        return piece(p, 2 + k, lines(p)[1][k], lines(p)[0][k], k, ff_far.at[2 * p + k])

    def ff_column(p, r, k):
        return piece(p, 4 + 2 * r + k, lines(p)[2](r), lines(p)[6][k])

    def ff_onward(p, n, k):
        return piece(p, 12 + 2 * n + k, lines(p)[3 + k](n + 2 * k), lines(p)[6][k])

    def ff_arrive(p, s):
        piece(p, 0, s, side).wait_recv()

    def begin(p):
        pltpu.make_async_copy(source(p), shard(p, sp), ff_own.at[p]).start()
        for k in range(2):
            ff_first(p, k).start()

    def halves(p):
        for k in range(2):
            ff_arrive(p, lines(p)[1][k])
            ff_half(p, k).start()

    def gathered(p):
        for k in range(2):
            piece(p, 0, lines(p)[1][2], side, k, ff_far.at[2 * p + k]).wait_recv()
        pltpu.make_async_copy(source(p), shard(p, sp), ff_own.at[p]).wait()

    def columns(p, second):
        for n in range(2):
            for k in range(2):
                ff_column(p, (n + 2 - 2 * k) if second else (n + 2 * k), k).start()

    def onward(p):
        for n in range(2):
            for k in range(2):
                ff_arrive(p, lines(p)[3 + k](n + 2 * k))
                ff_onward(p, n, k).start()

    def complete(p):
        for n in range(2):
            for k in range(2):
                ff_arrive(p, lines(p)[3 + k](n + 2 - 2 * k))
        for r in range(4):
            ff_arrive(p, lines(p)[5](r))


    @pl.when(home)
    def _():
        by_group(own_shard)

    begin(DOWN_A)
    begin(DOWN_B)

    @pl.when(home)
    def _():
        pass_on(0, 1)
        pass_on(0, 2)


    kinds = (0, 0, 0, 0, 1, 2, 1, 1, 2, 2, 3, 1, 2, 3, 3, 3)
    order = (0, 1, 2, 3, 0, 0, 1, 2, 1, 2, 0, 3, 3, 1, 2, 3)
    home_duties = {0: ((1, 0),), 1: ((0, 3),), 5: ((1, 1), (1, 2)), 10: ((1, 3),)}
    away_duties = {1: ((2, 0),), 4: ((3, 0),), 5: ((2, 1), (2, 2)), 9: ((3, 1), (3, 2)), 10: ((2, 3),), 13: ((3, 3),)}

    def pick(i, table):
        value = jnp.int32(table[0])
        for n in range(1, 16):
            if table[n] != table[n - 1]:
                value = jnp.where(i >= n, table[n], value)
        return value

    def slot_of(i):
        kind, row = pick(i, kinds), pick(i, order)
        row = jnp.where(row == 0, z, jnp.where(row == 1, below, jnp.where(row == 2, above, far)))
        spot = jnp.where(kind == 0, y, jnp.where(kind == 1, y + 1 - 2 * odd, jnp.where(kind == 2, 3 - y, lax.rem(y + 2, 4))))
        return row * 4 + spot

    def duty(i):
        for n in range(16):
            for mine, duties in ((home, home_duties), (jnp.logical_not(home), away_duties)):
                if n in duties:
                    @pl.when(jnp.logical_and(i == n, mine))
                    def _():
                        for kind, row in duties[n]:
                            pass_on(kind, row)
        kind = pick(i + 1, kinds)

        @pl.when(jnp.logical_and(i < 15, jnp.logical_not(home) == (kind < 2)))
        def _():
            arrive(slot_of(i + 1))

        @pl.when(i == 0)
        def _():
            near_or_far(True)
            begin(UP)
            for n in range(3):
                w_copy(n).start()
            pltpu.make_async_copy(w_ref, w_all.at[head_here], w_own).start()

        @pl.when(i == 3)
        def _():
            halves(DOWN_A)
            halves(DOWN_B)
            halves(UP)

        @pl.when(i == 5)
        def _():
            gathered(DOWN_A)
            columns(DOWN_A, False)
            columns(DOWN_A, True)

        @pl.when(i == 7)
        def _():
            gathered(DOWN_B)
            columns(DOWN_B, False)
            columns(DOWN_B, True)

        @pl.when(i == 9)
        def _():
            gathered(UP)
            columns(UP, False)
            columns(UP, True)

        @pl.when(i == 12)
        def _():
            onward(DOWN_A)
            onward(DOWN_B)

        @pl.when(i == 8)
        def _():
            w_arrive(head_west)
            w_copy(3).start()
            w_arrive(head_east)
            w_copy(4).start()
            w_copy(5).start()
            w_copy(6).start()

        @pl.when(i == 12)
        def _():
            for k in range(2):
                remote(w_all.at[0, pl.ds(0, 128)], w_all.at[head_far, pl.ds(k * 128, 128)], w_send.at[0], w_far.at[k],
                       side).wait_recv()
            w_copy(7).start()

    for j in range(2):
        @pl.when(jnp.logical_not(jnp.logical_and(home, odd == j)))
        def _():
            by_group(lambda g: remote(*q_views(g, j), q_send.at[0], q_recv.at[j], side).wait_recv())
            remote(prm_own.at[0], prm_all.at[j], prm_send.at[0], prm_recv.at[j], side).wait_recv()

    @pl.when(odd == 0)
    def _():
        both = q_all[0]
        nothing = jnp.zeros((SIZE // 2, 2 * TOK), BF16)
        q_all[1, 0 : SIZE // 2] = nothing
        q_all[1, SIZE // 2 : SIZE] = both[SIZE // 2 : SIZE]
        q_all[0, SIZE // 2 : SIZE] = nothing

    top[...] = jnp.full(top.shape, LOWEST, F32)
    acc[...] = jnp.zeros(acc.shape, F32)
    ones = jnp.ones((ROWS - VALUE, 256), BF16)

    def scores(slot, tile, m, held):
        queries = q_all[m, :, pl.ds(pl.multiple_of(tile * TILE, TILE), TILE)]
        peak = None
        for h in range(2):
            start = KEYS + (odd * HALF if h else 0)
            entry = m * SIZE if h == m else (odd if m else 1 - odd) * SIZE
            keys = kv_all[slot, pl.ds(pl.multiple_of(start, HALF), HALF), pl.ds(pl.multiple_of(entry, SIZE), SIZE)]
            s = jnp.dot(keys, queries, preferred_element_type=F32)
            held[h * HALF : (h + 1) * HALF] = s
            p = jnp.max(s, axis=0, keepdims=True)
            peak = p if peak is None else jnp.maximum(peak, p)
        return peak

    def absorb(slot, tile, m, held, peak):
        old = top[tile, m]
        new = jnp.maximum(old, peak)
        top[tile, m] = new
        weights = jnp.exp2(held[...] - new).astype(BF16)
        added = None
        for b in range(TOK // 256):
            values = kv_all[slot, b * VALUE : (b + 1) * VALUE, :]
            d = jnp.dot(jnp.concatenate([values, ones], axis=0), weights[b * 256 : (b + 1) * 256],
                        preferred_element_type=F32)
            added = d if added is None else added + d
        acc[tile, m] = acc[tile, m] * jnp.exp2(old - new) + added

    @pl.when(jnp.logical_not(home))
    def _():
        arrive(slot_of(jnp.int32(0)))

    peak = scores(slot_of(jnp.int32(0)), 0, 0, s0)

    def step(t, peak0):
        i, tile = lax.div(t, TILES), lax.rem(t, TILES)
        slot = slot_of(i)

        @pl.when(tile == TILES - 1)
        def _():
            duty(i)

        peak1 = scores(slot, tile, 1, s1)
        absorb(slot, tile, 0, s0, peak0)
        later = jnp.minimum(t + 1, 16 * TILES - 1)
        peak0 = scores(slot_of(lax.div(later, TILES)), lax.rem(later, TILES), 0, s0)
        absorb(slot, tile, 1, s1, peak1)
        return peak0

    lax.fori_loop(0, 16 * TILES, step, peak)

    gain = prm_all[0, 0:1, :]
    mix = prm_all[0, 1:2, 0:1]
    for tile in range(TILES):
        a1, a2 = acc[tile, 0], acc[tile, 1]
        attended = a1[:VALUE] / a1[VALUE : VALUE + 1] - mix * (a2[:VALUE] / a2[VALUE : VALUE + 1])
        square = jnp.mean(attended * attended, axis=0, keepdims=True)
        scaled = attended * lax.rsqrt(square + EPSILON)
        heads[tile * TILE : (tile + 1) * TILE, :] = (scaled.T * gain).astype(BF16)

    unit = (2 * x + lax.div(y, 2)) * 2 + lax.rem(y, 2)

    def deliver(n):
        j, tp_ = n // 8, n % 8
        to = {"sp": z * 4 + 2 * c + j, "tp": jnp.int32(tp_)}
        mine = jnp.logical_and(2 * c + j == y, tp == tp_)
        return heads.at[pl.ds(n * OWN, OWN)], got.at[unit], head_send.at[n], head_recv.at[unit], to, mine

    for n in range(16):
        src, dst, send, recv, to, mine = deliver(n)

        @pl.when(mine)
        def _():
            pltpu.make_async_copy(src, dst, recv).start()

        @pl.when(jnp.logical_not(mine))
        def _():
            remote(src, dst, send, recv, to).start()

    onward(UP)
    for n in range(4):
        w_arrive(2 * n + 1 - c)
    pltpu.make_async_copy(w_ref, w_all.at[head_here], w_own).wait()
    for n in range(16):
        remote(got.at[n], got.at[n], head_send.at[n], head_recv.at[n], side).wait_recv()

    residual_copy.wait()

    def project(n, carry):
        columns = pl.ds(pl.multiple_of(n * 512, 512), 512)
        total = residual_ref[:, columns].astype(F32)
        for h in range(8):
            pair = jnp.concatenate([got[2 * h], got[2 * h + 1]], axis=1)
            total = total + jnp.dot(pair, w_all[h, :, columns], preferred_element_type=F32)
        normed[:, columns] = total
        return carry

    lax.fori_loop(0, 4, project, 0)
    for r in range(0, OWN, 32):
        value = layer_norm(normed[r : r + 32], gain_ref[0:1])
        normed[r : r + 32] = value
        tokens[tp, r : r + 32] = value.astype(BF16)

    def tok_copy(n):
        t_west, t_east, t_far = 2 * lax.rem(x + 3, 4) + c, 2 * lax.rem(x + 1, 4) + c, 2 * lax.rem(x + 2, 4) + c
        half_of = lambda t, k: tokens.at[t, pl.ds(k * 48, 48)]
        return (
            lambda: remote(tokens.at[tp], tokens.at[tp], tok_send.at[0], tok_recv.at[tp], east),
            lambda: remote(tokens.at[tp], tokens.at[tp], tok_send.at[1], tok_recv.at[tp], west),
            lambda: remote(tokens.at[tp], tokens.at[tp], tok_send.at[2], tok_recv.at[tp], side),
            lambda: remote(half_of(t_west, 0), half_of(t_west, 0), tok_send.at[3], tok_far.at[0], east),
            lambda: remote(half_of(t_east, 1), half_of(t_east, 1), tok_send.at[4], tok_far.at[1], west),
            lambda: remote(tokens.at[t_west], tokens.at[t_west], tok_send.at[5], tok_recv.at[t_west], side),
            lambda: remote(tokens.at[t_east], tokens.at[t_east], tok_send.at[6], tok_recv.at[t_east], side),
            lambda: remote(tokens.at[t_far], tokens.at[t_far], tok_send.at[7], tok_recv.at[t_far], side),
        )[n]()

    def tok_arrive(t):
        remote(tokens.at[t], tokens.at[t], tok_send.at[0], tok_recv.at[t], side).wait_recv()

    for n in range(3):
        tok_copy(n).start()
    complete(UP)

    chips = (x, lax.rem(x + 3, 4), lax.rem(x + 1, 4), lax.rem(x + 2, 4))

    def feed(k):
        chip = chips[k]
        rows_in = (2 * chip + c, 2 * chip + 1 - c)

        def up(n, carry):
            columns = pl.ds(pl.multiple_of(n * 512, 512), 512)
            block = jnp.concatenate([tokens[rows_in[0]], tokens[rows_in[1]]], axis=0)
            e = jnp.maximum(jnp.dot(block, up_all[:, columns], preferred_element_type=F32), 0.0)
            hidden[:, columns] = (e * e).astype(BF16)
            return carry

        lax.fori_loop(0, 2, up, 0)
        if k == 0:
            complete(DOWN_A)
            complete(DOWN_B)

        def down(n, carry):
            columns = pl.ds(pl.multiple_of(n * 512, 512), 512)
            p = jnp.dot(hidden[...], down_all[:, columns], preferred_element_type=F32)
            keep[k, :, columns] = p[:OWN]
            to_sib[k, :, columns] = p[OWN:].astype(BF16)
            return carry

        lax.fori_loop(0, 4, down, 0)

    def to_sibling(k):
        return remote(to_sib.at[k], from_sib.at[k], sib_send.at[k], sib_recv.at[k], side)

    def to_owner(k):
        return remote(to_chip.at[k - 1], from_chip.at[k - 1], chip_send.at[k - 1], chip_recv.at[k - 1], (None, west, east, at(z, y, lax.rem(x + 2, 4), c))[k])

    def chip_sum(k):
        to_sibling(k).wait_recv()
        for r in range(0, OWN, 32):
            to_chip[k - 1, r : r + 32] = (keep[k, r : r + 32] + from_sib[k, r : r + 32].astype(F32)).astype(BF16)
        to_owner(k).start()

    tok_arrive(2 * x + 1 - c)
    feed(0)
    to_sibling(0).start()
    west_tok, east_tok, far_tok = (2 * chips[k] + c for k in (1, 2, 3))
    tok_arrive(west_tok)
    tok_copy(3).start()
    tok_copy(5).start()
    tok_arrive(east_tok)
    tok_copy(4).start()
    tok_copy(6).start()
    tok_arrive(2 * chips[1] + 1 - c)
    feed(1)
    to_sibling(1).start()
    tok_arrive(2 * chips[2] + 1 - c)
    feed(2)
    to_sibling(2).start()
    chip_sum(1)
    for k in range(2):
        spot = tokens.at[far_tok, pl.ds(k * 48, 48)]
        remote(spot, spot, tok_send.at[0], tok_far.at[k], side).wait_recv()
    tok_copy(7).start()
    chip_sum(2)
    tok_arrive(2 * chips[3] + 1 - c)
    feed(3)
    to_sibling(3).start()
    chip_sum(3)
    to_sibling(0).wait_recv()
    for k in range(1, 4):
        to_owner(k).wait_recv()
    for r in range(0, OWN, 32):
        span = slice(r, r + 32)
        total = normed[span] + keep[0, span] + from_sib[0, span].astype(F32)
        for k in range(3):
            total = total + from_chip[k, span].astype(F32)
        out_ref[span] = layer_norm(total, gain_ref[1:2]).astype(BF16)

    for part in range(3):
        for g in range(2):
            src, dst, send, recv, to = spread(g)[part]

            @pl.when(jnp.logical_not(2 * c + g == y))
            def _():
                remote(src, dst, send, recv, to).wait_send()

    def sent(g):
        for n in range(3):
            to_right(0, n, g).wait_send()
            to_left(0, n, g).wait_send()
        for n in range(8):
            to_side(0, n, g).wait_send()

    by_group(sent)
    for n in range(8):
        w_copy(n).wait_send()
        tok_copy(n).wait_send()
    for n in range(16):
        src, dst, send, recv, to, mine = deliver(n)

        @pl.when(jnp.logical_not(mine))
        def _():
            remote(src, dst, send, recv, to).wait_send()

    for w in range(3):
        for k in range(2):
            ff_first(w, k).wait_send()
            ff_half(w, k).wait_send()
            for row in range(4):
                ff_column(w, row, k).wait_send()
            for n in range(2):
                ff_onward(w, n, k).wait_send()
    for k in range(4):
        to_sibling(k).wait_send()
    for k in range(1, 4):
        to_owner(k).wait_send()


def layer(*operands):
    dma = pltpu.SemaphoreType.DMA
    vmem, hbm = pl.BlockSpec(memory_space=pltpu.VMEM), pl.BlockSpec(memory_space=pl.ANY)
    return pl.pallas_call(
        attention_kernel,
        out_shape=jax.ShapeDtypeStruct((OWN, 2048), BF16),
        in_specs=[vmem] * 8 + [hbm] * 4 + [vmem],
        out_specs=vmem,
        scratch_shapes=[
            pltpu.VMEM((2, 2, SIZE, TOK), BF16),
            pltpu.VMEM((2, SLAB, 256), BF16),
            pltpu.VMEM((2, 8, 128), F32),
            pltpu.VMEM((OWN, 2048), BF16),
            dma(()),
            pltpu.VMEM((2, SIZE, 2 * TOK), BF16),
            pltpu.VMEM((16, SLAB, 256), BF16),
            pltpu.VMEM((2, 8, 128), F32),
            pltpu.VMEM((8, 256, 2048), BF16),
            pltpu.VMEM((TOK, TILE), F32),
            pltpu.VMEM((TOK, TILE), F32),
            pltpu.VMEM((TILES, 2, 1, TILE), F32),
            pltpu.VMEM((TILES, 2, ROWS, TILE), F32),
            pltpu.VMEM((2 * TOK, VALUE), BF16),
            pltpu.VMEM((16, OWN, VALUE), BF16),
            dma((2,)), dma((2,)), dma((2,)), dma((3,)), dma((3,)), dma((8,)), dma((16,)), dma((8,)),
            dma((2,)), dma((16,)), dma((2,)), dma((16,)), dma((8,)), dma((2,)), dma(()),
            pltpu.VMEM((2048, 1024), BF16),
            pltpu.VMEM((1024, 2048), BF16),
            pltpu.VMEM((8, OWN, 2048), BF16),
            pltpu.VMEM((OWN, 2048), F32),
            pltpu.VMEM((2 * OWN, 1024), BF16),
            pltpu.VMEM((4, OWN, 2048), F32),
            pltpu.VMEM((4, OWN, 2048), BF16),
            pltpu.VMEM((4, OWN, 2048), BF16),
            pltpu.VMEM((3, OWN, 2048), BF16),
            pltpu.VMEM((3, OWN, 2048), BF16),
            dma((48,)), dma((16,)), dma((16,)), dma((16,)), dma((6,)), dma((3,)), dma((8,)), dma((8,)), dma((2,)), dma((4,)), dma((4,)),
            dma((3,)), dma((3,)),
        ],
        compiler_params=pltpu.CompilerParams(collective_id=0, has_side_effects=True, vmem_limit_bytes=63 << 20),
        cost_estimate=pl.CostEstimate(flops=4 * 768 * 12288 * 4 * 128, bytes_accessed=4 << 20, transcendentals=4 * 768 * 12288),
        name="attention",
    )(*operands)


def layer_norm(activations, scales):
    average = jnp.mean(activations, axis=-1, keepdims=True)
    centred = activations - average
    spread = jnp.mean(centred * centred, axis=-1, keepdims=True)
    return centred * lax.rsqrt(spread + EPSILON) * scales


def local(query_first, key_first, value_first, query_second, key_second, value_second, mix_lambda, head_gain, out_weight,
          residual, norm_gain, up_weight, down_weight):
    return layer(query_first[:, 0], key_first[:, 0], value_first[:, 0], query_second[:, 0], key_second[:, 0], value_second[:, 0],
                 mix_lambda, head_gain[:, 0], out_weight.reshape(2 * VALUE, -1), up_weight, down_weight, residual, norm_gain)


def solution(mesh):
    heads = P("sp", "tp", None)
    return jax.shard_map(
        local,
        mesh=mesh,
        in_specs=(heads, heads, heads, heads, heads, heads, P(None, "tp"), P(None, "tp", None), P(None, "tp", None, None),
                  P(("sp", "tp"), None), P(), P("sp", "tp"), P("tp", "sp")),
        out_specs=P(("sp", "tp"), None),
        check_vma=False,
    )
```
